512 devices in a mesh: grp: 2 (over y), dp: 8 (over x), kv: 16 (over z), tp: 2 (over core).
Axes of the slice: x: 8, y: 2, z: 16, core: 2. Of those that a mesh axis runs over, the one named last changes fastest.
The devices are a block of a 8x8x16 slice.
Arguments:
- tokens: bfloat16 [512, 2048], P(('grp', 'dp'), ('kv', 'tp')), parts along dimension 0, may hold values from -40 to 40
- past_state: float32 [512, 16, 128, 128], P(('grp', 'dp', 'kv'), 'tp'), parts along dimension 0, may hold values from -4 to 4
- mix_gain: float32 [2048], P('kv'), may hold values from 0.1 to 1.9
- w_query: bfloat16 [2048, 2048], P('kv', 'tp'), may hold values from -0.125 to 0.125
- w_forget: bfloat16 [2048, 2048], P('kv', 'tp'), may hold values from -0.125 to 0.125
- w_value: bfloat16 [2048, 2048], P('kv', 'tp'), may hold values from -0.125 to 0.125
- w_gate_out: bfloat16 [2048, 2048], P('kv', 'tp'), may hold values from -0.125 to 0.125
- floor_logits: float32 [2048], P('tp'), may hold values from -6 to 6
- head_gain: float32 [128], replicated, may hold values from 0.1 to 1.9
- w_out: bfloat16 [2048, 2048], P(None, ('kv', 'tp')), may hold values from -0.125 to 0.125
- mlp_gain: float32 [2048], replicated, may hold values from 0.1 to 1.9
- w_gate: bfloat16 [2048, 5632], P(None, ('kv', 'tp')), may hold values from -0.125 to 0.125
- w_up: bfloat16 [2048, 5632], P(None, ('kv', 'tp')), may hold values from -0.125 to 0.125
- w_down: bfloat16 [5632, 2048], P(('kv', 'tp')), may hold values from -0.15625 to 0.15625
Outputs:
- result: bfloat16 [512, 2048], P(('grp', 'dp'), ('kv', 'tp')), parts along dimension 0
- new_state: float32 [512, 16, 128, 128], P(('grp', 'dp', 'kv'), 'tp'), parts along dimension 0
The draws below stay inside these ranges and needn't reach their ends.
There are 2 independent parts, one for each index of `grp`. The reference program is written for one: setup_inputs(seed, part) draws one part's arguments, and reference() takes and returns one part's arrays. A program takes and returns all parts, laid end to end along the dimension named above; an argument that names none is the same for every part. Nothing has to cross between parts.
All inputs are finite; a program needn't handle non-finite values.
Results may differ from the reference program's by a relative error of at most 0.0091.
Values may be sent and summed in bfloat16 or wider, within the bound.
A program may use at most 64 MiB of HBM per device.

```python
import math
import jax
import jax.numpy as jnp
from jax import lax

D = 2048
H = 16
DK = 128
DV = 128
FF = 5632
HK = 2048
HV = 2048
SEQS = 256


def draw_tokens(key, part):
    key_base = jax.random.fold_in(key, 101)
    key_rows = jax.random.fold_in(key, 202)
    columns = 10.0 ** (0.5 * (jnp.arange(D, dtype=jnp.float32) / D - 0.5))
    rows = jnp.exp(jax.random.uniform(key_rows, (SEQS, 1), jnp.float32, math.log(0.3), math.log(3.0)))
    base = jnp.clip(jax.random.normal(key_base, (SEQS, D), jnp.float32), -6.0, 6.0)
    return (base * columns * rows).astype(jnp.bfloat16)


def strengthened(drawn, key, source, target, blocks, factor):
    def block_of(position):
        return (jnp.arange(drawn.shape[position]) // (drawn.shape[position] // blocks)).reshape((-1,) + (1,) * (drawn.ndim - 1 - position))

    first = jax.random.permutation(key, blocks)[block_of(target)]
    far = (block_of(target) + blocks // 2) % blocks
    return jnp.where((block_of(source) == first) | (block_of(source) == far), factor * drawn, drawn)


def block_levels(stream_key, shape, split, least, largest):
    factor_of, own = 1.0, jax.random.fold_in(stream_key, 6)
    for position, parts in split:
        draws = jnp.exp(jax.random.uniform(jax.random.fold_in(own, position), (parts,), jnp.float32, least / len(split), largest / len(split)))
        factor_of = factor_of * jnp.repeat(draws, shape[position] // parts).reshape([-1 if axis == position else 1 for axis in range(len(shape))])
    return factor_of


def bell_draw(own_key, extent, deviation, limit, pieces=(), kind=jnp.bfloat16):
    values = jax.random.normal(own_key, extent, jnp.float32) * deviation
    if len(pieces) > 0:
        values = block_levels(own_key, extent, pieces, -0.22, 0.18) * values
    return jnp.clip(values, min=-limit, max=limit).astype(kind)


def bell_draw_with(rng, shape, spread, bound, shards, heavy, held_as=jnp.bfloat16):
    array = spread * jax.random.normal(rng, shape, jnp.float32)
    if shards:
        array = array * block_levels(rng, shape, shards, -0.22, 0.18)
    return jnp.clip(strengthened(array, jax.random.fold_in(rng, 3), *heavy), -bound, bound).astype(held_as)


def setup_inputs(seed: int = 0, part: int = 0) -> dict:
    keys = jax.random.split(jax.random.key(seed), 15)
    own_keys = jax.random.split(jax.random.fold_in(keys[14], part), 15)
    tokens = draw_tokens(jax.random.fold_in(jax.random.fold_in(keys[14], part), 71), part)
    past_state = bell_draw(own_keys[1], (SEQS, H, DK, DV), 0.5, 4.0, ((0, 128), (1, 2)), jnp.float32)
    mix_gain = jnp.clip(1.0 + 0.18 * jax.random.normal(keys[2], (D,), jnp.float32), 0.1, 1.9)
    w_query = bell_draw(keys[3], (D, HK), D ** -0.5, 0.125, ((0, 16), (1, 2)))
    w_forget = bell_draw(keys[4], (D, HK), D ** -0.5, 0.125, ((0, 16), (1, 2)))
    w_value = bell_draw(keys[5], (D, HV), D ** -0.5, 0.125, ((0, 16), (1, 2)))
    w_gate_out = bell_draw(keys[6], (D, HV), D ** -0.5, 0.125, ((0, 16), (1, 2)))
    floor_logits = bell_draw(keys[7], (HK,), 1.5, 6.0, ((0, 2),), jnp.float32)
    head_gain = jnp.clip(1.0 + 0.18 * jax.random.normal(keys[8], (DV,), jnp.float32), 0.1, 1.9)
    w_out = bell_draw(keys[9], (HV, D), HV ** -0.5, 0.125, ((1, 32),))
    mlp_gain = jnp.clip(1.0 + 0.18 * jax.random.normal(keys[10], (D,), jnp.float32), 0.1, 1.9)
    w_gate = bell_draw(keys[11], (D, FF), D ** -0.5, 0.125, ((1, 32),))
    w_up = bell_draw(keys[12], (D, FF), D ** -0.5, 0.125, ((1, 32),))
    w_down = bell_draw_with(keys[13], (FF, D), FF ** -0.5, 0.15625, ((0, 32),), (0, 1, 32, 2.75))
    return dict(tokens=tokens, past_state=past_state, mix_gain=mix_gain, w_query=w_query, w_forget=w_forget, w_value=w_value, w_gate_out=w_gate_out, floor_logits=floor_logits, head_gain=head_gain, w_out=w_out, mlp_gain=mlp_gain, w_gate=w_gate, w_up=w_up, w_down=w_down)


epsilon = 1e-06

def reference(tokens, past_state, mix_gain, w_query, w_forget, w_value, w_gate_out, floor_logits, head_gain, w_out, mlp_gain, w_gate, w_up, w_down):
    count = tokens.shape[0]
    token_f = tokens.astype(jnp.float32)
    row_scale = lax.rsqrt(lax.optimization_barrier(jnp.mean(token_f * token_f, axis=1, keepdims=True)) + epsilon)
    gained = (token_f * mix_gain).astype(jnp.bfloat16)
    query = jnp.dot(gained, w_query, preferred_element_type=jnp.float32) * row_scale
    forget_pre = jnp.dot(gained, w_forget, preferred_element_type=jnp.float32) * row_scale
    value = jnp.dot(gained, w_value, preferred_element_type=jnp.float32) * row_scale
    gate_pre = jnp.dot(gained, w_gate_out, preferred_element_type=jnp.float32) * row_scale
    lower = jax.nn.sigmoid(floor_logits).reshape(H, DK)
    forget = lower + (1.0 - lower) * jax.nn.sigmoid(forget_pre.reshape(count, H, DK))
    values = value.reshape(count, H, DV)
    new_state = forget[..., None] * past_state + (1.0 - forget)[..., None] * values[:, :, None, :]
    activ = jax.nn.silu(query.reshape(count, H, DK))
    head_out = jnp.einsum('shkv,shk->shv', new_state, activ, precision=lax.Precision.HIGHEST)
    normed = head_out * lax.rsqrt(lax.optimization_barrier(jnp.mean(head_out * head_out, axis=2, keepdims=True)) + epsilon)
    normed = normed * head_gain * jax.nn.silu(gate_pre.reshape(count, H, DV))
    mixed = normed.reshape(count, H * DV).astype(jnp.bfloat16)
    middle = (token_f + jnp.dot(mixed, w_out, preferred_element_type=jnp.float32)).astype(jnp.bfloat16)
    middle_f = middle.astype(jnp.float32)
    mlp_scale = lax.rsqrt(lax.optimization_barrier(jnp.mean(middle_f * middle_f, axis=1, keepdims=True)) + epsilon)
    mlp_in = (middle_f * mlp_scale * mlp_gain).astype(jnp.bfloat16)
    gate = jnp.dot(mlp_in, w_gate, preferred_element_type=jnp.float32)
    upward = jnp.dot(mlp_in, w_up, preferred_element_type=jnp.float32)
    hidden = (jax.nn.silu(gate) * upward).astype(jnp.bfloat16)
    result = (middle_f + jnp.dot(hidden, w_down, preferred_element_type=jnp.float32)).astype(jnp.bfloat16)
    return (result, new_state)
```

```python
import functools

import jax
import jax.numpy as jnp
from jax import lax
from jax.experimental import pallas as pl
from jax.experimental.pallas import tpu as pltpu
from jax.sharding import PartitionSpec as P

MESH = pl.DeviceIdType.MESH
EPS = 1e-06
F32 = jnp.float32
BF16 = jnp.bfloat16


def dot(a, b):
    return jnp.dot(a, b, preferred_element_type=F32)


def packed(x):
    half = x.shape[0] // 2
    return jnp.concatenate([x[:half], x[half:]], axis=1)


def halves_swapped(x):
    return pltpu.roll(x, x.shape[1] // 2, 1)


def kernel(
    kv,
    tp,
    tokens,
    past_state,
    mix_gain,
    w_query,
    w_forget,
    w_value,
    w_gate_out,
    floor_logits,
    head_gain,
    w_out,
    mlp_gain,
    w_gate,
    w_up,
    w_down,
    result,
    new_state,
    tok_other,
    proj_w,
    state,
    out_w,
    mlp_w,
    down_w,
    floors,
    heads,
    chunk_out,
    chunk_in,
    sq_out,
    sq_in,
    mix,
    part_out,
    part_in,
    mid,
    wide_out,
    wide_in,
    terms_out,
    terms_in,
    local_sem,
    pair_send,
    pair_recv,
    rs_send,
    rs_recv,
    sq_send,
    sq_recv,
    mix_send,
    mix_recv,
    mid_send,
    mid_recv,
    term_send,
    term_recv,
):
    z = lax.axis_index("kv")
    c = lax.axis_index("tp")
    other = 1 - c
    rows, feats = tokens.shape
    seqs, heads_local, dk, dv = past_state.shape
    units = w_gate.shape[3]
    group = heads_local * seqs
    half_rows = rows // 2
    width = kv * tp * feats
    half_kv = kv // tp
    half_cols = half_kv * tp * feats

    def local(src, dst, i):
        copy = pltpu.make_async_copy(src, dst, local_sem.at[i])
        copy.start()
        return copy

    def remote(src, dst, send, recv, to_z, to_c):
        return pltpu.make_async_remote_copy(
            src_ref=src,
            dst_ref=dst,
            send_sem=send,
            recv_sem=recv,
            device_id={"kv": to_z, "tp": to_c},
            device_id_type=MESH,
        )

    def peer(d):
        return lax.rem(z + d, kv)

    far_first = sorted(range(1, kv), key=lambda d: -min(d, kv - d))
    near_first = far_first[::-1]

    barrier = pltpu.get_barrier_semaphore()
    for d in far_first:
        pl.semaphore_signal(barrier, inc=1, device_id={"kv": peer(d), "tp": c}, device_id_type=MESH)
    pl.semaphore_signal(barrier, inc=1, device_id={"kv": z, "tp": other}, device_id_type=MESH)

    proj_copies = [
        local(w, proj_w.at[i], i) for i, w in enumerate((w_query, w_forget, w_value, w_gate_out))
    ]
    state_copy = local(past_state, state, 4)
    half_of = pl.ds(pl.multiple_of(c * half_cols, half_cols), half_cols)
    half_of_other = pl.ds(pl.multiple_of(other * half_cols, half_cols), half_cols)
    weight_copies = [
        local(w_out.at[c], out_w.at[0], 5),
        local(w_gate.at[:, c], mlp_w.at[0], 6),
        local(w_up.at[:, c], mlp_w.at[2], 7),
        local(w_down.at[:, half_of], down_w.at[0], 8),
    ]

    r = lax.broadcasted_iota(jnp.int32, (kv * group, kv * group), 0)
    col = lax.broadcasted_iota(jnp.int32, (kv * group, kv * group), 1)
    s_of = lax.rem(r, seqs)
    to_chunks = lax.rem(r // seqs, heads_local) * (kv * seqs) + (r // group) * seqs + s_of
    spread = jnp.where(col == to_chunks, 1.0, 0.0).astype(BF16)
    to_heads = lax.rem(r // seqs, kv) * group + (r // (kv * seqs)) * seqs + s_of
    gather = jnp.where(col == to_heads, 1.0, 0.0).astype(BF16)

    lower_in = jax.nn.sigmoid(floor_logits[...])
    for h in range(heads_local):
        floors[pl.ds(h * seqs, seqs), :] = jnp.broadcast_to(lower_in[h : h + 1], (seqs, dk))

    pl.semaphore_wait(barrier, kv)

    tok = remote(tokens, tok_other, pair_send.at[0], pair_recv.at[0], z, other)
    tok.start()
    lane = lax.broadcasted_iota(jnp.int32, (1, tp * feats), 1)
    low = lane < feats
    own = tokens[...].astype(F32)
    own_twice = jnp.concatenate([own, own], axis=1)
    tok.wait_recv()
    got = tok_other[...].astype(F32)
    got_twice = jnp.concatenate([got, got], axis=1)
    mine = lax.broadcasted_iota(jnp.int32, (rows, tp * feats), 1) // feats == c
    block = jnp.where(mine, own_twice, got_twice)
    squares = jnp.sum(block * block, axis=1, keepdims=True)
    sq_out[...] = jnp.broadcast_to(squares, (rows, dk)).reshape(kv, seqs, dk)
    gained = (block * mix_gain[...]).astype(BF16)
    for i in range(4):
        proj_copies[i].wait()
        product = dot(gained, proj_w[i]).astype(BF16)
        stack = jnp.concatenate([product[:, h * dk : (h + 1) * dk] for h in range(heads_local)], axis=0)
        ordered = dot(spread, stack).astype(BF16)
        chunk_out[:, pl.ds(i * group, group), :] = ordered.reshape(kv, group, dk)

    rs, sq = {}, {}
    for d in far_first:
        to = peer(d)
        rs[d] = remote(chunk_out.at[to], chunk_in.at[d], rs_send.at[d], rs_recv.at[d], to, c)
        sq[d] = remote(sq_out.at[to], sq_in.at[d], sq_send.at[d], sq_recv.at[d], to, c)
        sq[d].start()
        rs[d].start()
    swaps = [
        remote(w_out.at[other], out_w.at[1], pair_send.at[1], pair_recv.at[1], z, other),
        remote(w_gate.at[:, other], mlp_w.at[1], pair_send.at[2], pair_recv.at[2], z, other),
        remote(w_up.at[:, other], mlp_w.at[3], pair_send.at[3], pair_recv.at[3], z, other),
        remote(w_down.at[:, half_of_other], down_w.at[1], pair_send.at[4], pair_recv.at[4], z, other),
    ]
    for s in swaps:
        s.start()

    total_sq = sq_out[z]
    total = chunk_out[z].astype(F32)
    for d in near_first:
        sq[d].wait_recv()
        total_sq = total_sq + sq_in[d]
        rs[d].wait_recv()
        total = total + chunk_in[d].astype(F32)

    scale_s = lax.rsqrt(total_sq / width + EPS)
    row_of = lax.broadcasted_iota(jnp.int32, (group, dk), 0)
    scale = jnp.broadcast_to(scale_s[0:1], (group, dk))
    for s in range(1, seqs):
        scale = jnp.where(lax.rem(row_of, seqs) == s, jnp.broadcast_to(scale_s[s : s + 1], (group, dk)), scale)
    query = total[0:group] * scale
    forget_pre = total[group : 2 * group] * scale
    value = total[2 * group : 3 * group] * scale
    gate_pre = total[3 * group : 4 * group] * scale
    lower = floors[...]
    forget = lower + (1.0 - lower) * jax.nn.sigmoid(forget_pre)
    activ = query * jax.nn.sigmoid(query)
    columns = jnp.concatenate([forget, activ, jnp.zeros((dk - 2 * group, dk), F32)], axis=0).T

    state_copy.wait()
    for h in range(heads_local):
        for s in range(seqs):
            i = h * seqs + s
            v_row = value[i : i + 1]
            f_col = columns[:, i : i + 1]
            q_col = columns[:, group + i : group + i + 1]
            new = v_row + f_col * (state[s, h] - v_row)
            state[s, h] = new
            heads[pl.ds(i, 1), :] = jnp.sum(new * q_col, axis=0, keepdims=True)
    state_out = pltpu.make_async_copy(state, new_state, local_sem.at[4])
    state_out.start()

    head_out = heads[...]
    normed = head_out * lax.rsqrt(jnp.mean(head_out * head_out, axis=1, keepdims=True) + EPS)
    mixed = normed * head_gain[...] * (gate_pre * jax.nn.sigmoid(gate_pre))
    mix[z] = mixed.astype(BF16)
    ag = {}
    for d in far_first:
        ag[d] = remote(mix.at[z], mix.at[z], mix_send.at[d], mix_recv.at[d], peer(d), c)
        ag[d].start()
    weight_copies[0].wait()
    swaps[0].wait_recv()
    for d in near_first:
        ag[d].wait_recv()
    by_head = dot(gather, mix[...].reshape(kv * group, dv)).astype(BF16)
    every = jnp.concatenate([by_head[h * rows : (h + 1) * rows] for h in range(heads_local)], axis=1)
    part_out[...] = packed(dot(every, out_w[1]))
    part = remote(part_out, part_in, pair_send.at[5], pair_recv.at[5], z, other)
    part.start()
    kept = packed(dot(every, out_w[0])) + packed(own)
    part.wait_recv()
    middle = (kept + part_in[...]).astype(BF16)
    mid[z] = middle
    am = {}
    for d in far_first:
        am[d] = remote(mid.at[z], mid.at[z], mid_send.at[d], mid_recv.at[d], peer(d), c)
        am[d].start()

    gain = mlp_gain[...]
    gain_swapped = halves_swapped(gain)
    first = c == 0
    gain_low = jnp.where(first, gain, gain_swapped)
    gain_high = jnp.where(first, gain_swapped, gain)
    for w in weight_copies[1:]:
        w.wait()
    for s in swaps[1:]:
        s.wait_recv()
    for d in near_first:
        am[d].wait_recv()
    tops, bottoms = [], []
    squares = jnp.zeros((half_rows, tp * feats), F32)
    for i in range(kv // 2):
        a = mid[2 * i].astype(F32)
        b = mid[2 * i + 1].astype(F32)
        squares = squares + a * a + b * b
        g = jnp.where(low, gain_low[2 * i : 2 * i + 1], gain_high[2 * i + 1 : 2 * i + 2])
        tops.append((jnp.where(low, a, halves_swapped(b)) * g).astype(BF16))
        bottoms.append((jnp.where(low, halves_swapped(a), b) * g).astype(BF16))
    features = jnp.concatenate(
        [jnp.concatenate(tops, axis=1), jnp.concatenate(bottoms, axis=1)], axis=0
    )
    sq_top = jnp.sum(jnp.where(low, squares, 0.0), axis=1, keepdims=True)
    sq_bottom = jnp.sum(jnp.where(low, 0.0, squares), axis=1, keepdims=True)
    sq_mid = jnp.concatenate([sq_top, sq_bottom], axis=0)
    sums = []
    for i in range(4):
        sums.append(dot(features, mlp_w[i].reshape(kv * feats, units)))
        wide_out[i, :, pl.ds(0, units)] = sums[i]
    wide_out[4, :, :] = jnp.broadcast_to(sq_mid, wide_out.shape[1:])
    wide = remote(wide_out, wide_in, pair_send.at[6], pair_recv.at[6], z, other)
    wide.start()
    wide.wait_recv()
    mlp_scale = lax.rsqrt((sq_mid + wide_in[4, :, 0:1]) / width + EPS)
    terms = None
    for i in range(2):
        gate = (sums[i] + wide_in[1 - i, :, pl.ds(0, units)]) * mlp_scale
        upward = (sums[2 + i] + wide_in[3 - i, :, pl.ds(0, units)]) * mlp_scale
        hidden = (gate * jax.nn.sigmoid(gate) * upward).astype(BF16)
        term = dot(hidden, down_w[i])
        terms = term if terms is None else terms + term

    sends = []
    for i in range(half_kv):
        at = slice(i * tp * feats, (i + 1) * tp * feats)
        top, bottom = terms[:half_rows, at], terms[half_rows:, at]
        to = c * half_kv + i
        for to_c, message in (
            (0, jnp.where(low, top, halves_swapped(bottom))),
            (1, jnp.where(low, halves_swapped(top), bottom)),
        ):
            n = 2 * i + to_c
            terms_out[n] = message.astype(BF16)
            copy = remote(terms_out.at[n], terms_in.at[z], term_send.at[n], term_recv.at[z], to, to_c)
            to_self = jnp.logical_and(to == z, to_c == c)
            sends.append((copy, to_self, n))

            @pl.when(jnp.logical_not(to_self))
            def _(copy=copy):
                copy.start()

            @pl.when(to_self)
            def _(n=n):
                terms_in[z] = terms_out[n]

    for i in range(kv):
        from_self = jnp.logical_and(i == z, c == z // half_kv)

        @pl.when(jnp.logical_not(from_self))
        def _(i=i):
            remote(terms_out.at[0], terms_in.at[i], term_send.at[0], term_recv.at[i], z, other).wait_recv()

    summed = middle.astype(F32) + jnp.sum(terms_in[...].astype(F32), axis=0)
    result[pl.ds(0, half_rows), :] = summed[:, :feats].astype(BF16)
    result[pl.ds(half_rows, half_rows), :] = summed[:, feats:].astype(BF16)

    tok.wait_send()
    part.wait_send()
    wide.wait_send()
    for s in swaps:
        s.wait_send()
    for d in near_first:
        rs[d].wait_send()
        sq[d].wait_send()
        ag[d].wait_send()
        am[d].wait_send()
    for copy, to_self, n in sends:

        @pl.when(jnp.logical_not(to_self))
        def _(copy=copy):
            copy.wait_send()

    state_out.wait()


def body(
    kv,
    tp,
    tokens,
    past_state,
    mix_gain,
    w_query,
    w_forget,
    w_value,
    w_gate_out,
    floor_logits,
    head_gain,
    w_out,
    mlp_gain,
    w_gate,
    w_up,
    w_down,
):
    rows, feats = tokens.shape
    seqs, heads_local, dk, dv = past_state.shape
    units = w_gate.shape[1]
    group = heads_local * seqs
    channels = heads_local * dv
    half_cols = w_down.shape[1] // tp
    wide = -(-units // 128) * 128
    in_vmem = pl.BlockSpec(memory_space=pltpu.VMEM)
    anywhere = pl.BlockSpec(memory_space=pl.ANY)
    dma = pltpu.SemaphoreType.DMA
    return pl.pallas_call(
        functools.partial(kernel, kv, tp),
        name="decode_step",
        out_shape=(
            jax.ShapeDtypeStruct((rows, feats), BF16),
            jax.ShapeDtypeStruct(past_state.shape, F32),
        ),
        in_specs=[
            in_vmem,
            anywhere,
            in_vmem,
            anywhere,
            anywhere,
            anywhere,
            anywhere,
            in_vmem,
            in_vmem,
            anywhere,
            in_vmem,
            anywhere,
            anywhere,
            anywhere,
        ],
        out_specs=(in_vmem, anywhere),
        scratch_shapes=[
            pltpu.VMEM((rows, feats), BF16),
            pltpu.VMEM((4, *w_query.shape), BF16),
            pltpu.VMEM(past_state.shape, F32),
            pltpu.VMEM((2, channels, feats), BF16),
            pltpu.VMEM((4, kv, feats, units), BF16),
            pltpu.VMEM((2, units, half_cols), BF16),
            pltpu.VMEM((group, dk), F32),
            pltpu.VMEM((group, dv), F32),
            pltpu.VMEM((kv, 4 * group, dk), BF16),
            pltpu.VMEM((kv, 4 * group, dk), BF16),
            pltpu.VMEM((kv, seqs, dk), F32),
            pltpu.VMEM((kv, seqs, dk), F32),
            pltpu.VMEM((kv, group, dv), BF16),
            pltpu.VMEM((rows // 2, 2 * feats), F32),
            pltpu.VMEM((rows // 2, 2 * feats), F32),
            pltpu.VMEM((kv, rows // 2, 2 * feats), BF16),
            pltpu.VMEM((5, rows, wide), F32),
            pltpu.VMEM((5, rows, wide), F32),
            pltpu.VMEM((kv, rows // 2, 2 * feats), BF16),
            pltpu.VMEM((kv, rows // 2, 2 * feats), BF16),
            dma((9,)),
            dma((7,)),
            dma((7,)),
            dma((kv,)),
            dma((kv,)),
            dma((kv,)),
            dma((kv,)),
            dma((kv,)),
            dma((kv,)),
            dma((kv,)),
            dma((kv,)),
            dma((kv,)),
            dma((kv,)),
        ],
        compiler_params=pltpu.CompilerParams(
            collective_id=0, has_side_effects=True, vmem_limit_bytes=32 * 1024 * 1024
        ),
    )(
        tokens,
        past_state,
        mix_gain.reshape(1, -1),
        w_query,
        w_forget,
        w_value,
        w_gate_out,
        floor_logits.reshape(heads_local, dk),
        head_gain.reshape(1, -1),
        w_out.reshape(tp, channels, feats),
        mlp_gain.reshape(kv, tp * feats),
        w_gate.reshape(kv, tp, feats, units),
        w_up.reshape(kv, tp, feats, units),
        w_down,
    )


def solution(mesh):
    placed = (
        P(("grp", "dp"), ("kv", "tp")),
        P(("grp", "dp", "kv"), "tp", None, None),
        P("kv"),
        P("kv", "tp"),
        P("kv", "tp"),
        P("kv", "tp"),
        P("kv", "tp"),
        P("tp"),
        P(),
        P(None, ("kv", "tp")),
        P(),
        P(None, ("kv", "tp")),
        P(None, ("kv", "tp")),
        P(("kv", "tp"), None),
    )
    return jax.shard_map(
        functools.partial(body, mesh.shape["kv"], mesh.shape["tp"]),
        mesh=mesh,
        in_specs=placed,
        out_specs=(P(("grp", "dp"), ("kv", "tp")), P(("grp", "dp", "kv"), "tp", None, None)),
        check_vma=False,
    )
```

```python
import functools

import jax
import jax.numpy as jnp
from jax import lax
from jax.experimental import pallas as pl
from jax.experimental.pallas import tpu as pltpu
from jax.sharding import PartitionSpec as P

MESH = pl.DeviceIdType.MESH
EPS = 1e-06
F32 = jnp.float32
BF16 = jnp.bfloat16


def dot(a, b):
    return jnp.dot(a, b, preferred_element_type=F32)


def dot_t(a, b):
    return lax.dot_general(a, b, (((1,), (1,)), ((), ())), preferred_element_type=F32)


def packed(x):
    half = x.shape[0] // 2
    return jnp.concatenate([x[:half], x[half:]], axis=1)


def halves_swapped(x):
    return pltpu.roll(x, x.shape[1] // 2, 1)


def kernel(
    kv,
    tp,
    tokens,
    past_state,
    mix_gain,
    w_query,
    w_forget,
    w_value,
    w_gate_out,
    floor_logits,
    head_gain,
    w_out,
    mlp_gain,
    w_gate,
    w_up,
    w_down,
    result,
    new_state,
    tok_other,
    proj_w,
    state,
    out_w,
    mlp_w,
    down_w,
    floors,
    heads,
    chunk_out,
    chunk_in,
    sq_out,
    sq_in,
    mix,
    part_out,
    part_in,
    mid_own,
    mid,
    wide_out,
    wide_in,
    terms_out,
    terms_in,
    local_sem,
    pair_send,
    pair_recv,
    rs_send,
    rs_recv,
    sq_send,
    sq_recv,
    mix_send,
    mix_recv,
    mid_send,
    mid_recv,
    term_send,
    term_recv,
):
    z = lax.axis_index("kv")
    c = lax.axis_index("tp")
    other = 1 - c
    rows, feats = tokens.shape
    seqs, heads_local, dk, dv = past_state.shape
    units = w_gate.shape[0]
    group = heads_local * seqs
    half_rows = rows // 2
    width = kv * tp * feats
    half_kv = kv // tp
    half_cols = half_kv * tp * feats

    def local(src, dst, i):
        copy = pltpu.make_async_copy(src, dst, local_sem.at[i])
        copy.start()
        return copy

    def remote(src, dst, send, recv, to_z, to_c):
        return pltpu.make_async_remote_copy(
            src_ref=src,
            dst_ref=dst,
            send_sem=send,
            recv_sem=recv,
            device_id={"kv": to_z, "tp": to_c},
            device_id_type=MESH,
        )

    def peer(d):
        return lax.rem(z + d, kv)

    far_first = sorted(range(1, kv), key=lambda d: -min(d, kv - d))
    near_first = far_first[::-1]

    barrier = pltpu.get_barrier_semaphore()
    for d in far_first:
        pl.semaphore_signal(barrier, inc=1, device_id={"kv": peer(d), "tp": c}, device_id_type=MESH)
    pl.semaphore_signal(barrier, inc=1, device_id={"kv": z, "tp": other}, device_id_type=MESH)

    proj_copies = [
        local(w, proj_w.at[i], i) for i, w in enumerate((w_query, w_forget, w_value, w_gate_out))
    ]
    state_copy = local(past_state, state, 4)
    half_of = pl.ds(pl.multiple_of(c * half_cols, half_cols), half_cols)
    half_of_other = pl.ds(pl.multiple_of(other * half_cols, half_cols), half_cols)
    weight_copies = [
        local(w_out.at[:, half_of], out_w.at[0], 5),
        local(w_gate.at[:, half_of], mlp_w.at[0], 6),
        local(w_up.at[:, half_of], mlp_w.at[2], 7),
        local(w_down.at[:, half_of], down_w.at[0], 8),
    ]

    r = lax.broadcasted_iota(jnp.int32, (kv * group, kv * group), 0)
    col = lax.broadcasted_iota(jnp.int32, (kv * group, kv * group), 1)
    s_of = lax.rem(r, seqs)
    to_chunks = lax.rem(r // seqs, heads_local) * (kv * seqs) + (r // group) * seqs + s_of
    spread = jnp.where(col == to_chunks, 1.0, 0.0).astype(BF16)
    to_heads = lax.rem(r // seqs, kv) * group + (r // (kv * seqs)) * seqs + s_of
    gather = jnp.where(col == to_heads, 1.0, 0.0).astype(BF16)

    lower_in = jax.nn.sigmoid(floor_logits[...])
    for h in range(heads_local):
        floors[pl.ds(h * seqs, seqs), :] = jnp.broadcast_to(lower_in[h : h + 1], (seqs, dk))

    pl.semaphore_wait(barrier, kv)

    tok = remote(tokens, tok_other, pair_send.at[0], pair_recv.at[0], z, other)
    tok.start()
    lane = lax.broadcasted_iota(jnp.int32, (1, tp * feats), 1)
    low = lane < feats
    own = tokens[...].astype(F32)
    own_twice = jnp.concatenate([own, own], axis=1)
    tok.wait_recv()
    got = tok_other[...].astype(F32)
    got_twice = jnp.concatenate([got, got], axis=1)
    mine = lax.broadcasted_iota(jnp.int32, (rows, tp * feats), 1) // feats == c
    block = jnp.where(mine, own_twice, got_twice)
    squares = jnp.sum(block * block, axis=1, keepdims=True)
    sq_out[...] = jnp.broadcast_to(squares, (rows, dk)).reshape(kv, seqs, dk)
    gained = (block * mix_gain[...]).astype(BF16)
    for i in range(4):
        proj_copies[i].wait()
        product = dot(gained, proj_w[i]).astype(BF16)
        stack = jnp.concatenate([product[:, h * dk : (h + 1) * dk] for h in range(heads_local)], axis=0)
        ordered = dot(spread, stack).astype(BF16)
        chunk_out[:, pl.ds(i * group, group), :] = ordered.reshape(kv, group, dk)

    rs, sq = {}, {}
    for d in far_first:
        to = peer(d)
        rs[d] = remote(chunk_out.at[to], chunk_in.at[d], rs_send.at[d], rs_recv.at[d], to, c)
        sq[d] = remote(sq_out.at[to], sq_in.at[d], sq_send.at[d], sq_recv.at[d], to, c)
        sq[d].start()
        rs[d].start()
    swaps = [
        remote(w_out.at[:, half_of_other], out_w.at[1], pair_send.at[1], pair_recv.at[1], z, other),
        remote(w_gate.at[:, half_of_other], mlp_w.at[1], pair_send.at[2], pair_recv.at[2], z, other),
        remote(w_up.at[:, half_of_other], mlp_w.at[3], pair_send.at[3], pair_recv.at[3], z, other),
        remote(w_down.at[:, half_of_other], down_w.at[1], pair_send.at[4], pair_recv.at[4], z, other),
    ]
    for s in swaps:
        s.start()

    total_sq = sq_out[z]
    total = chunk_out[z].astype(F32)
    for d in near_first:
        sq[d].wait_recv()
        total_sq = total_sq + sq_in[d]
        rs[d].wait_recv()
        total = total + chunk_in[d].astype(F32)

    scale_s = lax.rsqrt(total_sq / width + EPS)
    row_of = lax.broadcasted_iota(jnp.int32, (group, dk), 0)
    scale = jnp.broadcast_to(scale_s[0:1], (group, dk))
    for s in range(1, seqs):
        scale = jnp.where(lax.rem(row_of, seqs) == s, jnp.broadcast_to(scale_s[s : s + 1], (group, dk)), scale)
    query = total[0:group] * scale
    forget_pre = total[group : 2 * group] * scale
    value = total[2 * group : 3 * group] * scale
    gate_pre = total[3 * group : 4 * group] * scale
    lower = floors[...]
    forget = lower + (1.0 - lower) * jax.nn.sigmoid(forget_pre)
    activ = query * jax.nn.sigmoid(query)
    columns = jnp.concatenate([forget, activ, jnp.zeros((dk - 2 * group, dk), F32)], axis=0).T

    state_copy.wait()
    for h in range(heads_local):
        for s in range(seqs):
            i = h * seqs + s
            v_row = value[i : i + 1]
            f_col = columns[:, i : i + 1]
            q_col = columns[:, group + i : group + i + 1]
            new = v_row + f_col * (state[s, h] - v_row)
            state[s, h] = new
            heads[pl.ds(i, 1), :] = jnp.sum(new * q_col, axis=0, keepdims=True)
    state_out = pltpu.make_async_copy(state, new_state, local_sem.at[4])
    state_out.start()

    head_out = heads[...]
    normed = head_out * lax.rsqrt(jnp.mean(head_out * head_out, axis=1, keepdims=True) + EPS)
    mixed = normed * head_gain[...] * (gate_pre * jax.nn.sigmoid(gate_pre))
    mix[z] = mixed.astype(BF16)
    ag = {}
    for d in far_first:
        ag[d] = remote(mix.at[z], mix.at[z], mix_send.at[d], mix_recv.at[d], peer(d), c)
        ag[d].start()
    weight_copies[0].wait()
    swaps[0].wait_recv()
    for d in near_first:
        ag[d].wait_recv()
    by_head = dot(gather, mix[...].reshape(kv * group, dv)).astype(BF16)
    every = jnp.concatenate([by_head[h * rows : (h + 1) * rows] for h in range(heads_local)], axis=1)
    part_out[...] = packed(dot_t(every, out_w[1]))
    part = remote(part_out, part_in, pair_send.at[5], pair_recv.at[5], z, other)
    part.start()
    kept = packed(dot_t(every, out_w[0])) + packed(own)
    part.wait_recv()
    middle = (kept + part_in[...]).astype(BF16)
    mid_own[...] = middle
    half = z // half_kv
    half_z = lax.rem(z, half_kv)
    kept_here = half == c
    am = {}
    for d in far_first:
        am[d] = remote(mid_own, mid.at[half_z, c], mid_send.at[d], mid_recv.at[half_z, c], peer(d), half)
        am[d].start()
    am_pair = remote(mid_own, mid.at[half_z, c], mid_send.at[0], mid_recv.at[half_z, c], z, half)

    @pl.when(kept_here)
    def _():
        mid[half_z, c] = middle

    @pl.when(jnp.logical_not(kept_here))
    def _():
        am_pair.start()

    gain = mlp_gain[pl.ds(pl.multiple_of(c * half_kv, half_kv), half_kv), :]
    for w in weight_copies[1:]:
        w.wait()
    for s in swaps[1:]:
        s.wait_recv()
    for i in range(half_kv):
        for from_c in range(tp):
            from_self = jnp.logical_and(c * half_kv + i == z, c == from_c)

            @pl.when(jnp.logical_not(from_self))
            def _(i=i, from_c=from_c):
                remote(mid_own, mid.at[i, from_c], mid_send.at[0], mid_recv.at[i, from_c], z, other).wait_recv()

    tops, bottoms = [], []
    squares = jnp.zeros((half_rows, tp * feats), F32)
    for i in range(half_kv):
        a = mid[i, 0].astype(F32)
        b = mid[i, 1].astype(F32)
        squares = squares + a * a + b * b
        g = gain[i : i + 1]
        tops.append((jnp.where(low, a, halves_swapped(b)) * g).astype(BF16))
        bottoms.append((jnp.where(low, halves_swapped(a), b) * g).astype(BF16))
    features = jnp.concatenate(
        [jnp.concatenate(tops, axis=1), jnp.concatenate(bottoms, axis=1)], axis=0
    )
    sq_top = jnp.sum(jnp.where(low, squares, 0.0), axis=1, keepdims=True)
    sq_bottom = jnp.sum(jnp.where(low, 0.0, squares), axis=1, keepdims=True)
    sq_mid = jnp.concatenate([sq_top, sq_bottom], axis=0)
    sums = []
    for i in range(4):
        sums.append(dot_t(features, mlp_w[i]))
        wide_out[i, :, pl.ds(0, units)] = sums[i]
    wide_out[4, :, :] = jnp.broadcast_to(sq_mid, wide_out.shape[1:])
    wide = remote(wide_out, wide_in, pair_send.at[6], pair_recv.at[6], z, other)
    wide.start()
    wide.wait_recv()
    mlp_scale = lax.rsqrt((sq_mid + wide_in[4, :, 0:1]) / width + EPS)
    terms = None
    for i in range(2):
        gate = (sums[i] + wide_in[1 - i, :, pl.ds(0, units)]) * mlp_scale
        upward = (sums[2 + i] + wide_in[3 - i, :, pl.ds(0, units)]) * mlp_scale
        hidden = (gate * jax.nn.sigmoid(gate) * upward).astype(BF16)
        term = dot(hidden, down_w[i])
        terms = term if terms is None else terms + term

    sends = []
    for i in range(half_kv):
        at = slice(i * tp * feats, (i + 1) * tp * feats)
        top, bottom = terms[:half_rows, at], terms[half_rows:, at]
        to = c * half_kv + i
        for to_c, message in (
            (0, jnp.where(low, top, halves_swapped(bottom))),
            (1, jnp.where(low, halves_swapped(top), bottom)),
        ):
            n = 2 * i + to_c
            terms_out[n] = message.astype(BF16)
            copy = remote(terms_out.at[n], terms_in.at[z], term_send.at[n], term_recv.at[z], to, to_c)
            to_self = jnp.logical_and(to == z, to_c == c)
            sends.append((copy, to_self, n))

            @pl.when(jnp.logical_not(to_self))
            def _(copy=copy):
                copy.start()

            @pl.when(to_self)
            def _(n=n):
                terms_in[z] = terms_out[n]

    for i in range(kv):
        from_self = jnp.logical_and(i == z, c == z // half_kv)

        @pl.when(jnp.logical_not(from_self))
        def _(i=i):
            remote(terms_out.at[0], terms_in.at[i], term_send.at[0], term_recv.at[i], z, other).wait_recv()

    summed = middle.astype(F32) + jnp.sum(terms_in[...].astype(F32), axis=0)
    result[pl.ds(0, half_rows), :] = summed[:, :feats].astype(BF16)
    result[pl.ds(half_rows, half_rows), :] = summed[:, feats:].astype(BF16)

    tok.wait_send()
    part.wait_send()
    wide.wait_send()
    for s in swaps:
        s.wait_send()
    for d in near_first:
        rs[d].wait_send()
        sq[d].wait_send()
        ag[d].wait_send()
        am[d].wait_send()

    @pl.when(jnp.logical_not(kept_here))
    def _():
        am_pair.wait_send()

    for copy, to_self, n in sends:

        @pl.when(jnp.logical_not(to_self))
        def _(copy=copy):
            copy.wait_send()

    state_out.wait()


def body(
    kv,
    tp,
    tokens,
    past_state,
    mix_gain,
    w_query,
    w_forget,
    w_value,
    w_gate_out,
    floor_logits,
    head_gain,
    w_out,
    mlp_gain,
    w_gate,
    w_up,
    w_down,
):
    rows, feats = tokens.shape
    seqs, heads_local, dk, dv = past_state.shape
    units = w_gate.shape[1]
    group = heads_local * seqs
    channels = heads_local * dv
    half_cols = w_down.shape[1] // tp
    wide = -(-units // 128) * 128
    in_vmem = pl.BlockSpec(memory_space=pltpu.VMEM)
    anywhere = pl.BlockSpec(memory_space=pl.ANY)
    dma = pltpu.SemaphoreType.DMA
    return pl.pallas_call(
        functools.partial(kernel, kv, tp),
        name="decode_step",
        out_shape=(
            jax.ShapeDtypeStruct((rows, feats), BF16),
            jax.ShapeDtypeStruct(past_state.shape, F32),
        ),
        in_specs=[
            in_vmem,
            anywhere,
            in_vmem,
            anywhere,
            anywhere,
            anywhere,
            anywhere,
            in_vmem,
            in_vmem,
            anywhere,
            in_vmem,
            anywhere,
            anywhere,
            anywhere,
        ],
        out_specs=(in_vmem, anywhere),
        scratch_shapes=[
            pltpu.VMEM((rows, feats), BF16),
            pltpu.VMEM((4, *w_query.shape), BF16),
            pltpu.VMEM(past_state.shape, F32),
            pltpu.VMEM((2, feats, channels), BF16),
            pltpu.VMEM((4, units, half_cols), BF16),
            pltpu.VMEM((2, units, half_cols), BF16),
            pltpu.VMEM((group, dk), F32),
            pltpu.VMEM((group, dv), F32),
            pltpu.VMEM((kv, 4 * group, dk), BF16),
            pltpu.VMEM((kv, 4 * group, dk), BF16),
            pltpu.VMEM((kv, seqs, dk), F32),
            pltpu.VMEM((kv, seqs, dk), F32),
            pltpu.VMEM((kv, group, dv), BF16),
            pltpu.VMEM((rows // 2, 2 * feats), F32),
            pltpu.VMEM((rows // 2, 2 * feats), F32),
            pltpu.VMEM((rows // 2, 2 * feats), BF16),
            pltpu.VMEM((kv // tp, tp, rows // 2, 2 * feats), BF16),
            pltpu.VMEM((5, rows, wide), F32),
            pltpu.VMEM((5, rows, wide), F32),
            pltpu.VMEM((kv, rows // 2, 2 * feats), BF16),
            pltpu.VMEM((kv, rows // 2, 2 * feats), BF16),
            dma((9,)),
            dma((7,)),
            dma((7,)),
            dma((kv,)),
            dma((kv,)),
            dma((kv,)),
            dma((kv,)),
            dma((kv,)),
            dma((kv,)),
            dma((kv,)),
            dma((kv // tp, tp)),
            dma((kv,)),
            dma((kv,)),
        ],
        compiler_params=pltpu.CompilerParams(
            collective_id=0, has_side_effects=True, vmem_limit_bytes=67043328
        ),
    )(
        tokens,
        past_state,
        mix_gain.reshape(1, -1),
        w_query,
        w_forget,
        w_value,
        w_gate_out,
        floor_logits.reshape(heads_local, dk),
        head_gain.reshape(1, -1),
        w_out.T,
        mlp_gain.reshape(kv, tp * feats),
        w_gate.T,
        w_up.T,
        w_down,
    )


def solution(mesh):
    placed = (
        P(("grp", "dp"), ("kv", "tp")),
        P(("grp", "dp", "kv"), "tp", None, None),
        P("kv"),
        P("kv", "tp"),
        P("kv", "tp"),
        P("kv", "tp"),
        P("kv", "tp"),
        P("tp"),
        P(),
        P(None, ("kv", "tp")),
        P(),
        P(None, ("kv", "tp")),
        P(None, ("kv", "tp")),
        P(("kv", "tp"), None),
    )
    return jax.shard_map(
        functools.partial(body, mesh.shape["kv"], mesh.shape["tp"]),
        mesh=mesh,
        in_specs=placed,
        out_specs=(P(("grp", "dp"), ("kv", "tp")), P(("grp", "dp", "kv"), "tp", None, None)),
        check_vma=False,
    )
```

```python
import functools

import jax
import jax.numpy as jnp
from jax import lax
from jax.experimental import pallas as pl
from jax.experimental.pallas import tpu as pltpu
from jax.sharding import PartitionSpec as P

MESH = pl.DeviceIdType.MESH
EPS = 1e-06
VMEM_BYTES = 65_600_000
F32 = jnp.float32
BF16 = jnp.bfloat16


def dot(a, b):
    return jnp.dot(a, b, preferred_element_type=F32)


def dot_t(a, b):
    return lax.dot_general(a, b, (((1,), (1,)), ((), ())), preferred_element_type=F32)


def packed(x):
    half = x.shape[0] // 2
    return jnp.concatenate([x[:half], x[half:]], axis=1)


def halves_swapped(x):
    return pltpu.roll(x, x.shape[1] // 2, 1)


def kernel(
    kv,
    tp,
    tokens_hbm,
    past_state,
    mix_gain_hbm,
    w_query,
    w_forget,
    w_value,
    w_gate_out,
    floor_hbm,
    head_gain_hbm,
    w_out,
    mlp_gain_hbm,
    w_gate,
    w_up,
    w_down,
    result,
    forget_out,
    value_out,
    tokens,
    mix_gain,
    floor_logits,
    head_gain,
    mlp_gain,
    tok_other,
    proj_w,
    state,
    out_w,
    mlp_w,
    down_w,
    floors,
    heads,
    chunk_out,
    chunk_in,
    sq_out,
    sq_in,
    mix,
    part_out,
    part_in,
    mid_own,
    mid,
    wide_out,
    wide_in,
    terms_out,
    terms_in,
    local_sem,
    pair_send,
    pair_recv,
    rs_send,
    rs_recv,
    sq_send,
    sq_recv,
    mix_send,
    mix_recv,
    mid_send,
    mid_recv,
    term_send,
    term_recv,
    pair_in,
    ready,
):
    z = lax.axis_index("kv")
    c = lax.axis_index("tp")
    other = 1 - c
    rows, feats = tokens.shape
    seqs, heads_local, dk, dv = past_state.shape
    units = w_gate.shape[0]
    group = heads_local * seqs
    half_rows = rows // 2
    width = kv * tp * feats
    half_kv = kv // tp
    half_cols = half_kv * tp * feats

    def local(src, dst, i):
        copy = pltpu.make_async_copy(src, dst, local_sem.at[i])
        copy.start()
        return copy

    def remote(src, dst, send, recv, to_z, to_c):
        return pltpu.make_async_remote_copy(
            src_ref=src,
            dst_ref=dst,
            send_sem=send,
            recv_sem=recv,
            device_id={"kv": to_z, "tp": to_c},
            device_id_type=MESH,
        )

    def peer(d):
        return lax.rem(z + d, kv)

    def place(w):
        return lax.rem(w + kv - 1, kv)

    order = [*range(1, kv), 0]
    far_first = sorted(range(1, kv), key=lambda d: -min(d, kv - d))
    near_first = far_first[::-1]

    barrier = pltpu.get_barrier_semaphore()

    def signal(sem, to_z, to_c):
        pl.semaphore_signal(sem, inc=1, device_id={"kv": to_z, "tp": to_c}, device_id_type=MESH)

    @pl.when(c == 1)
    def _():
        signal(barrier, z, 0)

    tokens_copy = local(tokens_hbm, tokens, 9)
    gain_copy = local(mix_gain_hbm, mix_gain, 10)
    proj_copies = [
        local(w, proj_w.at[i], i) for i, w in enumerate((w_query, w_forget, w_value, w_gate_out))
    ]
    state_copy = local(past_state, state, 4)
    small_copies = [
        local(floor_hbm, floor_logits, 11),
        local(head_gain_hbm, head_gain, 12),
        local(mlp_gain_hbm, mlp_gain, 13),
    ]
    half_of = pl.ds(pl.multiple_of(c * half_cols, half_cols), half_cols)
    half_of_other = pl.ds(pl.multiple_of(other * half_cols, half_cols), half_cols)
    weight_copies = [
        local(w_out.at[:, half_of], out_w.at[0], 5),
        local(w_gate.at[:, half_of], mlp_w.at[0], 6),
        local(w_up.at[:, half_of], mlp_w.at[2], 7),
        local(w_down.at[:, half_of], down_w.at[0], 8),
    ]

    @pl.when(c == 0)
    def _():
        pl.semaphore_wait(barrier, 1)
        signal(pair_in, z, 1)

    @pl.when(c == 1)
    def _():
        pl.semaphore_wait(pair_in, 1)
        for w in order:

            @pl.when(place(z) < place(w))
            def _(w=w):
                signal(barrier, w, 1)

    tokens_copy.wait()
    tok = remote(tokens, tok_other, pair_send.at[0], pair_recv.at[0], z, other)
    tok.start()

    @pl.when(c == 1)
    def _():
        @pl.when(place(z) > 0)
        def _():
            pl.semaphore_wait(barrier, place(z))

        signal(pair_in, z, 0)

    @pl.when(c == 0)
    def _():
        pl.semaphore_wait(pair_in, 1)

    for d in far_first:
        to = peer(d)

        @pl.when(place(to) < place(z))
        def _(to=to):
            signal(ready.at[z], to, c)

    r = lax.broadcasted_iota(jnp.int32, (kv * group, kv * group), 0)
    col = lax.broadcasted_iota(jnp.int32, (kv * group, kv * group), 1)
    s_of = lax.rem(r, seqs)
    to_chunks = lax.rem(r // seqs, heads_local) * (kv * seqs) + (r // group) * seqs + s_of
    spread = jnp.where(col == to_chunks, 1.0, 0.0).astype(BF16)
    to_heads = lax.rem(r // seqs, kv) * group + (r // (kv * seqs)) * seqs + s_of
    gather = jnp.where(col == to_heads, 1.0, 0.0).astype(BF16)

    lane = lax.broadcasted_iota(jnp.int32, (1, tp * feats), 1)
    low = lane < feats
    own = tokens[...].astype(F32)
    own_twice = jnp.concatenate([own, own], axis=1)
    tok.wait_recv()
    got = tok_other[...].astype(F32)
    got_twice = jnp.concatenate([got, got], axis=1)
    mine = lax.broadcasted_iota(jnp.int32, (rows, tp * feats), 1) // feats == c
    block = jnp.where(mine, own_twice, got_twice)
    squares = jnp.sum(block * block, axis=1, keepdims=True)
    sq_out[...] = jnp.broadcast_to(squares, (rows, dk)).reshape(kv, seqs, dk)
    gain_copy.wait()
    gained = (block * mix_gain[...]).astype(BF16)
    for i in range(4):
        proj_copies[i].wait()
        product = dot(gained, proj_w[i]).astype(BF16)
        stack = jnp.concatenate([product[:, h * dk : (h + 1) * dk] for h in range(heads_local)], axis=0)
        ordered = dot(spread, stack).astype(BF16)
        chunk_out[:, pl.ds(i * group, group), :] = ordered.reshape(kv, group, dk)

    def send_chunk(to, start):
        for copy in (
            remote(sq_out.at[to], sq_in.at[z], sq_send.at[to], sq_recv.at[z], to, c),
            remote(chunk_out.at[to], chunk_in.at[z], rs_send.at[to], rs_recv.at[z], to, c),
        ):
            copy.start() if start else copy.wait_send()

    for d in far_first:
        to = peer(d)

        @pl.when(place(to) < place(z))
        def _(to=to):
            send_chunk(to, True)

    swaps = [
        remote(w_out.at[:, half_of_other], out_w.at[1], pair_send.at[1], pair_recv.at[1], z, other),
        remote(w_gate.at[:, half_of_other], mlp_w.at[1], pair_send.at[2], pair_recv.at[2], z, other),
        remote(w_up.at[:, half_of_other], mlp_w.at[3], pair_send.at[3], pair_recv.at[3], z, other),
        remote(w_down.at[:, half_of_other], down_w.at[1], pair_send.at[4], pair_recv.at[4], z, other),
    ]
    for s in swaps:
        s.start()

    sq_in[z] = sq_out[z]
    chunk_in[z] = chunk_out[z]
    for copy in small_copies:
        copy.wait()
    lower_in = jax.nn.sigmoid(floor_logits[...])
    for h in range(heads_local):
        floors[pl.ds(h * seqs, seqs), :] = jnp.broadcast_to(lower_in[h : h + 1], (seqs, dk))

    for w in order:

        @pl.when(place(z) < place(w))
        def _(w=w):
            pl.semaphore_wait(ready.at[w], 1)
            send_chunk(w, True)

    total_sq = jnp.zeros((seqs, dk), F32)
    total = jnp.zeros((4 * group, dk), F32)
    for w in order:

        @pl.when(z != w)
        def _(w=w):
            remote(sq_out.at[w], sq_in.at[w], sq_send.at[w], sq_recv.at[w], w, c).wait_recv()
            remote(chunk_out.at[w], chunk_in.at[w], rs_send.at[w], rs_recv.at[w], w, c).wait_recv()

        total_sq = total_sq + sq_in[w]
        total = total + chunk_in[w].astype(F32)

    scale_s = lax.rsqrt(total_sq / width + EPS)
    row_of = lax.broadcasted_iota(jnp.int32, (group, dk), 0)
    scale = jnp.broadcast_to(scale_s[0:1], (group, dk))
    for s in range(1, seqs):
        scale = jnp.where(lax.rem(row_of, seqs) == s, jnp.broadcast_to(scale_s[s : s + 1], (group, dk)), scale)
    query = total[0:group] * scale
    forget_pre = total[group : 2 * group] * scale
    value = total[2 * group : 3 * group] * scale
    gate_pre = total[3 * group : 4 * group] * scale
    lower = floors[...]
    forget = lower + (1.0 - lower) * jax.nn.sigmoid(forget_pre)
    activ = query * jax.nn.sigmoid(query)
    columns = jnp.concatenate([forget, activ, jnp.zeros((dk - 2 * group, dk), F32)], axis=0).T

    state_copy.wait()
    for h in range(heads_local):
        for s in range(seqs):
            i = h * seqs + s
            v_row = value[i : i + 1]
            f_col = columns[:, i : i + 1]
            q_col = columns[:, group + i : group + i + 1]
            new = v_row + f_col * (state[s, h] - v_row)
            heads[pl.ds(i, 1), :] = jnp.sum(new * q_col, axis=0, keepdims=True)

    head_out = heads[...]
    normed = head_out * lax.rsqrt(jnp.mean(head_out * head_out, axis=1, keepdims=True) + EPS)
    mixed = normed * head_gain[...] * (gate_pre * jax.nn.sigmoid(gate_pre))
    mix[z] = mixed.astype(BF16)
    ag = {}
    for d in far_first:
        ag[d] = remote(mix.at[z], mix.at[z], mix_send.at[d], mix_recv.at[d], peer(d), c)
        ag[d].start()
    for h in range(heads_local):
        for s in range(seqs):
            i = h * seqs + s
            forget_out[s, pl.ds(h, 1), :] = forget[i : i + 1]
            value_out[s, pl.ds(h, 1), :] = value[i : i + 1]
    weight_copies[0].wait()
    swaps[0].wait_recv()
    for d in near_first:
        ag[d].wait_recv()
    by_head = dot(gather, mix[...].reshape(kv * group, dv)).astype(BF16)
    every = jnp.concatenate([by_head[h * rows : (h + 1) * rows] for h in range(heads_local)], axis=1)
    part_out[...] = packed(dot_t(every, out_w[1]))
    part = remote(part_out, part_in, pair_send.at[5], pair_recv.at[5], z, other)
    part.start()
    kept = packed(dot_t(every, out_w[0])) + packed(own)
    part.wait_recv()
    middle = (kept + part_in[...]).astype(BF16)
    mid_own[...] = middle
    half = z // half_kv
    half_z = lax.rem(z, half_kv)
    kept_here = half == c
    am = {}
    for d in far_first:
        am[d] = remote(mid_own, mid.at[half_z, c], mid_send.at[d], mid_recv.at[half_z, c], peer(d), half)
        am[d].start()
    am_pair = remote(mid_own, mid.at[half_z, c], mid_send.at[0], mid_recv.at[half_z, c], z, half)

    @pl.when(kept_here)
    def _():
        mid[half_z, c] = middle

    @pl.when(jnp.logical_not(kept_here))
    def _():
        am_pair.start()

    gain = mlp_gain[pl.ds(pl.multiple_of(c * half_kv, half_kv), half_kv), :]
    for w in weight_copies[1:]:
        w.wait()
    for s in swaps[1:]:
        s.wait_recv()
    for i in range(half_kv):
        for from_c in range(tp):
            from_self = jnp.logical_and(c * half_kv + i == z, c == from_c)

            @pl.when(jnp.logical_not(from_self))
            def _(i=i, from_c=from_c):
                remote(mid_own, mid.at[i, from_c], mid_send.at[0], mid_recv.at[i, from_c], z, other).wait_recv()

    tops, bottoms = [], []
    squares = jnp.zeros((half_rows, tp * feats), F32)
    for i in range(half_kv):
        a = mid[i, 0].astype(F32)
        b = mid[i, 1].astype(F32)
        squares = squares + a * a + b * b
        g = gain[i : i + 1]
        tops.append((jnp.where(low, a, halves_swapped(b)) * g).astype(BF16))
        bottoms.append((jnp.where(low, halves_swapped(a), b) * g).astype(BF16))
    features = jnp.concatenate(
        [jnp.concatenate(tops, axis=1), jnp.concatenate(bottoms, axis=1)], axis=0
    )
    sq_top = jnp.sum(jnp.where(low, squares, 0.0), axis=1, keepdims=True)
    sq_bottom = jnp.sum(jnp.where(low, 0.0, squares), axis=1, keepdims=True)
    sq_mid = jnp.concatenate([sq_top, sq_bottom], axis=0)
    sums = []
    for i in range(4):
        sums.append(dot_t(features, mlp_w[i]))
        wide_out[i, :, pl.ds(0, units)] = sums[i]
    wide_out[4, :, :] = jnp.broadcast_to(sq_mid, wide_out.shape[1:])
    wide = remote(wide_out, wide_in, pair_send.at[6], pair_recv.at[6], z, other)
    wide.start()
    wide.wait_recv()
    mlp_scale = lax.rsqrt((sq_mid + wide_in[4, :, 0:1]) / width + EPS)
    terms = None
    for i in range(2):
        gate = (sums[i] + wide_in[1 - i, :, pl.ds(0, units)]) * mlp_scale
        upward = (sums[2 + i] + wide_in[3 - i, :, pl.ds(0, units)]) * mlp_scale
        hidden = (gate * jax.nn.sigmoid(gate) * upward).astype(BF16)
        term = dot(hidden, down_w[i])
        terms = term if terms is None else terms + term

    sends = []
    for i in range(half_kv):
        at = slice(i * tp * feats, (i + 1) * tp * feats)
        top, bottom = terms[:half_rows, at], terms[half_rows:, at]
        to = c * half_kv + i
        for to_c, message in (
            (0, jnp.where(low, top, halves_swapped(bottom))),
            (1, jnp.where(low, halves_swapped(top), bottom)),
        ):
            n = 2 * i + to_c
            terms_out[n] = message.astype(BF16)
            copy = remote(terms_out.at[n], terms_in.at[z], term_send.at[n], term_recv.at[z], to, to_c)
            to_self = jnp.logical_and(to == z, to_c == c)
            sends.append((copy, to_self, n))

            @pl.when(jnp.logical_not(to_self))
            def _(copy=copy):
                copy.start()

            @pl.when(to_self)
            def _(n=n):
                terms_in[z] = terms_out[n]

    for i in range(kv):
        from_self = jnp.logical_and(i == z, c == z // half_kv)

        @pl.when(jnp.logical_not(from_self))
        def _(i=i):
            remote(terms_out.at[0], terms_in.at[i], term_send.at[0], term_recv.at[i], z, other).wait_recv()

    summed = middle.astype(F32) + jnp.sum(terms_in[...].astype(F32), axis=0)
    result[pl.ds(0, half_rows), :] = summed[:, :feats].astype(BF16)
    result[pl.ds(half_rows, half_rows), :] = summed[:, feats:].astype(BF16)

    tok.wait_send()
    part.wait_send()
    wide.wait_send()
    for s in swaps:
        s.wait_send()
    for d in near_first:
        send_chunk(peer(d), False)
        ag[d].wait_send()
        am[d].wait_send()

    @pl.when(jnp.logical_not(kept_here))
    def _():
        am_pair.wait_send()

    for copy, to_self, n in sends:

        @pl.when(jnp.logical_not(to_self))
        def _(copy=copy):
            copy.wait_send()


def body(
    kv,
    tp,
    tokens,
    past_state,
    mix_gain,
    w_query,
    w_forget,
    w_value,
    w_gate_out,
    floor_logits,
    head_gain,
    w_out,
    mlp_gain,
    w_gate,
    w_up,
    w_down,
):
    rows, feats = tokens.shape
    seqs, heads_local, dk, dv = past_state.shape
    units = w_gate.shape[1]
    group = heads_local * seqs
    channels = heads_local * dv
    half_cols = w_down.shape[1] // tp
    wide = -(-units // 128) * 128
    in_vmem = pl.BlockSpec(memory_space=pltpu.VMEM)
    dma = pltpu.SemaphoreType.DMA
    result, forget, value = pl.pallas_call(
        functools.partial(kernel, kv, tp),
        name="decode_step",
        out_shape=(
            jax.ShapeDtypeStruct((rows, feats), BF16),
            jax.ShapeDtypeStruct((seqs, heads_local, dk), F32),
            jax.ShapeDtypeStruct((seqs, heads_local, dv), F32),
        ),
        in_specs=[pl.BlockSpec(memory_space=pltpu.HBM)] * 14,
        out_specs=(in_vmem, in_vmem, in_vmem),
        scratch_shapes=[
            pltpu.VMEM((rows, feats), BF16),
            pltpu.VMEM((1, tp * feats), F32),
            pltpu.VMEM((heads_local, dk), F32),
            pltpu.VMEM((1, dv), F32),
            pltpu.VMEM((kv, tp * feats), F32),
            pltpu.VMEM((rows, feats), BF16),
            pltpu.VMEM((4, *w_query.shape), BF16),
            pltpu.VMEM(past_state.shape, F32),
            pltpu.VMEM((2, feats, channels), BF16),
            pltpu.VMEM((4, units, half_cols), BF16),
            pltpu.VMEM((2, units, half_cols), BF16),
            pltpu.VMEM((group, dk), F32),
            pltpu.VMEM((group, dv), F32),
            pltpu.VMEM((kv, 4 * group, dk), BF16),
            pltpu.VMEM((kv, 4 * group, dk), BF16),
            pltpu.VMEM((kv, seqs, dk), F32),
            pltpu.VMEM((kv, seqs, dk), F32),
            pltpu.VMEM((kv, group, dv), BF16),
            pltpu.VMEM((rows // 2, 2 * feats), F32),
            pltpu.VMEM((rows // 2, 2 * feats), F32),
            pltpu.VMEM((rows // 2, 2 * feats), BF16),
            pltpu.VMEM((kv // tp, tp, rows // 2, 2 * feats), BF16),
            pltpu.VMEM((5, rows, wide), F32),
            pltpu.VMEM((5, rows, wide), F32),
            pltpu.VMEM((kv, rows // 2, 2 * feats), BF16),
            pltpu.VMEM((kv, rows // 2, 2 * feats), BF16),
            dma((14,)),
            dma((7,)),
            dma((7,)),
            dma((kv,)),
            dma((kv,)),
            dma((kv,)),
            dma((kv,)),
            dma((kv,)),
            dma((kv,)),
            dma((kv,)),
            dma((kv // tp, tp)),
            dma((kv,)),
            dma((kv,)),
            pltpu.SemaphoreType.REGULAR,
            pltpu.SemaphoreType.REGULAR((kv,)),
        ],
        compiler_params=pltpu.CompilerParams(
            collective_id=0, has_side_effects=True, vmem_limit_bytes=VMEM_BYTES
        ),
    )(
        tokens,
        past_state,
        mix_gain.reshape(1, -1),
        w_query,
        w_forget,
        w_value,
        w_gate_out,
        floor_logits.reshape(heads_local, dk),
        head_gain.reshape(1, -1),
        w_out.T,
        mlp_gain.reshape(kv, tp * feats),
        w_gate.T,
        w_up.T,
        w_down,
    )
    value = value[:, :, None, :]
    return result, value + forget[..., None] * (past_state - value)


def solution(mesh):
    placed = (
        P(("grp", "dp"), ("kv", "tp")),
        P(("grp", "dp", "kv"), "tp", None, None),
        P("kv"),
        P("kv", "tp"),
        P("kv", "tp"),
        P("kv", "tp"),
        P("kv", "tp"),
        P("tp"),
        P(),
        P(None, ("kv", "tp")),
        P(),
        P(None, ("kv", "tp")),
        P(None, ("kv", "tp")),
        P(("kv", "tp"), None),
    )
    return jax.shard_map(
        functools.partial(body, mesh.shape["kv"], mesh.shape["tp"]),
        mesh=mesh,
        in_specs=placed,
        out_specs=(P(("grp", "dp"), ("kv", "tp")), P(("grp", "dp", "kv"), "tp", None, None)),
        check_vma=False,
    )
```

```python
import functools

import jax
import jax.numpy as jnp
from jax import lax
from jax.experimental import pallas as pl
from jax.experimental.pallas import tpu as pltpu
from jax.sharding import PartitionSpec as P

MESH = pl.DeviceIdType.MESH
EPS = 1e-06
VMEM_BYTES = 48 * 1024 * 1024
F32 = jnp.float32
BF16 = jnp.bfloat16


def dot(a, b):
    return jnp.dot(a, b, preferred_element_type=F32)


def dot_t(a, b):
    return lax.dot_general(a, b, (((1,), (1,)), ((), ())), preferred_element_type=F32)


def hbm(*arrays):
    return [pltpu.with_memory_space_constraint(a, pltpu.HBM) for a in arrays]


def packed(x):
    half = x.shape[0] // 2
    return jnp.concatenate([x[:half], x[half:]], axis=1)


def halves_swapped(x):
    return pltpu.roll(x, x.shape[1] // 2, 1)


def kernel(
    kv,
    tp,
    tokens_hbm,
    past_state,
    mix_gain_hbm,
    w_query,
    w_forget,
    w_value,
    w_gate_out,
    floor_hbm,
    head_gain_hbm,
    w_out,
    mlp_gain_hbm,
    w_gate,
    w_up,
    w_down,
    result,
    forget_out,
    value_out,
    tokens,
    mix_gain,
    floor_logits,
    head_gain,
    mlp_gain,
    tok_other,
    proj_w,
    state,
    out_w,
    mlp_w,
    down_w,
    floors,
    heads,
    chunk_out,
    chunk_in,
    sq_out,
    sq_in,
    mix,
    part_out,
    part_in,
    mid_own,
    mid,
    wide_out,
    wide_in,
    terms_out,
    terms_in,
    local_sem,
    pair_send,
    pair_recv,
    rs_send,
    rs_recv,
    sq_send,
    sq_recv,
    mix_send,
    mix_recv,
    mid_send,
    mid_recv,
    term_send,
    term_recv,
    pair_in,
    ready,
):
    z = lax.axis_index("kv")
    c = lax.axis_index("tp")
    other = 1 - c
    rows, feats = tokens.shape
    seqs, heads_local, dk, dv = past_state.shape
    units = w_gate.shape[0]
    group = heads_local * seqs
    half_rows = rows // 2
    width = kv * tp * feats
    half_kv = kv // tp
    half_cols = half_kv * tp * feats

    def local(src, dst, i):
        copy = pltpu.make_async_copy(src, dst, local_sem.at[i])
        copy.start()
        return copy

    def remote(src, dst, send, recv, to_z, to_c):
        return pltpu.make_async_remote_copy(
            src_ref=src,
            dst_ref=dst,
            send_sem=send,
            recv_sem=recv,
            device_id={"kv": to_z, "tp": to_c},
            device_id_type=MESH,
        )

    def peer(d):
        return lax.rem(z + d, kv)

    def place(w):
        return jnp.where(w == 0, kv - 2, jnp.where(w == kv - 1, kv - 1, w - 1))

    order = [*range(1, kv - 1), 0, kv - 1]
    far_first = sorted(range(1, kv), key=lambda d: -min(d, kv - d))
    near_first = far_first[::-1]

    barrier = pltpu.get_barrier_semaphore()

    def signal(sem, to_z, to_c):
        pl.semaphore_signal(sem, inc=1, device_id={"kv": to_z, "tp": to_c}, device_id_type=MESH)

    @pl.when(c == 1)
    def _():
        signal(barrier, z, 0)

    tokens_copy = local(tokens_hbm, tokens, 9)
    gain_copy = local(mix_gain_hbm, mix_gain, 10)
    proj_copies = [
        local(w, proj_w.at[i], i) for i, w in enumerate((w_query, w_forget, w_value, w_gate_out))
    ]
    state_copy = local(past_state, state, 4)
    small_copies = [
        local(floor_hbm, floor_logits, 11),
        local(head_gain_hbm, head_gain, 12),
        local(mlp_gain_hbm, mlp_gain, 13),
    ]
    half_of = pl.ds(pl.multiple_of(c * half_cols, half_cols), half_cols)
    half_of_other = pl.ds(pl.multiple_of(other * half_cols, half_cols), half_cols)
    weight_copies = [
        local(w_out.at[:, half_of], out_w.at[0], 5),
        local(w_gate.at[:, half_of], mlp_w.at[0], 6),
        local(w_up.at[:, half_of], mlp_w.at[2], 7),
        local(w_down.at[:, half_of], down_w.at[0], 8),
    ]

    @pl.when(c == 0)
    def _():
        pl.semaphore_wait(barrier, 1)
        signal(pair_in, z, 1)

    @pl.when(c == 1)
    def _():
        pl.semaphore_wait(pair_in, 1)
        for w in order:

            @pl.when(place(z) < place(w))
            def _(w=w):
                signal(barrier, w, 1)

    @pl.when(c == 1)
    def _():
        @pl.when(place(z) > 0)
        def _():
            pl.semaphore_wait(barrier, place(z))

        signal(pair_in, z, 0)

    @pl.when(c == 0)
    def _():
        pl.semaphore_wait(pair_in, 1)

    for d in far_first:
        to = peer(d)

        @pl.when(place(to) < place(z))
        def _(to=to):
            signal(ready.at[z], to, c)

    tokens_copy.wait()
    tok = remote(tokens, tok_other, pair_send.at[0], pair_recv.at[0], z, other)
    tok.start()

    r = lax.broadcasted_iota(jnp.int32, (kv * group, kv * group), 0)
    col = lax.broadcasted_iota(jnp.int32, (kv * group, kv * group), 1)
    s_of = lax.rem(r, seqs)
    to_chunks = lax.rem(r // seqs, heads_local) * (kv * seqs) + (r // group) * seqs + s_of
    spread = jnp.where(col == to_chunks, 1.0, 0.0).astype(BF16)
    to_heads = lax.rem(r // seqs, kv) * group + (r // (kv * seqs)) * seqs + s_of
    gather = jnp.where(col == to_heads, 1.0, 0.0).astype(BF16)

    lane = lax.broadcasted_iota(jnp.int32, (1, tp * feats), 1)
    low = lane < feats
    own = tokens[...].astype(F32)
    own_twice = jnp.concatenate([own, own], axis=1)
    tok.wait_recv()
    got = tok_other[...].astype(F32)
    got_twice = jnp.concatenate([got, got], axis=1)
    mine = lax.broadcasted_iota(jnp.int32, (rows, tp * feats), 1) // feats == c
    block = jnp.where(mine, own_twice, got_twice)
    squares = jnp.sum(block * block, axis=1, keepdims=True)
    sq_out[...] = jnp.broadcast_to(squares, (rows, dk)).reshape(kv, seqs, dk)
    gain_copy.wait()
    gained = (block * mix_gain[...]).astype(BF16)
    def sq_copy(to):
        return remote(sq_out.at[to], sq_in.at[z], sq_send.at[to], sq_recv.at[z], to, c)

    def chunk_copy(to):
        return remote(chunk_out.at[to], chunk_in.at[z], rs_send.at[to], rs_recv.at[z], to, c)

    for d in far_first:
        to = peer(d)

        @pl.when(place(to) < place(z))
        def _(to=to):
            sq_copy(to).start()

    for copy in proj_copies:
        copy.wait()
    products = [dot(gained, proj_w[i]).astype(BF16) for i in range(4)]
    for i in (0, 2):
        stack = jnp.concatenate(
            [
                jnp.concatenate([p[:, h * dk : (h + 1) * dk] for p in products[i : i + 2]], axis=1)
                for h in range(heads_local)
            ],
            axis=0,
        )
        ordered = dot(spread, stack).astype(BF16)
        for j in range(2):
            chunk_out[:, pl.ds((i + j) * group, group), :] = ordered[:, j * dk : (j + 1) * dk].reshape(
                kv, group, dk
            )

    for d in far_first:
        to = peer(d)

        @pl.when(place(to) < place(z))
        def _(to=to):
            chunk_copy(to).start()

    swaps = [
        remote(w_out.at[:, half_of_other], out_w.at[1], pair_send.at[1], pair_recv.at[1], z, other),
        remote(w_gate.at[:, half_of_other], mlp_w.at[1], pair_send.at[2], pair_recv.at[2], z, other),
        remote(w_up.at[:, half_of_other], mlp_w.at[3], pair_send.at[3], pair_recv.at[3], z, other),
        remote(w_down.at[:, half_of_other], down_w.at[1], pair_send.at[4], pair_recv.at[4], z, other),
    ]
    for s in swaps:
        s.start()

    sq_in[z] = sq_out[z]
    chunk_in[z] = chunk_out[z]
    for copy in small_copies:
        copy.wait()
    lower_in = jax.nn.sigmoid(floor_logits[...])
    for h in range(heads_local):
        floors[pl.ds(h * seqs, seqs), :] = jnp.broadcast_to(lower_in[h : h + 1], (seqs, dk))

    for w in order:

        @pl.when(place(z) < place(w))
        def _(w=w):
            pl.semaphore_wait(ready.at[w], 1)
            sq_copy(w).start()
            chunk_copy(w).start()

    total_sq = jnp.zeros((seqs, dk), F32)
    total = jnp.zeros((4 * group, dk), F32)
    for w in order:

        @pl.when(z != w)
        def _(w=w):
            remote(sq_out.at[w], sq_in.at[w], sq_send.at[w], sq_recv.at[w], w, c).wait_recv()
            remote(chunk_out.at[w], chunk_in.at[w], rs_send.at[w], rs_recv.at[w], w, c).wait_recv()

        total_sq = total_sq + sq_in[w]
        total = total + chunk_in[w].astype(F32)

    scale_s = lax.rsqrt(total_sq / width + EPS)
    row_of = lax.broadcasted_iota(jnp.int32, (group, dk), 0)
    scale = jnp.broadcast_to(scale_s[0:1], (group, dk))
    for s in range(1, seqs):
        scale = jnp.where(lax.rem(row_of, seqs) == s, jnp.broadcast_to(scale_s[s : s + 1], (group, dk)), scale)
    query = total[0:group] * scale
    forget_pre = total[group : 2 * group] * scale
    value = total[2 * group : 3 * group] * scale
    gate_pre = total[3 * group : 4 * group] * scale
    lower = floors[...]
    forget = lower + (1.0 - lower) * jax.nn.sigmoid(forget_pre)
    activ = query * jax.nn.sigmoid(query)
    columns = jnp.concatenate([forget, activ, jnp.zeros((dk - 2 * group, dk), F32)], axis=0).T

    state_copy.wait()
    for h in range(heads_local):
        for s in range(seqs):
            i = h * seqs + s
            v_row = value[i : i + 1]
            f_col = columns[:, i : i + 1]
            q_col = columns[:, group + i : group + i + 1]
            new = v_row + f_col * (state[s, h] - v_row)
            heads[pl.ds(i, 1), :] = jnp.sum(new * q_col, axis=0, keepdims=True)

    head_out = heads[...]
    normed = head_out * lax.rsqrt(jnp.mean(head_out * head_out, axis=1, keepdims=True) + EPS)
    mixed = normed * head_gain[...] * (gate_pre * jax.nn.sigmoid(gate_pre))
    mix[z] = mixed.astype(BF16)
    ag = {}
    for d in far_first:
        ag[d] = remote(mix.at[z], mix.at[z], mix_send.at[d], mix_recv.at[d], peer(d), c)
        ag[d].start()
    tok.wait_send()
    for d in far_first:
        sq_copy(peer(d)).wait_send()
        chunk_copy(peer(d)).wait_send()
    for h in range(heads_local):
        for s in range(seqs):
            i = h * seqs + s
            forget_out[s, pl.ds(h, 1), :] = forget[i : i + 1]
            value_out[s, pl.ds(h, 1), :] = value[i : i + 1]
    weight_copies[0].wait()
    swaps[0].wait_recv()
    for d in near_first:
        ag[d].wait_recv()
    by_head = dot(gather, mix[...].reshape(kv * group, dv)).astype(BF16)
    every = jnp.concatenate([by_head[h * rows : (h + 1) * rows] for h in range(heads_local)], axis=1)
    part_out[...] = packed(dot_t(every, out_w[1]))
    part = remote(part_out, part_in, pair_send.at[5], pair_recv.at[5], z, other)
    part.start()
    kept = packed(dot_t(every, out_w[0])) + packed(own)
    part.wait_recv()
    middle = (kept + part_in[...]).astype(BF16)
    mid_own[...] = middle
    half = z // half_kv
    half_z = lax.rem(z, half_kv)
    kept_here = half == c
    am = {}
    for d in far_first:
        am[d] = remote(mid_own, mid.at[half_z, c], mid_send.at[d], mid_recv.at[half_z, c], peer(d), half)
        am[d].start()
    am_pair = remote(mid_own, mid.at[half_z, c], mid_send.at[0], mid_recv.at[half_z, c], z, half)

    @pl.when(kept_here)
    def _():
        mid[half_z, c] = middle

    @pl.when(jnp.logical_not(kept_here))
    def _():
        am_pair.start()

    part.wait_send()
    for d in far_first:
        ag[d].wait_send()
    for copy in swaps:
        copy.wait_send()
    gain = mlp_gain[pl.ds(pl.multiple_of(c * half_kv, half_kv), half_kv), :]
    for w in weight_copies[1:]:
        w.wait()
    for s in swaps[1:]:
        s.wait_recv()
    for i in range(half_kv):
        for from_c in range(tp):
            from_self = jnp.logical_and(c * half_kv + i == z, c == from_c)

            @pl.when(jnp.logical_not(from_self))
            def _(i=i, from_c=from_c):
                remote(mid_own, mid.at[i, from_c], mid_send.at[0], mid_recv.at[i, from_c], z, other).wait_recv()

    tops, bottoms = [], []
    squares = jnp.zeros((half_rows, tp * feats), F32)
    for i in range(half_kv):
        a = mid[i, 0].astype(F32)
        b = mid[i, 1].astype(F32)
        squares = squares + a * a + b * b
        g = gain[i : i + 1]
        tops.append((jnp.where(low, a, halves_swapped(b)) * g).astype(BF16))
        bottoms.append((jnp.where(low, halves_swapped(a), b) * g).astype(BF16))
    features = jnp.concatenate(
        [jnp.concatenate(tops, axis=1), jnp.concatenate(bottoms, axis=1)], axis=0
    )
    sq_top = jnp.sum(jnp.where(low, squares, 0.0), axis=1, keepdims=True)
    sq_bottom = jnp.sum(jnp.where(low, 0.0, squares), axis=1, keepdims=True)
    sq_mid = jnp.concatenate([sq_top, sq_bottom], axis=0)
    wide_out[4, :, :] = jnp.broadcast_to(sq_mid, wide_out.shape[1:])
    wides = [
        remote(wide_out.at[i], wide_in.at[i], pair_send.at[6 + i], pair_recv.at[6 + i], z, other) for i in range(5)
    ]
    wides[4].start()
    sums = []
    for i in range(4):
        sums.append(dot_t(features, mlp_w[i]))
        wide_out[i, :, pl.ds(0, units)] = sums[i]
        wides[i].start()
    for copy in wides:
        copy.wait_recv()
    mlp_scale = lax.rsqrt((sq_mid + wide_in[4, :, 0:1]) / width + EPS)
    terms = None
    for i in range(2):
        gate = (sums[i] + wide_in[1 - i, :, pl.ds(0, units)]) * mlp_scale
        upward = (sums[2 + i] + wide_in[3 - i, :, pl.ds(0, units)]) * mlp_scale
        hidden = (gate * jax.nn.sigmoid(gate) * upward).astype(BF16)
        term = dot(hidden, down_w[i])
        terms = term if terms is None else terms + term

    sends = []
    for i in range(half_kv):
        at = slice(i * tp * feats, (i + 1) * tp * feats)
        top, bottom = terms[:half_rows, at], terms[half_rows:, at]
        to = c * half_kv + i
        for to_c, message in (
            (0, jnp.where(low, top, halves_swapped(bottom))),
            (1, jnp.where(low, halves_swapped(top), bottom)),
        ):
            n = 2 * i + to_c
            terms_out[n] = message.astype(BF16)
            copy = remote(terms_out.at[n], terms_in.at[z], term_send.at[n], term_recv.at[z], to, to_c)
            to_self = jnp.logical_and(to == z, to_c == c)
            sends.append((copy, to_self, n))

            @pl.when(jnp.logical_not(to_self))
            def _(copy=copy):
                copy.start()

            @pl.when(to_self)
            def _(n=n):
                terms_in[z] = terms_out[n]

    for copy in wides:
        copy.wait_send()
    for d in far_first:
        am[d].wait_send()

    @pl.when(jnp.logical_not(kept_here))
    def _():
        am_pair.wait_send()

    for i in range(kv):
        from_self = jnp.logical_and(i == z, c == z // half_kv)

        @pl.when(jnp.logical_not(from_self))
        def _(i=i):
            remote(terms_out.at[0], terms_in.at[i], term_send.at[0], term_recv.at[i], z, other).wait_recv()

    summed = middle.astype(F32) + jnp.sum(terms_in[...].astype(F32), axis=0)
    result[pl.ds(0, half_rows), :] = summed[:, :feats].astype(BF16)
    result[pl.ds(half_rows, half_rows), :] = summed[:, feats:].astype(BF16)

    for copy, to_self, n in sends:

        @pl.when(jnp.logical_not(to_self))
        def _(copy=copy):
            copy.wait_send()


def body(
    kv,
    tp,
    tokens,
    past_state,
    mix_gain,
    w_query,
    w_forget,
    w_value,
    w_gate_out,
    floor_logits,
    head_gain,
    w_out,
    mlp_gain,
    w_gate,
    w_up,
    w_down,
):
    rows, feats = tokens.shape
    seqs, heads_local, dk, dv = past_state.shape
    units = w_gate.shape[1]
    group = heads_local * seqs
    channels = heads_local * dv
    half_cols = w_down.shape[1] // tp
    wide = -(-units // 128) * 128
    in_vmem = pl.BlockSpec(memory_space=pltpu.VMEM)
    dma = pltpu.SemaphoreType.DMA
    result, forget, value = pl.pallas_call(
        functools.partial(kernel, kv, tp),
        name="decode_step",
        out_shape=(
            jax.ShapeDtypeStruct((rows, feats), BF16),
            jax.ShapeDtypeStruct((seqs, heads_local, dk), F32),
            jax.ShapeDtypeStruct((seqs, heads_local, dv), F32),
        ),
        in_specs=[pl.BlockSpec(memory_space=pltpu.HBM)] * 14,
        out_specs=(in_vmem, in_vmem, in_vmem),
        scratch_shapes=[
            pltpu.VMEM((rows, feats), BF16),
            pltpu.VMEM((1, tp * feats), F32),
            pltpu.VMEM((heads_local, dk), F32),
            pltpu.VMEM((1, dv), F32),
            pltpu.VMEM((kv, tp * feats), F32),
            pltpu.VMEM((rows, feats), BF16),
            pltpu.VMEM((4, *w_query.shape), BF16),
            pltpu.VMEM(past_state.shape, F32),
            pltpu.VMEM((2, feats, channels), BF16),
            pltpu.VMEM((4, units, half_cols), BF16),
            pltpu.VMEM((2, units, half_cols), BF16),
            pltpu.VMEM((group, dk), F32),
            pltpu.VMEM((group, dv), F32),
            pltpu.VMEM((kv, 4 * group, dk), BF16),
            pltpu.VMEM((kv, 4 * group, dk), BF16),
            pltpu.VMEM((kv, seqs, dk), F32),
            pltpu.VMEM((kv, seqs, dk), F32),
            pltpu.VMEM((kv, group, dv), BF16),
            pltpu.VMEM((rows // 2, 2 * feats), F32),
            pltpu.VMEM((rows // 2, 2 * feats), F32),
            pltpu.VMEM((rows // 2, 2 * feats), BF16),
            pltpu.VMEM((kv // tp, tp, rows // 2, 2 * feats), BF16),
            pltpu.VMEM((5, rows, wide), F32),
            pltpu.VMEM((5, rows, wide), F32),
            pltpu.VMEM((kv, rows // 2, 2 * feats), BF16),
            pltpu.VMEM((kv, rows // 2, 2 * feats), BF16),
            dma((14,)),
            dma((11,)),
            dma((11,)),
            dma((kv,)),
            dma((kv,)),
            dma((kv,)),
            dma((kv,)),
            dma((kv,)),
            dma((kv,)),
            dma((kv,)),
            dma((kv // tp, tp)),
            dma((kv,)),
            dma((kv,)),
            pltpu.SemaphoreType.REGULAR,
            pltpu.SemaphoreType.REGULAR((kv,)),
        ],
        compiler_params=pltpu.CompilerParams(
            collective_id=0, has_side_effects=True, vmem_limit_bytes=VMEM_BYTES
        ),
    )(*hbm(
        tokens,
        past_state,
        mix_gain.reshape(1, -1),
        w_query,
        w_forget,
        w_value,
        w_gate_out,
        floor_logits.reshape(heads_local, dk),
        head_gain.reshape(1, -1),
        w_out.T,
        mlp_gain.reshape(kv, tp * feats),
        w_gate.T,
        w_up.T,
        w_down,
    ))
    value = value[:, :, None, :]
    return result, value + forget[..., None] * (past_state - value)


def solution(mesh):
    placed = (
        P(("grp", "dp"), ("kv", "tp")),
        P(("grp", "dp", "kv"), "tp", None, None),
        P("kv"),
        P("kv", "tp"),
        P("kv", "tp"),
        P("kv", "tp"),
        P("kv", "tp"),
        P("tp"),
        P(),
        P(None, ("kv", "tp")),
        P(),
        P(None, ("kv", "tp")),
        P(None, ("kv", "tp")),
        P(("kv", "tp"), None),
    )
    return jax.shard_map(
        functools.partial(body, mesh.shape["kv"], mesh.shape["tp"]),
        mesh=mesh,
        in_specs=placed,
        out_specs=(P(("grp", "dp"), ("kv", "tp")), P(("grp", "dp", "kv"), "tp", None, None)),
        check_vma=False,
    )
```

```python
import functools

import jax
import jax.numpy as jnp
from jax import lax
from jax.experimental import pallas as pl
from jax.experimental.pallas import tpu as pltpu
from jax.sharding import PartitionSpec as P

MESH = pl.DeviceIdType.MESH
EPS = 1e-06
VMEM_BYTES = 48 * 1024 * 1024
F32 = jnp.float32
BF16 = jnp.bfloat16


def dot(a, b):
    return jnp.dot(a, b, preferred_element_type=F32)


def dot_t(a, b):
    return lax.dot_general(a, b, (((1,), (1,)), ((), ())), preferred_element_type=F32)


def hbm(*arrays):
    return [pltpu.with_memory_space_constraint(a, pltpu.HBM) for a in arrays]


def packed(x):
    half = x.shape[0] // 2
    return jnp.concatenate([x[:half], x[half:]], axis=1)


def halves_swapped(x):
    return pltpu.roll(x, x.shape[1] // 2, 1)


def kernel(
    kv,
    tp,
    tokens_hbm,
    past_state,
    mix_gain_hbm,
    w_query,
    w_forget,
    w_value,
    w_gate_out,
    floor_hbm,
    head_gain_hbm,
    w_out,
    mlp_gain_hbm,
    w_gate,
    w_up,
    w_down,
    result,
    forget_out,
    value_out,
    tokens,
    mix_gain,
    floor_logits,
    head_gain,
    mlp_gain,
    tok_own,
    tok_other,
    proj_w,
    state,
    out_w,
    mlp_w,
    down_w,
    floors,
    heads,
    chunk_out,
    chunk_in,
    sq_out,
    sq_in,
    total,
    relay_in,
    relay_sq_in,
    relayed_out,
    relayed_in,
    mix,
    part_out,
    part_in,
    mid_own,
    mid,
    wide_out,
    wide_in,
    terms_out,
    terms_in,
    local_sem,
    pair_send,
    pair_recv,
    rs_send,
    rs_recv,
    sq_send,
    sq_recv,
    mix_send,
    mix_recv,
    mid_send,
    mid_recv,
    term_send,
    term_recv,
    relay_recv,
    relay_sq_recv,
    relayed_send,
    relayed_recv,
    pair_in,
    ready,
):
    z = lax.axis_index("kv")
    c = lax.axis_index("tp")
    other = 1 - c
    rows, feats = tokens.shape
    seqs, heads_local, dk, dv = past_state.shape
    units = w_gate.shape[0]
    group = heads_local * seqs
    half_rows = rows // 2
    width = kv * tp * feats
    half_kv = kv // tp
    half_cols = half_kv * tp * feats

    def local(src, dst, i):
        copy = pltpu.make_async_copy(src, dst, local_sem.at[i])
        copy.start()
        return copy

    def remote(src, dst, send, recv, to_z, to_c):
        return pltpu.make_async_remote_copy(
            src_ref=src,
            dst_ref=dst,
            send_sem=send,
            recv_sem=recv,
            device_id={"kv": to_z, "tp": to_c},
            device_id_type=MESH,
        )

    def peer(d):
        return lax.rem(z + d, kv)

    def place(w):
        return jnp.where(w == 0, kv - 2, jnp.where(w == kv - 1, kv - 1, w - 1))

    order = [*range(1, kv - 1), 0, kv - 1]
    last = kv - 1
    near_last = [w for w in range(kv - tp - 2, kv - 1)]
    relays = {0: kv // 4, last: near_last[0] - 1}
    behind = near_last[0] - 1
    listeners = {0: [relays[0], *near_last], last: [relays[last], *near_last, 0]}
    far_first = sorted(range(1, kv), key=lambda d: -min(d, kv - d))

    def wait_all(buffer, count, sem, received=True):
        part_of = buffer.at[pl.ds(0, count)]
        copy = remote(part_of, part_of, sem, sem, z, other)
        copy.wait_recv() if received else copy.wait_send()

    barrier = pltpu.get_barrier_semaphore()

    def signal(sem, to_z, to_c):
        pl.semaphore_signal(sem, inc=1, device_id={"kv": to_z, "tp": to_c}, device_id_type=MESH)

    @pl.when(c == 1)
    def _():
        signal(barrier, z, 0)

    tokens_copy = local(tokens_hbm, tokens, 2)
    gain_copy = local(mix_gain_hbm, mix_gain, 3)
    for i, w in enumerate((w_query, w_forget, w_value, w_gate_out)):
        local(w, proj_w.at[i], 0)
    state_copy = local(past_state, state, 1)
    small_copies = [
        local(floor_hbm, floor_logits, 4),
        local(head_gain_hbm, head_gain, 5),
        local(mlp_gain_hbm, mlp_gain, 6),
    ]
    half_of = pl.ds(pl.multiple_of(c * half_cols, half_cols), half_cols)
    half_of_other = pl.ds(pl.multiple_of(other * half_cols, half_cols), half_cols)
    weight_copies = [
        local(w_out.at[:, half_of], out_w.at[0], 7),
        local(w_gate.at[:, half_of], mlp_w.at[0], 8),
        local(w_up.at[:, half_of], mlp_w.at[1], 9),
        local(w_down.at[:, half_of], down_w.at[0], 10),
    ]

    @pl.when(c == 0)
    def _():
        pl.semaphore_wait(barrier, 1)
        signal(pair_in, z, 1)

    @pl.when(c == 1)
    def _():
        pl.semaphore_wait(pair_in, 1)
        for w in order:

            @pl.when(place(z) < place(w))
            def _(w=w):
                signal(barrier, w, 1)

    @pl.when(c == 1)
    def _():
        @pl.when(place(z) > 0)
        def _():
            pl.semaphore_wait(barrier, place(z))

        signal(pair_in, z, 0)

    @pl.when(c == 0)
    def _():
        pl.semaphore_wait(pair_in, 1)

    for special, told in listeners.items():

        @pl.when(z == special)
        def _(special=special, told=told):
            for w in told:
                if order.index(w) < order.index(special):
                    signal(ready.at[special], w, c)

    for d in far_first:
        to = peer(d)

        @pl.when((place(to) < place(z)) & (place(z) < kv - 2))
        def _(to=to):
            signal(ready.at[z], to, c)

    tokens_copy.wait()
    own = tokens[...].astype(F32)
    tok_own[...] = packed(own).astype(BF16)
    tok = remote(tok_own, tok_other, pair_send.at[0], pair_recv.at[0], z, other)
    tok.start()

    r = lax.broadcasted_iota(jnp.int32, (kv * group, kv * group), 0)
    col = lax.broadcasted_iota(jnp.int32, (kv * group, kv * group), 1)
    s_of = lax.rem(r, seqs)
    to_chunks = lax.rem(r // seqs, heads_local) * (kv * seqs) + (r // group) * seqs + s_of
    spread = jnp.where(col == to_chunks, 1.0, 0.0).astype(BF16)
    to_heads = lax.rem(r // seqs, kv) * group + (r // (kv * seqs)) * seqs + s_of
    gather = jnp.where(col == to_heads, 1.0, 0.0).astype(BF16)

    lane = lax.broadcasted_iota(jnp.int32, (1, tp * feats), 1)
    low = lane < feats
    own_twice = jnp.concatenate([own, own], axis=1)
    tok.wait_recv()
    got = tok_other[...].astype(F32)
    got_swapped = halves_swapped(got)
    got_twice = jnp.concatenate(
        [jnp.where(low, got, got_swapped), jnp.where(low, got_swapped, got)], axis=0
    )
    mine = lax.broadcasted_iota(jnp.int32, (rows, tp * feats), 1) // feats == c
    block = jnp.where(mine, own_twice, got_twice)
    squares = jnp.sum(block * block, axis=1, keepdims=True)
    sq_out[...] = jnp.broadcast_to(squares, (rows, dk)).reshape(kv, seqs, dk)
    gain_copy.wait()
    gained = (block * mix_gain[...]).astype(BF16)
    def sq_copy(to):
        return remote(sq_out.at[to], sq_in.at[z], sq_send.at[0], sq_recv.at[0], to, c)

    def chunk_copy(to):
        return remote(chunk_out.at[to], chunk_in.at[z], rs_send.at[0], rs_recv.at[0], to, c)

    def sq_to_relay(special):
        return remote(
            sq_out.at[special], relay_sq_in.at[z - 1], sq_send.at[0], relay_sq_recv.at[0], relays[special], c
        )

    def chunk_to_relay(special):
        return remote(
            chunk_out.at[special], relay_in.at[z - 1], rs_send.at[0], relay_recv.at[0], relays[special], c
        )

    for d in far_first:
        to = peer(d)

        @pl.when(place(to) < place(z))
        def _(to=to):
            sq_copy(to).start()

    for special, relay in relays.items():

        @pl.when((z > relay) & (z <= behind))
        def _(special=special):
            sq_to_relay(special).start()

    pltpu.make_async_copy(proj_w, proj_w, local_sem.at[0]).wait()
    products = [dot(gained, proj_w[i]).astype(BF16) for i in range(4)]
    for i in (0, 2):
        stack = jnp.concatenate(
            [
                jnp.concatenate([p[:, h * dk : (h + 1) * dk] for p in products[i : i + 2]], axis=1)
                for h in range(heads_local)
            ],
            axis=0,
        )
        ordered = dot(spread, stack).astype(BF16)
        for j in range(2):
            chunk_out[:, pl.ds((i + j) * group, group), :] = ordered[:, j * dk : (j + 1) * dk].reshape(
                kv, group, dk
            )

    for d in far_first:
        to = peer(d)

        @pl.when(place(to) < place(z))
        def _(to=to):
            chunk_copy(to).start()

    for special, relay in relays.items():

        @pl.when((z > relay) & (z <= behind))
        def _(special=special):
            chunk_to_relay(special).start()

    swaps = [
        remote(w_out.at[:, half_of_other], out_w.at[1], pair_send.at[1], pair_recv.at[1], z, other),
        remote(w_gate.at[:, half_of_other], mlp_w.at[2], pair_send.at[2], pair_recv.at[2], z, other),
        remote(w_up.at[:, half_of_other], mlp_w.at[3], pair_send.at[3], pair_recv.at[3], z, other),
        remote(w_down.at[:, half_of_other], down_w.at[1], pair_send.at[4], pair_recv.at[4], z, other),
    ]
    for s in swaps:
        s.start()

    sq_in[z] = sq_out[z]
    chunk_in[z] = chunk_out[z]
    for copy in small_copies:
        copy.wait()
    lower_in = jax.nn.sigmoid(floor_logits[...])
    for h in range(heads_local):
        floors[pl.ds(h * seqs, seqs), :] = jnp.broadcast_to(lower_in[h : h + 1], (seqs, dk))

    for w in order[:-2]:

        @pl.when(place(z) < place(w))
        def _(w=w):
            pl.semaphore_wait(ready.at[w], 1)
            sq_copy(w).start()
            chunk_copy(w).start()
            for special, relay in relays.items():
                if relay == w:
                    sq_to_relay(special).start()
                    chunk_to_relay(special).start()

    for special, relay in relays.items():
        forward = remote(relayed_out, relayed_in, relayed_send.at[0], relayed_recv.at[0], special, c)

        @pl.when(z == relay)
        def _(special=special, forward=forward):
            wait_all(relay_sq_in, behind - 1, relay_sq_recv.at[0])
            wait_all(relay_in, behind - 1, relay_recv.at[0])
            relay_sq_in[z - 1] = sq_out[special]
            relay_in[z - 1] = chunk_out[special]
            sums = relay_in[0].astype(F32)
            squares = relay_sq_in[0]
            for i in range(1, behind):
                sums = sums + relay_in[i].astype(F32)
                squares = squares + relay_sq_in[i]
            relayed_out[pl.ds(0, 4 * group), :] = sums
            relayed_out[pl.ds(4 * group, seqs), :] = squares
            pl.semaphore_wait(ready.at[special], 1)
            forward.start()

        for w in listeners[special]:
            if w != relay and order.index(w) < order.index(special):

                @pl.when(z == w)
                def _(special=special):
                    pl.semaphore_wait(ready.at[special], 1)
                    sq_copy(special).start()
                    chunk_copy(special).start()

    def add_up(slots):
        sums = chunk_in[slots[0]].astype(F32)
        squares = sq_in[slots[0]]
        for w in slots[1:]:
            sums = sums + chunk_in[w].astype(F32)
            squares = squares + sq_in[w]
        return sums, squares

    is_special = (z == 0) | (z == last)

    @pl.when(jnp.logical_not(is_special))
    def _():
        wait_all(sq_in, kv - 1, sq_recv.at[0])
        wait_all(chunk_in, kv - 1, rs_recv.at[0])
        sums, squares = add_up(order)
        total[pl.ds(0, 4 * group), :] = sums
        total[pl.ds(4 * group, seqs), :] = squares

    @pl.when(is_special)
    def _():
        wait_all(sq_in, len(near_last) + 1, sq_recv.at[0])
        wait_all(chunk_in, len(near_last) + 1, rs_recv.at[0])
        sums, squares = add_up([*near_last, 0, last])
        remote(relayed_out, relayed_in, relayed_send.at[0], relayed_recv.at[0], z, other).wait_recv()
        total[pl.ds(0, 4 * group), :] = sums + relayed_in[pl.ds(0, 4 * group), :]
        total[pl.ds(4 * group, seqs), :] = squares + relayed_in[pl.ds(4 * group, seqs), :]

    total_sq = total[pl.ds(4 * group, seqs), :]
    scale_s = lax.rsqrt(total_sq / width + EPS)
    row_of = lax.broadcasted_iota(jnp.int32, (group, dk), 0)
    scale = jnp.broadcast_to(scale_s[0:1], (group, dk))
    for s in range(1, seqs):
        scale = jnp.where(lax.rem(row_of, seqs) == s, jnp.broadcast_to(scale_s[s : s + 1], (group, dk)), scale)
    query = total[pl.ds(0, group), :] * scale
    forget_pre = total[pl.ds(group, group), :] * scale
    value = total[pl.ds(2 * group, group), :] * scale
    gate_pre = total[pl.ds(3 * group, group), :] * scale
    lower = floors[...]
    forget = lower + (1.0 - lower) * jax.nn.sigmoid(forget_pre)
    activ = query * jax.nn.sigmoid(query)
    columns = jnp.concatenate([forget, activ, jnp.zeros((dk - 2 * group, dk), F32)], axis=0).T

    state_copy.wait()
    for h in range(heads_local):
        for s in range(seqs):
            i = h * seqs + s
            v_row = value[i : i + 1]
            f_col = columns[:, i : i + 1]
            q_col = columns[:, group + i : group + i + 1]
            new = v_row + f_col * (state[s, h] - v_row)
            heads[pl.ds(i, 1), :] = jnp.sum(new * q_col, axis=0, keepdims=True)

    head_out = heads[...]
    normed = head_out * lax.rsqrt(jnp.mean(head_out * head_out, axis=1, keepdims=True) + EPS)
    mixed = normed * head_gain[...] * (gate_pre * jax.nn.sigmoid(gate_pre))
    mix[z] = mixed.astype(BF16)
    for d in far_first:
        remote(mix.at[z], mix.at[z], mix_send.at[0], mix_recv.at[0], peer(d), c).start()
    tok.wait_send()
    is_relay = (z == relays[0]) | (z == relays[last])

    @pl.when(jnp.logical_not(is_relay))
    def _():
        wait_all(sq_in, kv - 1, sq_send.at[0], False)
        wait_all(chunk_in, kv - 1, rs_send.at[0], False)

    @pl.when(is_relay)
    def _():
        wait_all(sq_in, kv - 2, sq_send.at[0], False)
        wait_all(chunk_in, kv - 2, rs_send.at[0], False)
        remote(relayed_out, relayed_in, relayed_send.at[0], relayed_recv.at[0], z, other).wait_send()

    for h in range(heads_local):
        for s in range(seqs):
            i = h * seqs + s
            forget_out[s, pl.ds(h, 1), :] = forget[i : i + 1]
            value_out[s, pl.ds(h, 1), :] = value[i : i + 1]
    weight_copies[0].wait()
    swaps[0].wait_recv()
    wait_all(mix, kv - 1, mix_recv.at[0])
    by_head = dot(gather, mix[...].reshape(kv * group, dv)).astype(BF16)
    every = jnp.concatenate([by_head[h * rows : (h + 1) * rows] for h in range(heads_local)], axis=1)
    part_out[...] = packed(dot_t(every, out_w[1]))
    part = remote(part_out, part_in, pair_send.at[5], pair_recv.at[5], z, other)
    part.start()
    kept = packed(dot_t(every, out_w[0])) + packed(own)
    part.wait_recv()
    middle = (kept + part_in[...]).astype(BF16)
    mid_own[...] = middle
    half = z // half_kv
    half_z = lax.rem(z, half_kv)
    kept_here = half == c
    for d in far_first:
        remote(mid_own, mid.at[half_z * tp + c], mid_send.at[0], mid_recv.at[0], peer(d), half).start()

    @pl.when(kept_here)
    def _():
        mid[half_z * tp + c] = middle

    @pl.when(jnp.logical_not(kept_here))
    def _():
        remote(mid_own, mid.at[half_z * tp + c], mid_send.at[0], mid_recv.at[0], z, half).start()

    part.wait_send()
    wait_all(mix, kv - 1, mix_send.at[0], False)
    for copy in swaps:
        copy.wait_send()
    gain = mlp_gain[pl.ds(pl.multiple_of(c * half_kv, half_kv), half_kv), :]
    for w in weight_copies[1:]:
        w.wait()
    for s in swaps[1:]:
        s.wait_recv()
    def wait_others(buffer, sem, received=True):
        @pl.when(kept_here)
        def _():
            wait_all(buffer, kv - 1, sem, received)

        @pl.when(jnp.logical_not(kept_here))
        def _():
            wait_all(buffer, kv, sem, received)

    wait_others(mid, mid_recv.at[0])
    tops, bottoms = [], []
    squares = jnp.zeros((half_rows, tp * feats), F32)
    for i in range(half_kv):
        a = mid[tp * i].astype(F32)
        b = mid[tp * i + 1].astype(F32)
        squares = squares + a * a + b * b
        g = gain[i : i + 1]
        tops.append((jnp.where(low, a, halves_swapped(b)) * g).astype(BF16))
        bottoms.append((jnp.where(low, halves_swapped(a), b) * g).astype(BF16))
    features = jnp.concatenate(
        [jnp.concatenate(tops, axis=1), jnp.concatenate(bottoms, axis=1)], axis=0
    )
    sq_top = jnp.sum(jnp.where(low, squares, 0.0), axis=1, keepdims=True)
    sq_bottom = jnp.sum(jnp.where(low, 0.0, squares), axis=1, keepdims=True)
    sq_mid = jnp.concatenate([sq_top, sq_bottom], axis=0)
    wide_out[4, :, :] = jnp.broadcast_to(sq_mid, wide_out.shape[1:])
    wides = [
        remote(wide_out.at[i], wide_in.at[i], pair_send.at[6], pair_recv.at[6], z, other) for i in range(5)
    ]
    wides[4].start()
    sums = []
    for i in range(4):
        sums.append(dot_t(features, mlp_w[i]))
        wide_out[i, :, pl.ds(0, units)] = sums[i]
        wides[i].start()
    remote(wide_out, wide_in, pair_send.at[6], pair_recv.at[6], z, other).wait_recv()
    mlp_scale = lax.rsqrt((sq_mid + wide_in[4, :, 0:1]) / width + EPS)
    terms = None
    for i in range(2):
        gate = (sums[2 * i] + wide_in[2 - 2 * i, :, pl.ds(0, units)]) * mlp_scale
        upward = (sums[2 * i + 1] + wide_in[3 - 2 * i, :, pl.ds(0, units)]) * mlp_scale
        hidden = (gate * jax.nn.sigmoid(gate) * upward).astype(BF16)
        term = dot(hidden, down_w[i])
        terms = term if terms is None else terms + term

    for i in range(half_kv):
        at = slice(i * tp * feats, (i + 1) * tp * feats)
        top, bottom = terms[:half_rows, at], terms[half_rows:, at]
        to = c * half_kv + i
        for to_c, message in (
            (0, jnp.where(low, top, halves_swapped(bottom))),
            (1, jnp.where(low, halves_swapped(top), bottom)),
        ):
            n = 2 * i + to_c
            terms_out[n] = message.astype(BF16)
            copy = remote(terms_out.at[n], terms_in.at[z], term_send.at[0], term_recv.at[0], to, to_c)
            to_self = jnp.logical_and(to == z, to_c == c)

            @pl.when(jnp.logical_not(to_self))
            def _(copy=copy):
                copy.start()

            @pl.when(to_self)
            def _(n=n):
                terms_in[z] = terms_out[n]

    remote(wide_out, wide_in, pair_send.at[6], pair_recv.at[6], z, other).wait_send()
    wait_others(mid, mid_send.at[0], False)
    wait_others(terms_in, term_recv.at[0])
    summed = middle.astype(F32) + jnp.sum(terms_in[...].astype(F32), axis=0)
    result[pl.ds(0, half_rows), :] = summed[:, :feats].astype(BF16)
    result[pl.ds(half_rows, half_rows), :] = summed[:, feats:].astype(BF16)

    wait_others(terms_in, term_send.at[0], False)


def body(
    kv,
    tp,
    tokens,
    past_state,
    mix_gain,
    w_query,
    w_forget,
    w_value,
    w_gate_out,
    floor_logits,
    head_gain,
    w_out,
    mlp_gain,
    w_gate,
    w_up,
    w_down,
):
    rows, feats = tokens.shape
    seqs, heads_local, dk, dv = past_state.shape
    units = w_gate.shape[1]
    group = heads_local * seqs
    channels = heads_local * dv
    half_cols = w_down.shape[1] // tp
    wide = -(-units // 128) * 128
    in_vmem = pl.BlockSpec(memory_space=pltpu.VMEM)
    dma = pltpu.SemaphoreType.DMA
    result, forget, value = pl.pallas_call(
        functools.partial(kernel, kv, tp),
        name="decode_step",
        out_shape=(
            jax.ShapeDtypeStruct((rows, feats), BF16),
            jax.ShapeDtypeStruct((seqs, heads_local, dk), F32),
            jax.ShapeDtypeStruct((seqs, heads_local, dv), F32),
        ),
        in_specs=[pl.BlockSpec(memory_space=pltpu.HBM)] * 14,
        out_specs=(in_vmem, in_vmem, in_vmem),
        scratch_shapes=[
            pltpu.VMEM((rows, feats), BF16),
            pltpu.VMEM((1, tp * feats), F32),
            pltpu.VMEM((heads_local, dk), F32),
            pltpu.VMEM((1, dv), F32),
            pltpu.VMEM((kv, tp * feats), F32),
            pltpu.VMEM((rows // 2, 2 * feats), BF16),
            pltpu.VMEM((rows // 2, 2 * feats), BF16),
            pltpu.VMEM((4, *w_query.shape), BF16),
            pltpu.VMEM(past_state.shape, F32),
            pltpu.VMEM((2, feats, channels), BF16),
            pltpu.VMEM((4, units, half_cols), BF16),
            pltpu.VMEM((2, units, half_cols), BF16),
            pltpu.VMEM((group, dk), F32),
            pltpu.VMEM((group, dv), F32),
            pltpu.VMEM((kv, 4 * group, dk), BF16),
            pltpu.VMEM((kv, 4 * group, dk), BF16),
            pltpu.VMEM((kv, seqs, dk), F32),
            pltpu.VMEM((kv, seqs, dk), F32),
            pltpu.VMEM((4 * group + 8, dk), F32),
            pltpu.VMEM((kv, 4 * group, dk), BF16),
            pltpu.VMEM((kv, seqs, dk), F32),
            pltpu.VMEM((4 * group + 8, dk), F32),
            pltpu.VMEM((4 * group + 8, dk), F32),
            pltpu.VMEM((kv, group, dv), BF16),
            pltpu.VMEM((rows // 2, 2 * feats), F32),
            pltpu.VMEM((rows // 2, 2 * feats), F32),
            pltpu.VMEM((rows // 2, 2 * feats), BF16),
            pltpu.VMEM((kv, rows // 2, 2 * feats), BF16),
            pltpu.VMEM((5, rows, wide), F32),
            pltpu.VMEM((5, rows, wide), F32),
            pltpu.VMEM((kv, rows // 2, 2 * feats), BF16),
            pltpu.VMEM((kv, rows // 2, 2 * feats), BF16),
            dma((11,)),
            dma((7,)),
            dma((7,)),
            *[dma((1,))] * 14,
            pltpu.SemaphoreType.REGULAR,
            pltpu.SemaphoreType.REGULAR((kv,)),
        ],
        compiler_params=pltpu.CompilerParams(
            collective_id=0, has_side_effects=True, vmem_limit_bytes=VMEM_BYTES
        ),
    )(*hbm(
        tokens,
        past_state,
        mix_gain.reshape(1, -1),
        w_query,
        w_forget,
        w_value,
        w_gate_out,
        floor_logits.reshape(heads_local, dk),
        head_gain.reshape(1, -1),
        w_out.T,
        mlp_gain.reshape(kv, tp * feats),
        w_gate.T,
        w_up.T,
        w_down,
    ))
    value = value[:, :, None, :]
    return result, value + forget[..., None] * (past_state - value)


def solution(mesh):
    placed = (
        P(("grp", "dp"), ("kv", "tp")),
        P(("grp", "dp", "kv"), "tp", None, None),
        P("kv"),
        P("kv", "tp"),
        P("kv", "tp"),
        P("kv", "tp"),
        P("kv", "tp"),
        P("tp"),
        P(),
        P(None, ("kv", "tp")),
        P(),
        P(None, ("kv", "tp")),
        P(None, ("kv", "tp")),
        P(("kv", "tp"), None),
    )
    return jax.shard_map(
        functools.partial(body, mesh.shape["kv"], mesh.shape["tp"]),
        mesh=mesh,
        in_specs=placed,
        out_specs=(P(("grp", "dp"), ("kv", "tp")), P(("grp", "dp", "kv"), "tp", None, None)),
        check_vma=False,
    )
```

```python
import functools

import jax
import jax.numpy as jnp
from jax import lax
from jax.experimental import pallas as pl
from jax.experimental.pallas import tpu as pltpu
from jax.sharding import PartitionSpec as P

MESH = pl.DeviceIdType.MESH
EPS = 1e-06
VMEM_BYTES = 48 * 1024 * 1024
F32 = jnp.float32
BF16 = jnp.bfloat16


def dot(a, b):
    return jnp.dot(a, b, preferred_element_type=F32)


def dot_t(a, b):
    return lax.dot_general(a, b, (((1,), (1,)), ((), ())), preferred_element_type=F32)


def hbm(*arrays):
    return [pltpu.with_memory_space_constraint(a, pltpu.HBM) for a in arrays]


def packed(x):
    half = x.shape[0] // 2
    return jnp.concatenate([x[:half], x[half:]], axis=1)


def halves_swapped(x):
    return pltpu.roll(x, x.shape[1] // 2, 1)


def kernel(
    kv,
    tp,
    tokens_hbm,
    past_state,
    mix_gain_hbm,
    w_query,
    w_forget,
    w_value,
    w_gate_out,
    floor_hbm,
    head_gain_hbm,
    w_out,
    mlp_gain_hbm,
    w_gate,
    w_up,
    w_down,
    result,
    forget_out,
    value_out,
    tokens,
    mix_gain,
    floor_logits,
    head_gain,
    mlp_gain,
    tok_own,
    tok_other,
    proj_w,
    state,
    out_w,
    mlp_w,
    down_w,
    floors,
    heads,
    chunk_out,
    chunk_in,
    sq_out,
    sq_in,
    total,
    relay_in,
    relay_sq_in,
    relayed_out,
    relayed_in,
    mix_own,
    mix,
    part_out,
    part_in,
    mid_own,
    mid,
    wide_out,
    wide_in,
    terms_out,
    terms_in,
    local_sem,
    pair_send,
    pair_recv,
    rs_send,
    rs_recv,
    sq_send,
    sq_recv,
    mix_send,
    mix_recv,
    mid_send,
    mid_recv,
    term_send,
    term_recv,
    relay_recv,
    relay_sq_recv,
    relayed_send,
    relayed_recv,
    pair_in,
    ready,
):
    z = lax.axis_index("kv")
    c = lax.axis_index("tp")
    other = 1 - c
    rows, feats = tokens.shape
    seqs, heads_local, dk, dv = past_state.shape
    units = w_gate.shape[0]
    group = heads_local * seqs
    half_rows = rows // 2
    width = kv * tp * feats
    half_kv = kv // tp
    half_cols = half_kv * tp * feats

    def local(src, dst, i):
        copy = pltpu.make_async_copy(src, dst, local_sem.at[i])
        copy.start()
        return copy

    def remote(src, dst, send, recv, to_z, to_c):
        return pltpu.make_async_remote_copy(
            src_ref=src,
            dst_ref=dst,
            send_sem=send,
            recv_sem=recv,
            device_id={"kv": to_z, "tp": to_c},
            device_id_type=MESH,
        )

    def peer(d):
        return lax.rem(z + d, kv)

    def place(w):
        return jnp.where(w == 0, kv - 2, jnp.where(w == kv - 1, kv - 1, w - 1))

    order = [*range(1, kv - 1), 0, kv - 1]
    last = kv - 1
    near_last = [w for w in range(kv - tp - 2, kv - 1)]
    relays = {0: kv // 4, last: near_last[0] - 1}
    behind = near_last[0] - 1
    listeners = {0: [relays[0], *near_last], last: [relays[last], *near_last, 0]}
    far_first = sorted(range(1, kv), key=lambda d: -min(d, kv - d))

    def wait_all(buffer, count, sem, received=True):
        part_of = buffer.at[pl.ds(0, count)]
        copy = remote(part_of, part_of, sem, sem, z, other)
        copy.wait_recv() if received else copy.wait_send()

    first = pl.ds(0, 3 * group)
    second = pl.ds(3 * group, group)

    def wait_rows(buffer, count, at, sem, received=True):
        part_of = buffer.at[pl.ds(0, count), at]
        copy = remote(part_of, part_of, sem, sem, z, other)
        copy.wait_recv() if received else copy.wait_send()

    barrier = pltpu.get_barrier_semaphore()

    def signal(sem, to_z, to_c):
        pl.semaphore_signal(sem, inc=1, device_id={"kv": to_z, "tp": to_c}, device_id_type=MESH)

    @pl.when(c == 1)
    def _():
        signal(barrier, z, 0)

    tokens_copy = local(tokens_hbm, tokens, 2)
    gain_copy = local(mix_gain_hbm, mix_gain, 3)
    for i, w in enumerate((w_query, w_forget, w_value, w_gate_out)):
        local(w, proj_w.at[i], 0)
    state_copy = local(past_state, state, 1)
    small_copies = [
        local(floor_hbm, floor_logits, 4),
        local(head_gain_hbm, head_gain, 5),
        local(mlp_gain_hbm, mlp_gain, 6),
    ]
    half_of = pl.ds(pl.multiple_of(c * half_cols, half_cols), half_cols)
    half_of_other = pl.ds(pl.multiple_of(other * half_cols, half_cols), half_cols)
    weight_copies = [
        local(w_out.at[:, half_of_other], out_w.at[0], 7),
        local(w_gate.at[:, half_of], mlp_w.at[0], 8),
        local(w_up.at[:, half_of], mlp_w.at[1], 9),
        local(w_down.at[:, half_of], down_w.at[0], 10),
    ]

    @pl.when(c == 0)
    def _():
        pl.semaphore_wait(barrier, 1)
        signal(pair_in, z, 1)

    @pl.when(c == 1)
    def _():
        pl.semaphore_wait(pair_in, 1)
        for w in order:

            @pl.when(place(z) < place(w))
            def _(w=w):
                signal(barrier, w, 1)

    @pl.when(c == 1)
    def _():
        @pl.when(place(z) > 0)
        def _():
            pl.semaphore_wait(barrier, place(z))

        signal(pair_in, z, 0)

    @pl.when(c == 0)
    def _():
        pl.semaphore_wait(pair_in, 1)

    for special, told in listeners.items():

        @pl.when(z == special)
        def _(special=special, told=told):
            for w in told:
                if order.index(w) < order.index(special):
                    signal(ready.at[special], w, c)

    for d in far_first:
        to = peer(d)

        @pl.when((place(to) < place(z)) & (place(z) < kv - 2))
        def _(to=to):
            signal(ready.at[z], to, c)

    tokens_copy.wait()
    own = tokens[...].astype(F32)
    tok_own[...] = packed(own).astype(BF16)
    tok = remote(tok_own, tok_other, pair_send.at[0], pair_recv.at[0], z, other)
    tok.start()

    r = lax.broadcasted_iota(jnp.int32, (kv * group, kv * group), 0)
    col = lax.broadcasted_iota(jnp.int32, (kv * group, kv * group), 1)
    s_of = lax.rem(r, seqs)
    to_chunks = lax.rem(r // seqs, heads_local) * (kv * seqs) + (r // group) * seqs + s_of
    spread = jnp.where(col == to_chunks, 1.0, 0.0).astype(BF16)
    to_heads = lax.rem(r // seqs, kv) * group + (r // (kv * seqs)) * seqs + s_of
    gather = jnp.where(col == to_heads, 1.0, 0.0).astype(BF16)

    lane = lax.broadcasted_iota(jnp.int32, (1, tp * feats), 1)
    low = lane < feats
    own_twice = jnp.concatenate([own, own], axis=1)
    tok.wait_recv()
    got = tok_other[...].astype(F32)
    got_swapped = halves_swapped(got)
    got_twice = jnp.concatenate(
        [jnp.where(low, got, got_swapped), jnp.where(low, got_swapped, got)], axis=0
    )
    mine = lax.broadcasted_iota(jnp.int32, (rows, tp * feats), 1) // feats == c
    block = jnp.where(mine, own_twice, got_twice)
    squares = jnp.sum(block * block, axis=1, keepdims=True)
    sq_out[...] = jnp.broadcast_to(squares, (rows, dk)).reshape(kv, seqs, dk)
    gain_copy.wait()
    gained = (block * mix_gain[...]).astype(BF16)
    def sq_copy(to):
        return remote(sq_out.at[to], sq_in.at[z], sq_send.at[0], sq_recv.at[0], to, c)

    def chunk_copy(to, at):
        which = 0 if at is first else 1
        return remote(
            chunk_out.at[to, at], chunk_in.at[z, at], rs_send.at[which], rs_recv.at[which], to, c
        )

    def sq_to_relay(special):
        return remote(
            sq_out.at[special], relay_sq_in.at[z - 1], sq_send.at[0], relay_sq_recv.at[0], relays[special], c
        )

    def chunk_to_relay(special, at):
        return remote(
            chunk_out.at[special, at],
            relay_in.at[z - 1, at],
            rs_send.at[0 if at is first else 1],
            relay_recv.at[0],
            relays[special],
            c,
        )

    for d in far_first:
        to = peer(d)

        @pl.when(place(to) < place(z))
        def _(to=to):
            sq_copy(to).start()

    for special, relay in relays.items():

        @pl.when((z > relay) & (z <= behind))
        def _(special=special):
            sq_to_relay(special).start()

    pltpu.make_async_copy(proj_w, proj_w, local_sem.at[0]).wait()
    products = [dot(gained, proj_w[i]).astype(BF16) for i in range(4)]
    for i in (0, 2):
        stack = jnp.concatenate(
            [
                jnp.concatenate([p[:, h * dk : (h + 1) * dk] for p in products[i : i + 2]], axis=1)
                for h in range(heads_local)
            ],
            axis=0,
        )
        ordered = dot(spread, stack).astype(BF16)
        for j in range(2):
            chunk_out[:, pl.ds((i + j) * group, group), :] = ordered[:, j * dk : (j + 1) * dk].reshape(
                kv, group, dk
            )

    for at in (first, second):
        for d in far_first:
            to = peer(d)

            @pl.when(place(to) < place(z))
            def _(to=to, at=at):
                chunk_copy(to, at).start()

        for special, relay in relays.items():

            @pl.when((z > relay) & (z <= behind))
            def _(special=special, at=at):
                chunk_to_relay(special, at).start()

    swaps = [
        remote(w_out.at[:, half_of], out_w.at[1], pair_send.at[1], pair_recv.at[1], z, other),
        remote(w_gate.at[:, half_of_other], mlp_w.at[2], pair_send.at[2], pair_recv.at[2], z, other),
        remote(w_up.at[:, half_of_other], mlp_w.at[3], pair_send.at[3], pair_recv.at[3], z, other),
        remote(w_down.at[:, half_of_other], down_w.at[1], pair_send.at[4], pair_recv.at[4], z, other),
    ]
    is_special = (z == 0) | (z == last)

    @pl.when(jnp.logical_not(is_special))
    def _():
        for s in swaps:
            s.start()


    sq_in[z] = sq_out[z]
    chunk_in[z] = chunk_out[z]
    for copy in small_copies:
        copy.wait()
    lower_in = jax.nn.sigmoid(floor_logits[...])
    for h in range(heads_local):
        floors[pl.ds(h * seqs, seqs), :] = jnp.broadcast_to(lower_in[h : h + 1], (seqs, dk))

    for w in order[:-2]:

        @pl.when(place(z) < place(w))
        def _(w=w):
            pl.semaphore_wait(ready.at[w], 1)
            sq_copy(w).start()
            chunk_copy(w, first).start()
            chunk_copy(w, second).start()
            for special, relay in relays.items():
                if relay == w:
                    sq_to_relay(special).start()
                    chunk_to_relay(special, first).start()
                    chunk_to_relay(special, second).start()

    for special, relay in relays.items():
        forward = remote(relayed_out, relayed_in, relayed_send.at[0], relayed_recv.at[0], special, c)

        @pl.when(z == relay)
        def _(special=special, forward=forward):
            wait_all(relay_sq_in, behind - 1, relay_sq_recv.at[0])
            wait_all(relay_in, behind - 1, relay_recv.at[0])
            relay_sq_in[z - 1] = sq_out[special]
            relay_in[z - 1] = chunk_out[special]
            sums = relay_in[0].astype(F32)
            squares = relay_sq_in[0]
            for i in range(1, behind):
                sums = sums + relay_in[i].astype(F32)
                squares = squares + relay_sq_in[i]
            relayed_out[pl.ds(0, 4 * group), :] = sums
            relayed_out[pl.ds(4 * group, seqs), :] = squares
            pl.semaphore_wait(ready.at[special], 1)
            forward.start()

        for w in listeners[special]:
            if w != relay and order.index(w) < order.index(special):

                @pl.when(z == w)
                def _(special=special):
                    pl.semaphore_wait(ready.at[special], 1)
                    sq_copy(special).start()
                    chunk_copy(special, first).start()
                    chunk_copy(special, second).start()

    def add_up(slots, at):
        sums = chunk_in[slots[0], at].astype(F32)
        for w in slots[1:]:
            sums = sums + chunk_in[w, at].astype(F32)
        return sums

    def add_up_sq(slots):
        squares = sq_in[slots[0]]
        for w in slots[1:]:
            squares = squares + sq_in[w]
        return squares

    direct = [*near_last, 0, last]
    sq_rows = pl.ds(4 * group, seqs)

    @pl.when(jnp.logical_not(is_special))
    def _():
        wait_all(sq_in, kv - 1, sq_recv.at[0])
        total[sq_rows, :] = add_up_sq(order)
        wait_rows(chunk_in, kv - 1, first, rs_recv.at[0])
        total[first, :] = add_up(order, first)

    @pl.when(is_special)
    def _():
        wait_all(sq_in, len(direct) - 1, sq_recv.at[0])
        wait_rows(chunk_in, len(direct) - 1, first, rs_recv.at[0])
        remote(relayed_out, relayed_in, relayed_send.at[0], relayed_recv.at[0], z, other).wait_recv()
        total[first, :] = add_up(direct, first) + relayed_in[first, :]
        total[sq_rows, :] = add_up_sq(direct) + relayed_in[sq_rows, :]
        for s in swaps:
            s.start()

    total_sq = total[pl.ds(4 * group, seqs), :]
    scale_s = lax.rsqrt(total_sq / width + EPS)
    row_of = lax.broadcasted_iota(jnp.int32, (group, dk), 0)
    scale = jnp.broadcast_to(scale_s[0:1], (group, dk))
    for s in range(1, seqs):
        scale = jnp.where(lax.rem(row_of, seqs) == s, jnp.broadcast_to(scale_s[s : s + 1], (group, dk)), scale)
    query = total[pl.ds(0, group), :] * scale
    forget_pre = total[pl.ds(group, group), :] * scale
    value = total[pl.ds(2 * group, group), :] * scale
    lower = floors[...]
    forget = lower + (1.0 - lower) * jax.nn.sigmoid(forget_pre)
    activ = query * jax.nn.sigmoid(query)
    columns = jnp.concatenate([forget, activ, jnp.zeros((dk - 2 * group, dk), F32)], axis=0).T

    state_copy.wait()
    for h in range(heads_local):
        for s in range(seqs):
            i = h * seqs + s
            v_row = value[i : i + 1]
            f_col = columns[:, i : i + 1]
            q_col = columns[:, group + i : group + i + 1]
            new = v_row + f_col * (state[s, h] - v_row)
            heads[pl.ds(i, 1), :] = jnp.sum(new * q_col, axis=0, keepdims=True)

    @pl.when(jnp.logical_not(is_special))
    def _():
        wait_rows(chunk_in, kv - 1, second, rs_recv.at[1])
        total[second, :] = add_up(order, second)

    @pl.when(is_special)
    def _():
        wait_rows(chunk_in, len(direct) - 1, second, rs_recv.at[1])
        total[second, :] = add_up(direct, second) + relayed_in[second, :]

    gate_pre = total[second, :] * scale
    head_out = heads[...]
    normed = head_out * lax.rsqrt(jnp.mean(head_out * head_out, axis=1, keepdims=True) + EPS)
    mixed = normed * head_gain[...] * (gate_pre * jax.nn.sigmoid(gate_pre))
    mix_own[...] = mixed.astype(BF16)
    for d in far_first:
        remote(mix_own, mix.at[z], mix_send.at[0], mix_recv.at[0], peer(d), other).start()
    remote(mix_own, mix.at[z], mix_send.at[0], mix_recv.at[0], z, other).start()
    tok.wait_send()
    is_relay = (z == relays[0]) | (z == relays[last])

    @pl.when(jnp.logical_not(is_relay))
    def _():
        wait_all(sq_in, kv - 1, sq_send.at[0], False)
        wait_rows(chunk_in, kv - 1, first, rs_send.at[0], False)
        wait_rows(chunk_in, kv - 1, second, rs_send.at[1], False)

    @pl.when(is_relay)
    def _():
        wait_all(sq_in, kv - 2, sq_send.at[0], False)
        wait_rows(chunk_in, kv - 2, first, rs_send.at[0], False)
        wait_rows(chunk_in, kv - 2, second, rs_send.at[1], False)
        remote(relayed_out, relayed_in, relayed_send.at[0], relayed_recv.at[0], z, other).wait_send()

    for h in range(heads_local):
        for s in range(seqs):
            i = h * seqs + s
            forget_out[s, pl.ds(h, 1), :] = forget[i : i + 1]
            value_out[s, pl.ds(h, 1), :] = value[i : i + 1]
    weight_copies[0].wait()
    swaps[0].wait_recv()
    wait_all(mix, kv, mix_recv.at[0])
    by_head = dot(gather, mix[...].reshape(kv * group, dv)).astype(BF16)
    every = jnp.concatenate([by_head[h * rows : (h + 1) * rows] for h in range(heads_local)], axis=1)
    part_out[...] = packed(dot_t(every, out_w[1]))
    part = remote(part_out, part_in, pair_send.at[5], pair_recv.at[5], z, other)
    part.start()
    kept = packed(dot_t(every, out_w[0])) + packed(own)
    part.wait_recv()
    middle = (kept + part_in[...]).astype(BF16)
    mid_own[...] = middle
    half = z // half_kv
    half_z = lax.rem(z, half_kv)
    kept_here = half == c
    for d in far_first:
        remote(mid_own, mid.at[half_z * tp + c], mid_send.at[0], mid_recv.at[0], peer(d), half).start()

    @pl.when(kept_here)
    def _():
        mid[half_z * tp + c] = middle

    @pl.when(jnp.logical_not(kept_here))
    def _():
        remote(mid_own, mid.at[half_z * tp + c], mid_send.at[0], mid_recv.at[0], z, half).start()

    part.wait_send()
    wait_all(mix, kv, mix_send.at[0], False)
    for copy in swaps:
        copy.wait_send()
    gain = mlp_gain[pl.ds(pl.multiple_of(c * half_kv, half_kv), half_kv), :]
    for w in weight_copies[1:]:
        w.wait()
    for s in swaps[1:]:
        s.wait_recv()
    def wait_others(buffer, sem, received=True):
        @pl.when(kept_here)
        def _():
            wait_all(buffer, kv - 1, sem, received)

        @pl.when(jnp.logical_not(kept_here))
        def _():
            wait_all(buffer, kv, sem, received)

    wait_others(mid, mid_recv.at[0])
    tops, bottoms = [], []
    squares = jnp.zeros((half_rows, tp * feats), F32)
    for i in range(half_kv):
        a = mid[tp * i].astype(F32)
        b = mid[tp * i + 1].astype(F32)
        squares = squares + a * a + b * b
        g = gain[i : i + 1]
        tops.append((jnp.where(low, a, halves_swapped(b)) * g).astype(BF16))
        bottoms.append((jnp.where(low, halves_swapped(a), b) * g).astype(BF16))
    features = jnp.concatenate(
        [jnp.concatenate(tops, axis=1), jnp.concatenate(bottoms, axis=1)], axis=0
    )
    sq_top = jnp.sum(jnp.where(low, squares, 0.0), axis=1, keepdims=True)
    sq_bottom = jnp.sum(jnp.where(low, 0.0, squares), axis=1, keepdims=True)
    sq_mid = jnp.concatenate([sq_top, sq_bottom], axis=0)
    wide_out[4, :, :] = jnp.broadcast_to(sq_mid, wide_out.shape[1:])
    wides = [
        remote(wide_out.at[i], wide_in.at[i], pair_send.at[6], pair_recv.at[6], z, other) for i in range(5)
    ]
    wides[4].start()
    sums = []
    for i in range(4):
        sums.append(dot_t(features, mlp_w[i]))
        wide_out[i, :, pl.ds(0, units)] = sums[i]
        wides[i].start()
    remote(wide_out, wide_in, pair_send.at[6], pair_recv.at[6], z, other).wait_recv()
    mlp_scale = lax.rsqrt((sq_mid + wide_in[4, :, 0:1]) / width + EPS)
    terms = None
    for i in range(2):
        gate = (sums[2 * i] + wide_in[2 - 2 * i, :, pl.ds(0, units)]) * mlp_scale
        upward = (sums[2 * i + 1] + wide_in[3 - 2 * i, :, pl.ds(0, units)]) * mlp_scale
        hidden = (gate * jax.nn.sigmoid(gate) * upward).astype(BF16)
        term = dot(hidden, down_w[i])
        terms = term if terms is None else terms + term

    for i in range(half_kv):
        at = slice(i * tp * feats, (i + 1) * tp * feats)
        top, bottom = terms[:half_rows, at], terms[half_rows:, at]
        to = c * half_kv + i
        for to_c, message in (
            (0, jnp.where(low, top, halves_swapped(bottom))),
            (1, jnp.where(low, halves_swapped(top), bottom)),
        ):
            n = 2 * i + to_c
            terms_out[n] = message.astype(BF16)
            copy = remote(terms_out.at[n], terms_in.at[z], term_send.at[0], term_recv.at[0], to, to_c)
            to_self = jnp.logical_and(to == z, to_c == c)

            @pl.when(jnp.logical_not(to_self))
            def _(copy=copy):
                copy.start()

            @pl.when(to_self)
            def _(n=n):
                terms_in[z] = terms_out[n]

    remote(wide_out, wide_in, pair_send.at[6], pair_recv.at[6], z, other).wait_send()
    wait_others(mid, mid_send.at[0], False)
    wait_others(terms_in, term_recv.at[0])
    summed = middle.astype(F32) + jnp.sum(terms_in[...].astype(F32), axis=0)
    result[pl.ds(0, half_rows), :] = summed[:, :feats].astype(BF16)
    result[pl.ds(half_rows, half_rows), :] = summed[:, feats:].astype(BF16)

    wait_others(terms_in, term_send.at[0], False)


def body(
    kv,
    tp,
    tokens,
    past_state,
    mix_gain,
    w_query,
    w_forget,
    w_value,
    w_gate_out,
    floor_logits,
    head_gain,
    w_out,
    mlp_gain,
    w_gate,
    w_up,
    w_down,
):
    rows, feats = tokens.shape
    seqs, heads_local, dk, dv = past_state.shape
    units = w_gate.shape[1]
    group = heads_local * seqs
    channels = heads_local * dv
    half_cols = w_down.shape[1] // tp
    wide = -(-units // 128) * 128
    in_vmem = pl.BlockSpec(memory_space=pltpu.VMEM)
    dma = pltpu.SemaphoreType.DMA
    result, forget, value = pl.pallas_call(
        functools.partial(kernel, kv, tp),
        name="decode_step",
        out_shape=(
            jax.ShapeDtypeStruct((rows, feats), BF16),
            jax.ShapeDtypeStruct((seqs, heads_local, dk), F32),
            jax.ShapeDtypeStruct((seqs, heads_local, dv), F32),
        ),
        in_specs=[pl.BlockSpec(memory_space=pltpu.HBM)] * 14,
        out_specs=(in_vmem, in_vmem, in_vmem),
        scratch_shapes=[
            pltpu.VMEM((rows, feats), BF16),
            pltpu.VMEM((1, tp * feats), F32),
            pltpu.VMEM((heads_local, dk), F32),
            pltpu.VMEM((1, dv), F32),
            pltpu.VMEM((kv, tp * feats), F32),
            pltpu.VMEM((rows // 2, 2 * feats), BF16),
            pltpu.VMEM((rows // 2, 2 * feats), BF16),
            pltpu.VMEM((4, *w_query.shape), BF16),
            pltpu.VMEM(past_state.shape, F32),
            pltpu.VMEM((2, feats, channels), BF16),
            pltpu.VMEM((4, units, half_cols), BF16),
            pltpu.VMEM((2, units, half_cols), BF16),
            pltpu.VMEM((group, dk), F32),
            pltpu.VMEM((group, dv), F32),
            pltpu.VMEM((kv, 4 * group, dk), BF16),
            pltpu.VMEM((kv, 4 * group, dk), BF16),
            pltpu.VMEM((kv, seqs, dk), F32),
            pltpu.VMEM((kv, seqs, dk), F32),
            pltpu.VMEM((4 * group + 8, dk), F32),
            pltpu.VMEM((kv, 4 * group, dk), BF16),
            pltpu.VMEM((kv, seqs, dk), F32),
            pltpu.VMEM((4 * group + 8, dk), F32),
            pltpu.VMEM((4 * group + 8, dk), F32),
            pltpu.VMEM((group, dv), BF16),
            pltpu.VMEM((kv, group, dv), BF16),
            pltpu.VMEM((rows // 2, 2 * feats), F32),
            pltpu.VMEM((rows // 2, 2 * feats), F32),
            pltpu.VMEM((rows // 2, 2 * feats), BF16),
            pltpu.VMEM((kv, rows // 2, 2 * feats), BF16),
            pltpu.VMEM((5, rows, wide), F32),
            pltpu.VMEM((5, rows, wide), F32),
            pltpu.VMEM((kv, rows // 2, 2 * feats), BF16),
            pltpu.VMEM((kv, rows // 2, 2 * feats), BF16),
            dma((11,)),
            dma((7,)),
            dma((7,)),
            *[dma((2,))] * 2,
            *[dma((1,))] * 12,
            pltpu.SemaphoreType.REGULAR,
            pltpu.SemaphoreType.REGULAR((kv,)),
        ],
        compiler_params=pltpu.CompilerParams(
            collective_id=0, has_side_effects=True, vmem_limit_bytes=VMEM_BYTES
        ),
    )(*hbm(
        tokens,
        past_state,
        mix_gain.reshape(1, -1),
        w_query,
        w_forget,
        w_value,
        w_gate_out,
        floor_logits.reshape(heads_local, dk),
        head_gain.reshape(1, -1),
        w_out.T,
        mlp_gain.reshape(kv, tp * feats),
        w_gate.T,
        w_up.T,
        w_down,
    ))
    value = value[:, :, None, :]
    return result, value + forget[..., None] * (past_state - value)


def solution(mesh):
    placed = (
        P(("grp", "dp"), ("kv", "tp")),
        P(("grp", "dp", "kv"), "tp", None, None),
        P("kv"),
        P("kv", "tp"),
        P("kv", "tp"),
        P("kv", "tp"),
        P("kv", "tp"),
        P("tp"),
        P(),
        P(None, ("kv", "tp")),
        P(),
        P(None, ("kv", "tp")),
        P(None, ("kv", "tp")),
        P(("kv", "tp"), None),
    )
    return jax.shard_map(
        functools.partial(body, mesh.shape["kv"], mesh.shape["tp"]),
        mesh=mesh,
        in_specs=placed,
        out_specs=(P(("grp", "dp"), ("kv", "tp")), P(("grp", "dp", "kv"), "tp", None, None)),
        check_vma=False,
    )
```

```python
import functools

import jax
import jax.numpy as jnp
from jax import lax
from jax.experimental import pallas as pl
from jax.experimental.pallas import tpu as pltpu
from jax.sharding import PartitionSpec as P

MESH = pl.DeviceIdType.MESH
EPS = 1e-06
VMEM_BYTES = 48 * 1024 * 1024
F32 = jnp.float32
BF16 = jnp.bfloat16


def dot(a, b):
    return jnp.dot(a, b, preferred_element_type=F32)


def dot_t(a, b):
    return lax.dot_general(a, b, (((1,), (1,)), ((), ())), preferred_element_type=F32)


def hbm(*arrays):
    return [pltpu.with_memory_space_constraint(a, pltpu.HBM) for a in arrays]


def packed(x):
    half = x.shape[0] // 2
    return jnp.concatenate([x[:half], x[half:]], axis=1)


def halves_swapped(x):
    return pltpu.roll(x, x.shape[1] // 2, 1)


def kernel(
    kv,
    tp,
    tokens_hbm,
    past_state,
    mix_gain_hbm,
    w_query,
    w_forget,
    w_value,
    w_gate_out,
    floor_hbm,
    head_gain_hbm,
    w_out,
    mlp_gain_hbm,
    w_gate,
    w_up,
    w_down,
    result,
    forget_out,
    value_out,
    tokens,
    mix_gain,
    floor_logits,
    head_gain,
    mlp_gain,
    tok_own,
    tok_other,
    proj_w,
    state,
    out_w,
    mlp_w,
    down_w,
    floors,
    heads,
    chunk_out,
    chunk_in,
    total,
    relay_in,
    relayed_out,
    relayed_in,
    mix_own,
    mix,
    part_out,
    part_in,
    mid_own,
    mid,
    wide_out,
    wide_in,
    terms_out,
    terms_in,
    local_sem,
    pair_send,
    pair_recv,
    rs_send,
    rs_recv,
    mix_send,
    mix_recv,
    mid_send,
    mid_recv,
    term_send,
    term_recv,
    relay_recv,
    relayed_send,
    relayed_recv,
    pair_in,
    ready,
):
    z = lax.axis_index("kv")
    c = lax.axis_index("tp")
    other = 1 - c
    rows, feats = tokens.shape
    seqs, heads_local, dk, dv = past_state.shape
    units = w_gate.shape[0]
    group = heads_local * seqs
    half_rows = rows // 2
    width = kv * tp * feats
    half_kv = kv // tp
    half_cols = half_kv * tp * feats

    def local(src, dst, i):
        copy = pltpu.make_async_copy(src, dst, local_sem.at[i])
        copy.start()
        return copy

    def remote(src, dst, send, recv, to_z, to_c):
        return pltpu.make_async_remote_copy(
            src_ref=src,
            dst_ref=dst,
            send_sem=send,
            recv_sem=recv,
            device_id={"kv": to_z, "tp": to_c},
            device_id_type=MESH,
        )

    def peer(d):
        return lax.rem(z + d, kv)

    def place(w):
        return jnp.where(w == 0, kv - 2, jnp.where(w == kv - 1, kv - 1, w - 1))

    order = [*range(1, kv - 1), 0, kv - 1]
    last = kv - 1
    near_last = [w for w in range(kv - tp - 2, kv - 1)]
    relays = {0: kv // 4, last: near_last[0] - 1}
    behind = near_last[0] - 1
    listeners = {0: [relays[0], *near_last], last: [relays[last], *near_last, 0]}
    far_first = sorted(range(1, kv), key=lambda d: -min(d, kv - d))

    def wait_all(buffer, count, sem, received=True):
        part_of = buffer.at[pl.ds(0, count)]
        copy = remote(part_of, part_of, sem, sem, z, other)
        copy.wait_recv() if received else copy.wait_send()

    barrier = pltpu.get_barrier_semaphore()

    def signal(sem, to_z, to_c):
        pl.semaphore_signal(sem, inc=1, device_id={"kv": to_z, "tp": to_c}, device_id_type=MESH)

    @pl.when(c == 1)
    def _():
        signal(barrier, z, 0)

    tokens_copy = local(tokens_hbm, tokens, 2)
    gain_copy = local(mix_gain_hbm, mix_gain, 3)
    for i, w in enumerate((w_query, w_forget, w_value, w_gate_out)):
        local(w, proj_w.at[i], 0)
    state_copy = local(past_state, state, 1)
    small_copies = [
        local(floor_hbm, floor_logits, 4),
        local(head_gain_hbm, head_gain, 5),
        local(mlp_gain_hbm, mlp_gain, 6),
    ]
    half_of = pl.ds(pl.multiple_of(c * half_cols, half_cols), half_cols)
    half_of_other = pl.ds(pl.multiple_of(other * half_cols, half_cols), half_cols)
    weight_copies = [
        local(w_out.at[:, half_of_other], out_w.at[0], 7),
        local(w_gate.at[:, half_of], mlp_w.at[0], 8),
        local(w_up.at[:, half_of], mlp_w.at[1], 9),
        local(w_down.at[:, half_of], down_w.at[0], 10),
    ]

    @pl.when(c == 0)
    def _():
        pl.semaphore_wait(barrier, 1)
        signal(pair_in, z, 1)

    @pl.when(c == 1)
    def _():
        pl.semaphore_wait(pair_in, 1)
        for w in order:

            @pl.when(place(z) < place(w))
            def _(w=w):
                signal(barrier, w, 1)

    @pl.when(c == 1)
    def _():
        @pl.when(place(z) > 0)
        def _():
            pl.semaphore_wait(barrier, place(z))

        signal(pair_in, z, 0)

    @pl.when(c == 0)
    def _():
        pl.semaphore_wait(pair_in, 1)

    for special, told in listeners.items():

        @pl.when(z == special)
        def _(special=special, told=told):
            for w in told:
                if order.index(w) < order.index(special):
                    signal(ready.at[special], w, c)

    for d in far_first:
        to = peer(d)

        @pl.when((place(to) < place(z)) & (place(z) < kv - 2))
        def _(to=to):
            signal(ready.at[z], to, c)

    tokens_copy.wait()
    own = tokens[...].astype(F32)
    tok_own[...] = packed(own).astype(BF16)
    tok = remote(tok_own, tok_other, pair_send.at[0], pair_recv.at[0], z, other)
    tok.start()

    r = lax.broadcasted_iota(jnp.int32, (kv * group, kv * group), 0)
    col = lax.broadcasted_iota(jnp.int32, (kv * group, kv * group), 1)
    s_of = lax.rem(r, seqs)
    to_chunks = lax.rem(r // seqs, heads_local) * (kv * seqs) + (r // group) * seqs + s_of
    spread = jnp.where(col == to_chunks, 1.0, 0.0).astype(BF16)
    to_heads = lax.rem(r // seqs, kv) * group + (r // (kv * seqs)) * seqs + s_of
    gather = jnp.where(col == to_heads, 1.0, 0.0).astype(BF16)

    lane = lax.broadcasted_iota(jnp.int32, (1, tp * feats), 1)
    low = lane < feats
    own_twice = jnp.concatenate([own, own], axis=1)
    tok.wait_recv()
    got = tok_other[...].astype(F32)
    got_swapped = halves_swapped(got)
    got_twice = jnp.concatenate(
        [jnp.where(low, got, got_swapped), jnp.where(low, got_swapped, got)], axis=0
    )
    mine = lax.broadcasted_iota(jnp.int32, (rows, tp * feats), 1) // feats == c
    block = jnp.where(mine, own_twice, got_twice)
    squares = jnp.sum(block * block, axis=1, keepdims=True)
    high = squares.astype(BF16).astype(F32)
    parts = jnp.where(low, high, squares - high).reshape(kv, seqs, dk)
    chunk_out[:, pl.ds(4 * group, seqs), :] = parts.astype(BF16)
    gain_copy.wait()
    gained = (block * mix_gain[...]).astype(BF16)
    def chunk_copy(to):
        return remote(chunk_out.at[to], chunk_in.at[z], rs_send.at[0], rs_recv.at[0], to, c)

    def chunk_to_relay(special):
        return remote(
            chunk_out.at[special], relay_in.at[z - 1], rs_send.at[0], relay_recv.at[0], relays[special], c
        )

    pltpu.make_async_copy(proj_w, proj_w, local_sem.at[0]).wait()
    products = [dot(gained, proj_w[i]).astype(BF16) for i in range(4)]
    for i in (0, 2):
        stack = jnp.concatenate(
            [
                jnp.concatenate([p[:, h * dk : (h + 1) * dk] for p in products[i : i + 2]], axis=1)
                for h in range(heads_local)
            ],
            axis=0,
        )
        ordered = dot(spread, stack).astype(BF16)
        for j in range(2):
            chunk_out[:, pl.ds((i + j) * group, group), :] = ordered[:, j * dk : (j + 1) * dk].reshape(
                kv, group, dk
            )

    for d in far_first:
        to = peer(d)

        @pl.when(place(to) < place(z))
        def _(to=to):
            chunk_copy(to).start()

    for special, relay in relays.items():

        @pl.when((z > relay) & (z <= behind))
        def _(special=special):
            chunk_to_relay(special).start()

    swaps = [
        remote(w_out.at[:, half_of], out_w.at[1], pair_send.at[1], pair_recv.at[1], z, other),
        remote(w_gate.at[:, half_of_other], mlp_w.at[2], pair_send.at[2], pair_recv.at[2], z, other),
        remote(w_up.at[:, half_of_other], mlp_w.at[3], pair_send.at[3], pair_recv.at[3], z, other),
        remote(w_down.at[:, half_of_other], down_w.at[1], pair_send.at[4], pair_recv.at[4], z, other),
    ]
    is_special = (z == 0) | (z == last)

    @pl.when(jnp.logical_not(is_special))
    def _():
        for s in swaps:
            s.start()


    chunk_in[z] = chunk_out[z]
    for copy in small_copies:
        copy.wait()
    lower_in = jax.nn.sigmoid(floor_logits[...])
    for h in range(heads_local):
        floors[pl.ds(h * seqs, seqs), :] = jnp.broadcast_to(lower_in[h : h + 1], (seqs, dk))

    for w in order[:-2]:

        @pl.when(place(z) < place(w))
        def _(w=w):
            pl.semaphore_wait(ready.at[w], 1)
            chunk_copy(w).start()
            for special, relay in relays.items():
                if relay == w:
                    chunk_to_relay(special).start()

    for special, relay in relays.items():
        forward = remote(relayed_out, relayed_in, relayed_send.at[0], relayed_recv.at[0], special, c)

        @pl.when(z == relay)
        def _(special=special, forward=forward):
            wait_all(relay_in, behind - 1, relay_recv.at[0])
            relay_in[z - 1] = chunk_out[special]
            sums = relay_in[0].astype(F32)
            for i in range(1, behind):
                sums = sums + relay_in[i].astype(F32)
            relayed_out[...] = sums
            pl.semaphore_wait(ready.at[special], 1)
            forward.start()

        for w in listeners[special]:
            if w != relay and order.index(w) < order.index(special):

                @pl.when(z == w)
                def _(special=special):
                    pl.semaphore_wait(ready.at[special], 1)
                    chunk_copy(special).start()

    def add_up(slots):
        sums = chunk_in[slots[0]].astype(F32)
        for w in slots[1:]:
            sums = sums + chunk_in[w].astype(F32)
        return sums

    direct = [*near_last, 0, last]

    @pl.when(jnp.logical_not(is_special))
    def _():
        wait_all(chunk_in, kv - 1, rs_recv.at[0])
        total[...] = add_up(order)

    @pl.when(is_special)
    def _():
        wait_all(chunk_in, len(direct) - 1, rs_recv.at[0])
        remote(relayed_out, relayed_in, relayed_send.at[0], relayed_recv.at[0], z, other).wait_recv()
        total[...] = add_up(direct) + relayed_in[...]
        for s in swaps:
            s.start()

    total_sq = total[pl.ds(4 * group, seqs), :]
    total_sq = total_sq + halves_swapped(total_sq)
    scale_s = lax.rsqrt(total_sq / width + EPS)
    row_of = lax.broadcasted_iota(jnp.int32, (group, dk), 0)
    scale = jnp.broadcast_to(scale_s[0:1], (group, dk))
    for s in range(1, seqs):
        scale = jnp.where(lax.rem(row_of, seqs) == s, jnp.broadcast_to(scale_s[s : s + 1], (group, dk)), scale)
    query = total[pl.ds(0, group), :] * scale
    forget_pre = total[pl.ds(group, group), :] * scale
    value = total[pl.ds(2 * group, group), :] * scale
    gate_pre = total[pl.ds(3 * group, group), :] * scale
    lower = floors[...]
    forget = lower + (1.0 - lower) * jax.nn.sigmoid(forget_pre)
    activ = query * jax.nn.sigmoid(query)
    columns = jnp.concatenate([forget, activ, jnp.zeros((dk - 2 * group, dk), F32)], axis=0).T

    state_copy.wait()
    for h in range(heads_local):
        for s in range(seqs):
            i = h * seqs + s
            v_row = value[i : i + 1]
            f_col = columns[:, i : i + 1]
            q_col = columns[:, group + i : group + i + 1]
            new = v_row + f_col * (state[s, h] - v_row)
            heads[pl.ds(i, 1), :] = jnp.sum(new * q_col, axis=0, keepdims=True)

    head_out = heads[...]
    normed = head_out * lax.rsqrt(jnp.mean(head_out * head_out, axis=1, keepdims=True) + EPS)
    mixed = normed * head_gain[...] * (gate_pre * jax.nn.sigmoid(gate_pre))
    mix_own[...] = mixed.astype(BF16)
    for d in far_first:
        remote(mix_own, mix.at[z], mix_send.at[0], mix_recv.at[0], peer(d), other).start()
    remote(mix_own, mix.at[z], mix_send.at[0], mix_recv.at[0], z, other).start()
    tok.wait_send()
    is_relay = (z == relays[0]) | (z == relays[last])

    @pl.when(jnp.logical_not(is_relay))
    def _():
        wait_all(chunk_in, kv - 1, rs_send.at[0], False)

    @pl.when(is_relay)
    def _():
        wait_all(chunk_in, kv - 2, rs_send.at[0], False)
        remote(relayed_out, relayed_in, relayed_send.at[0], relayed_recv.at[0], z, other).wait_send()

    for h in range(heads_local):
        for s in range(seqs):
            i = h * seqs + s
            forget_out[s, pl.ds(h, 1), :] = forget[i : i + 1]
            value_out[s, pl.ds(h, 1), :] = value[i : i + 1]
    weight_copies[0].wait()
    swaps[0].wait_recv()
    wait_all(mix, kv, mix_recv.at[0])
    by_head = dot(gather, mix[...].reshape(kv * group, dv)).astype(BF16)
    every = jnp.concatenate([by_head[h * rows : (h + 1) * rows] for h in range(heads_local)], axis=1)
    part_out[...] = packed(dot_t(every, out_w[1]))
    part = remote(part_out, part_in, pair_send.at[5], pair_recv.at[5], z, other)
    part.start()
    kept = packed(dot_t(every, out_w[0])) + packed(own)
    part.wait_recv()
    middle = (kept + part_in[...]).astype(BF16)
    mid_own[...] = middle
    half = z // half_kv
    half_z = lax.rem(z, half_kv)
    kept_here = half == c
    for d in far_first:
        remote(mid_own, mid.at[half_z * tp + c], mid_send.at[0], mid_recv.at[0], peer(d), half).start()

    @pl.when(kept_here)
    def _():
        mid[half_z * tp + c] = middle

    @pl.when(jnp.logical_not(kept_here))
    def _():
        remote(mid_own, mid.at[half_z * tp + c], mid_send.at[0], mid_recv.at[0], z, half).start()

    part.wait_send()
    wait_all(mix, kv, mix_send.at[0], False)
    for copy in swaps:
        copy.wait_send()
    gain = mlp_gain[pl.ds(pl.multiple_of(c * half_kv, half_kv), half_kv), :]
    for w in weight_copies[1:]:
        w.wait()
    for s in swaps[1:]:
        s.wait_recv()
    def wait_others(buffer, sem, received=True):
        @pl.when(kept_here)
        def _():
            wait_all(buffer, kv - 1, sem, received)

        @pl.when(jnp.logical_not(kept_here))
        def _():
            wait_all(buffer, kv, sem, received)

    wait_others(mid, mid_recv.at[0])
    tops, bottoms = [], []
    squares = jnp.zeros((half_rows, tp * feats), F32)
    for i in range(half_kv):
        a = mid[tp * i].astype(F32)
        b = mid[tp * i + 1].astype(F32)
        squares = squares + a * a + b * b
        g = gain[i : i + 1]
        tops.append((jnp.where(low, a, halves_swapped(b)) * g).astype(BF16))
        bottoms.append((jnp.where(low, halves_swapped(a), b) * g).astype(BF16))
    features = jnp.concatenate(
        [jnp.concatenate(tops, axis=1), jnp.concatenate(bottoms, axis=1)], axis=0
    )
    sq_top = jnp.sum(jnp.where(low, squares, 0.0), axis=1, keepdims=True)
    sq_bottom = jnp.sum(jnp.where(low, 0.0, squares), axis=1, keepdims=True)
    sq_mid = jnp.concatenate([sq_top, sq_bottom], axis=0)
    wide_out[4, :, :] = jnp.broadcast_to(sq_mid, wide_out.shape[1:])
    wides = [
        remote(wide_out.at[i], wide_in.at[i], pair_send.at[6], pair_recv.at[6], z, other) for i in range(5)
    ]
    wides[4].start()
    sums = []
    for i in range(4):
        sums.append(dot_t(features, mlp_w[i]))
        wide_out[i, :, pl.ds(0, units)] = sums[i]
        wides[i].start()
    remote(wide_out, wide_in, pair_send.at[6], pair_recv.at[6], z, other).wait_recv()
    mlp_scale = lax.rsqrt((sq_mid + wide_in[4, :, 0:1]) / width + EPS)
    terms = None
    for i in range(2):
        gate = (sums[2 * i] + wide_in[2 - 2 * i, :, pl.ds(0, units)]) * mlp_scale
        upward = (sums[2 * i + 1] + wide_in[3 - 2 * i, :, pl.ds(0, units)]) * mlp_scale
        hidden = (gate * jax.nn.sigmoid(gate) * upward).astype(BF16)
        term = dot(hidden, down_w[i])
        terms = term if terms is None else terms + term

    for i in range(half_kv):
        at = slice(i * tp * feats, (i + 1) * tp * feats)
        top, bottom = terms[:half_rows, at], terms[half_rows:, at]
        to = c * half_kv + i
        for to_c, message in (
            (0, jnp.where(low, top, halves_swapped(bottom))),
            (1, jnp.where(low, halves_swapped(top), bottom)),
        ):
            n = 2 * i + to_c
            terms_out[n] = message.astype(BF16)
            copy = remote(terms_out.at[n], terms_in.at[z], term_send.at[0], term_recv.at[0], to, to_c)
            to_self = jnp.logical_and(to == z, to_c == c)

            @pl.when(jnp.logical_not(to_self))
            def _(copy=copy):
                copy.start()

            @pl.when(to_self)
            def _(n=n):
                terms_in[z] = terms_out[n]

    remote(wide_out, wide_in, pair_send.at[6], pair_recv.at[6], z, other).wait_send()
    wait_others(mid, mid_send.at[0], False)
    wait_others(terms_in, term_recv.at[0])
    summed = middle.astype(F32) + jnp.sum(terms_in[...].astype(F32), axis=0)
    result[pl.ds(0, half_rows), :] = summed[:, :feats].astype(BF16)
    result[pl.ds(half_rows, half_rows), :] = summed[:, feats:].astype(BF16)

    wait_others(terms_in, term_send.at[0], False)


def body(
    kv,
    tp,
    tokens,
    past_state,
    mix_gain,
    w_query,
    w_forget,
    w_value,
    w_gate_out,
    floor_logits,
    head_gain,
    w_out,
    mlp_gain,
    w_gate,
    w_up,
    w_down,
):
    rows, feats = tokens.shape
    seqs, heads_local, dk, dv = past_state.shape
    units = w_gate.shape[1]
    group = heads_local * seqs
    channels = heads_local * dv
    half_cols = w_down.shape[1] // tp
    wide = -(-units // 128) * 128
    in_vmem = pl.BlockSpec(memory_space=pltpu.VMEM)
    dma = pltpu.SemaphoreType.DMA
    result, forget, value = pl.pallas_call(
        functools.partial(kernel, kv, tp),
        name="decode_step",
        out_shape=(
            jax.ShapeDtypeStruct((rows, feats), BF16),
            jax.ShapeDtypeStruct((seqs, heads_local, dk), F32),
            jax.ShapeDtypeStruct((seqs, heads_local, dv), F32),
        ),
        in_specs=[pl.BlockSpec(memory_space=pltpu.HBM)] * 14,
        out_specs=(in_vmem, in_vmem, in_vmem),
        scratch_shapes=[
            pltpu.VMEM((rows, feats), BF16),
            pltpu.VMEM((1, tp * feats), F32),
            pltpu.VMEM((heads_local, dk), F32),
            pltpu.VMEM((1, dv), F32),
            pltpu.VMEM((kv, tp * feats), F32),
            pltpu.VMEM((rows // 2, 2 * feats), BF16),
            pltpu.VMEM((rows // 2, 2 * feats), BF16),
            pltpu.VMEM((4, *w_query.shape), BF16),
            pltpu.VMEM(past_state.shape, F32),
            pltpu.VMEM((2, feats, channels), BF16),
            pltpu.VMEM((4, units, half_cols), BF16),
            pltpu.VMEM((2, units, half_cols), BF16),
            pltpu.VMEM((group, dk), F32),
            pltpu.VMEM((group, dv), F32),
            pltpu.VMEM((kv, 4 * group + seqs, dk), BF16),
            pltpu.VMEM((kv, 4 * group + seqs, dk), BF16),
            pltpu.VMEM((4 * group + seqs, dk), F32),
            pltpu.VMEM((kv, 4 * group + seqs, dk), BF16),
            pltpu.VMEM((4 * group + seqs, dk), F32),
            pltpu.VMEM((4 * group + seqs, dk), F32),
            pltpu.VMEM((group, dv), BF16),
            pltpu.VMEM((kv, group, dv), BF16),
            pltpu.VMEM((rows // 2, 2 * feats), F32),
            pltpu.VMEM((rows // 2, 2 * feats), F32),
            pltpu.VMEM((rows // 2, 2 * feats), BF16),
            pltpu.VMEM((kv, rows // 2, 2 * feats), BF16),
            pltpu.VMEM((5, rows, wide), F32),
            pltpu.VMEM((5, rows, wide), F32),
            pltpu.VMEM((kv, rows // 2, 2 * feats), BF16),
            pltpu.VMEM((kv, rows // 2, 2 * feats), BF16),
            dma((11,)),
            dma((7,)),
            dma((7,)),
            *[dma((1,))] * 11,
            pltpu.SemaphoreType.REGULAR,
            pltpu.SemaphoreType.REGULAR((kv,)),
        ],
        compiler_params=pltpu.CompilerParams(
            collective_id=0, has_side_effects=True, vmem_limit_bytes=VMEM_BYTES
        ),
    )(*hbm(
        tokens,
        past_state,
        mix_gain.reshape(1, -1),
        w_query,
        w_forget,
        w_value,
        w_gate_out,
        floor_logits.reshape(heads_local, dk),
        head_gain.reshape(1, -1),
        w_out.T,
        mlp_gain.reshape(kv, tp * feats),
        w_gate.T,
        w_up.T,
        w_down,
    ))
    value = value[:, :, None, :]
    return result, value + forget[..., None] * (past_state - value)


def solution(mesh):
    placed = (
        P(("grp", "dp"), ("kv", "tp")),
        P(("grp", "dp", "kv"), "tp", None, None),
        P("kv"),
        P("kv", "tp"),
        P("kv", "tp"),
        P("kv", "tp"),
        P("kv", "tp"),
        P("tp"),
        P(),
        P(None, ("kv", "tp")),
        P(),
        P(None, ("kv", "tp")),
        P(None, ("kv", "tp")),
        P(("kv", "tp"), None),
    )
    return jax.shard_map(
        functools.partial(body, mesh.shape["kv"], mesh.shape["tp"]),
        mesh=mesh,
        in_specs=placed,
        out_specs=(P(("grp", "dp"), ("kv", "tp")), P(("grp", "dp", "kv"), "tp", None, None)),
        check_vma=False,
    )
```

```python
import functools

import jax
import jax.numpy as jnp
from jax import lax
from jax.experimental import pallas as pl
from jax.experimental.pallas import tpu as pltpu
from jax.sharding import PartitionSpec as P

MESH = pl.DeviceIdType.MESH
EPS = 1e-06
VMEM_BYTES = 48 * 1024 * 1024
F32 = jnp.float32
BF16 = jnp.bfloat16


def dot(a, b):
    return jnp.dot(a, b, preferred_element_type=F32)


def dot_t(a, b):
    return lax.dot_general(a, b, (((1,), (1,)), ((), ())), preferred_element_type=F32)


def hbm(*arrays):
    return [pltpu.with_memory_space_constraint(a, pltpu.HBM) for a in arrays]


def packed(x):
    half = x.shape[0] // 2
    return jnp.concatenate([x[:half], x[half:]], axis=1)


def halves_swapped(x):
    return pltpu.roll(x, x.shape[1] // 2, 1)


def kernel(
    kv,
    tp,
    tokens_hbm,
    past_state,
    mix_gain_hbm,
    w_query,
    w_forget,
    w_value,
    w_gate_out,
    floor_hbm,
    head_gain_hbm,
    w_out,
    mlp_gain_hbm,
    w_gate,
    w_up,
    w_down,
    result,
    new_state,
    tokens,
    mix_gain,
    floor_logits,
    head_gain,
    mlp_gain,
    tok_own,
    tok_other,
    proj_w,
    state,
    out_w,
    mlp_w,
    down_w,
    floors,
    heads,
    chunk_out,
    chunk_in,
    sq_out,
    sq_in,
    total,
    relay_in,
    relay_sq_in,
    relayed_out,
    relayed_in,
    mix_own,
    mix,
    part_out,
    part_in,
    mid_own,
    mid,
    wide_out,
    wide_in,
    terms_out,
    terms_in,
    local_sem,
    pair_send,
    pair_recv,
    rs_send,
    rs_recv,
    sq_send,
    sq_recv,
    mix_send,
    mix_recv,
    mid_send,
    mid_recv,
    term_send,
    term_recv,
    relay_recv,
    relay_sq_recv,
    relayed_send,
    relayed_recv,
    pair_in,
    ready,
):
    z = lax.axis_index("kv")
    c = lax.axis_index("tp")
    other = 1 - c
    rows, feats = tokens.shape
    seqs, heads_local, dk, dv = past_state.shape
    units = w_gate.shape[0]
    group = heads_local * seqs
    half_rows = rows // 2
    width = kv * tp * feats
    half_kv = kv // tp
    half_cols = half_kv * tp * feats

    def local(src, dst, i):
        copy = pltpu.make_async_copy(src, dst, local_sem.at[i])
        copy.start()
        return copy

    def remote(src, dst, send, recv, to_z, to_c):
        return pltpu.make_async_remote_copy(
            src_ref=src,
            dst_ref=dst,
            send_sem=send,
            recv_sem=recv,
            device_id={"kv": to_z, "tp": to_c},
            device_id_type=MESH,
        )

    def peer(d):
        return lax.rem(z + d, kv)

    def place(w):
        return jnp.where(w == 0, kv - 2, jnp.where(w == kv - 1, kv - 1, w - 1))

    order = [*range(1, kv - 1), 0, kv - 1]
    last = kv - 1
    near_last = [w for w in range(kv - tp - 2, kv - 1)]
    relays = {0: kv // 4, last: near_last[0] - 1}
    behind = near_last[0] - 1
    listeners = {0: [relays[0], *near_last], last: [relays[last], *near_last, 0]}
    far_first = sorted(range(1, kv), key=lambda d: -min(d, kv - d))

    def wait_all(buffer, count, sem, received=True):
        part_of = buffer.at[pl.ds(0, count)]
        copy = remote(part_of, part_of, sem, sem, z, other)
        copy.wait_recv() if received else copy.wait_send()

    barrier = pltpu.get_barrier_semaphore()

    def signal(sem, to_z, to_c):
        pl.semaphore_signal(sem, inc=1, device_id={"kv": to_z, "tp": to_c}, device_id_type=MESH)

    @pl.when(c == 1)
    def _():
        signal(barrier, z, 0)

    tokens_copy = local(tokens_hbm, tokens, 2)
    gain_copy = local(mix_gain_hbm, mix_gain, 3)
    for i, w in enumerate((w_query, w_forget, w_value, w_gate_out)):
        local(w, proj_w.at[i], 0)
    state_copy = local(past_state, state, 1)
    small_copies = [
        local(floor_hbm, floor_logits, 4),
        local(head_gain_hbm, head_gain, 5),
        local(mlp_gain_hbm, mlp_gain, 6),
    ]
    half_of = pl.ds(pl.multiple_of(c * half_cols, half_cols), half_cols)
    half_of_other = pl.ds(pl.multiple_of(other * half_cols, half_cols), half_cols)
    weight_copies = [
        local(w_out.at[:, half_of_other], out_w.at[0], 7),
        local(w_gate.at[:, half_of], mlp_w.at[0], 8),
        local(w_up.at[:, half_of], mlp_w.at[1], 9),
        local(w_down.at[:, half_of], down_w.at[0], 10),
    ]

    @pl.when(c == 0)
    def _():
        pl.semaphore_wait(barrier, 1)
        signal(pair_in, z, 1)

    @pl.when(c == 1)
    def _():
        pl.semaphore_wait(pair_in, 1)
        for w in order:

            @pl.when(place(z) < place(w))
            def _(w=w):
                signal(barrier, w, 1)

    def count_and_tell():
        @pl.when(c == 1)
        def _():
            @pl.when(place(z) > 0)
            def _():
                pl.semaphore_wait(barrier, place(z))

            signal(pair_in, z, 0)

        @pl.when(c == 0)
        def _():
            pl.semaphore_wait(pair_in, 1)

        for special, told in listeners.items():

            @pl.when(z == special)
            def _(special=special, told=told):
                for w in told:
                    if order.index(w) < order.index(special):
                        signal(ready.at[special], w, c)

        for d in far_first:
            to = peer(d)

            @pl.when((place(to) < place(z)) & (place(z) < kv - 2))
            def _(to=to):
                signal(ready.at[z], to, c)

    @pl.when(z != last)
    def _():
        count_and_tell()

    tokens_copy.wait()
    own = tokens[...].astype(F32)
    tok_own[...] = packed(own).astype(BF16)
    tok = remote(tok_own, tok_other, pair_send.at[0], pair_recv.at[0], z, other)
    tok.start()

    r = lax.broadcasted_iota(jnp.int32, (kv * group, kv * group), 0)
    col = lax.broadcasted_iota(jnp.int32, (kv * group, kv * group), 1)
    s_of = lax.rem(r, seqs)
    to_chunks = lax.rem(r // seqs, heads_local) * (kv * seqs) + (r // group) * seqs + s_of
    spread = jnp.where(col == to_chunks, 1.0, 0.0).astype(BF16)
    to_heads = lax.rem(r // seqs, kv) * group + (r // (kv * seqs)) * seqs + s_of
    gather = jnp.where(col == to_heads, 1.0, 0.0).astype(BF16)

    lane = lax.broadcasted_iota(jnp.int32, (1, tp * feats), 1)
    low = lane < feats
    own_twice = jnp.concatenate([own, own], axis=1)
    tok.wait_recv()

    @pl.when(z == last)
    def _():
        count_and_tell()

    got = tok_other[...].astype(F32)
    got_swapped = halves_swapped(got)
    got_twice = jnp.concatenate(
        [jnp.where(low, got, got_swapped), jnp.where(low, got_swapped, got)], axis=0
    )
    mine = lax.broadcasted_iota(jnp.int32, (rows, tp * feats), 1) // feats == c
    block = jnp.where(mine, own_twice, got_twice)
    squares = jnp.sum(block * block, axis=1, keepdims=True)
    sq_out[...] = jnp.broadcast_to(squares, (rows, dk)).reshape(kv, seqs, dk)
    gain_copy.wait()
    gained = (block * mix_gain[...]).astype(BF16)
    def sq_copy(to):
        return remote(sq_out.at[to], sq_in.at[z], sq_send.at[0], sq_recv.at[0], to, c)

    def chunk_copy(to):
        return remote(chunk_out.at[to], chunk_in.at[z], rs_send.at[0], rs_recv.at[0], to, c)

    def sq_to_relay(special):
        return remote(
            sq_out.at[special], relay_sq_in.at[z - 1], sq_send.at[0], relay_sq_recv.at[0], relays[special], c
        )

    def chunk_to_relay(special):
        return remote(
            chunk_out.at[special], relay_in.at[z - 1], rs_send.at[0], relay_recv.at[0], relays[special], c
        )

    for d in far_first:
        to = peer(d)

        @pl.when(place(to) < place(z))
        def _(to=to):
            sq_copy(to).start()

    for special, relay in relays.items():

        @pl.when((z > relay) & (z <= behind))
        def _(special=special):
            sq_to_relay(special).start()

    pltpu.make_async_copy(proj_w, proj_w, local_sem.at[0]).wait()
    products = [dot(gained, proj_w[i]).astype(BF16) for i in range(4)]
    for i in (0, 2):
        stack = jnp.concatenate(
            [
                jnp.concatenate([p[:, h * dk : (h + 1) * dk] for p in products[i : i + 2]], axis=1)
                for h in range(heads_local)
            ],
            axis=0,
        )
        ordered = dot(spread, stack).astype(BF16)
        for j in range(2):
            chunk_out[:, pl.ds((i + j) * group, group), :] = ordered[:, j * dk : (j + 1) * dk].reshape(
                kv, group, dk
            )

    for d in far_first:
        to = peer(d)

        @pl.when(place(to) < place(z))
        def _(to=to):
            chunk_copy(to).start()

    for special, relay in relays.items():

        @pl.when((z > relay) & (z <= behind))
        def _(special=special):
            chunk_to_relay(special).start()

    swaps = [
        remote(w_out.at[:, half_of], out_w.at[1], pair_send.at[1], pair_recv.at[1], z, other),
        remote(w_gate.at[:, half_of_other], mlp_w.at[2], pair_send.at[2], pair_recv.at[2], z, other),
        remote(w_up.at[:, half_of_other], mlp_w.at[3], pair_send.at[3], pair_recv.at[3], z, other),
        remote(w_down.at[:, half_of_other], down_w.at[1], pair_send.at[4], pair_recv.at[4], z, other),
    ]
    is_special = (z == 0) | (z == last)

    @pl.when(jnp.logical_not(is_special))
    def _():
        for s in swaps:
            s.start()


    sq_in[z] = sq_out[z]
    chunk_in[z] = chunk_out[z]
    for copy in small_copies:
        copy.wait()
    lower_in = jax.nn.sigmoid(floor_logits[...])
    for h in range(heads_local):
        floors[pl.ds(h * seqs, seqs), :] = jnp.broadcast_to(lower_in[h : h + 1], (seqs, dk))

    for w in order[:-2]:

        @pl.when(place(z) < place(w))
        def _(w=w):
            pl.semaphore_wait(ready.at[w], 1)
            sq_copy(w).start()
            chunk_copy(w).start()
            for special, relay in relays.items():
                if relay == w:
                    sq_to_relay(special).start()
                    chunk_to_relay(special).start()

    for special, relay in relays.items():
        forward = remote(relayed_out, relayed_in, relayed_send.at[0], relayed_recv.at[0], special, c)

        @pl.when(z == relay)
        def _(special=special, forward=forward):
            wait_all(relay_sq_in, behind - 1, relay_sq_recv.at[0])
            wait_all(relay_in, behind - 1, relay_recv.at[0])
            relay_sq_in[z - 1] = sq_out[special]
            relay_in[z - 1] = chunk_out[special]
            sums = relay_in[0].astype(F32)
            squares = relay_sq_in[0]
            for i in range(1, behind):
                sums = sums + relay_in[i].astype(F32)
                squares = squares + relay_sq_in[i]
            relayed_out[pl.ds(0, 4 * group), :] = sums
            relayed_out[pl.ds(4 * group, seqs), :] = squares
            pl.semaphore_wait(ready.at[special], 1)
            forward.start()

        for w in listeners[special]:
            if w != relay and order.index(w) < order.index(special):

                @pl.when(z == w)
                def _(special=special):
                    pl.semaphore_wait(ready.at[special], 1)
                    sq_copy(special).start()
                    chunk_copy(special).start()

    def add_up(slots):
        sums = chunk_in[slots[0]].astype(F32)
        squares = sq_in[slots[0]]
        for w in slots[1:]:
            sums = sums + chunk_in[w].astype(F32)
            squares = squares + sq_in[w]
        return sums, squares

    is_special = (z == 0) | (z == last)

    @pl.when(jnp.logical_not(is_special))
    def _():
        wait_all(sq_in, kv - 1, sq_recv.at[0])
        wait_all(chunk_in, kv - 1, rs_recv.at[0])
        sums, squares = add_up(order)
        total[pl.ds(0, 4 * group), :] = sums
        total[pl.ds(4 * group, seqs), :] = squares

    @pl.when(is_special)
    def _():
        wait_all(sq_in, len(near_last) + 1, sq_recv.at[0])
        wait_all(chunk_in, len(near_last) + 1, rs_recv.at[0])
        sums, squares = add_up([*near_last, 0, last])
        remote(relayed_out, relayed_in, relayed_send.at[0], relayed_recv.at[0], z, other).wait_recv()
        total[pl.ds(0, 4 * group), :] = sums + relayed_in[pl.ds(0, 4 * group), :]
        total[pl.ds(4 * group, seqs), :] = squares + relayed_in[pl.ds(4 * group, seqs), :]
        for s in swaps:
            s.start()

    total_sq = total[pl.ds(4 * group, seqs), :]
    scale_s = lax.rsqrt(total_sq / width + EPS)
    row_of = lax.broadcasted_iota(jnp.int32, (group, dk), 0)
    scale = jnp.broadcast_to(scale_s[0:1], (group, dk))
    for s in range(1, seqs):
        scale = jnp.where(lax.rem(row_of, seqs) == s, jnp.broadcast_to(scale_s[s : s + 1], (group, dk)), scale)
    query = total[pl.ds(0, group), :] * scale
    forget_pre = total[pl.ds(group, group), :] * scale
    value = total[pl.ds(2 * group, group), :] * scale
    gate_pre = total[pl.ds(3 * group, group), :] * scale
    lower = floors[...]
    forget = lower + (1.0 - lower) * jax.nn.sigmoid(forget_pre)
    activ = query * jax.nn.sigmoid(query)
    columns = jnp.concatenate([forget, activ, jnp.zeros((dk - 2 * group, dk), F32)], axis=0).T

    state_copy.wait()
    for h in range(heads_local):
        for s in range(seqs):
            i = h * seqs + s
            v_row = value[i : i + 1]
            f_col = columns[:, i : i + 1]
            q_col = columns[:, group + i : group + i + 1]
            new = v_row + f_col * (state[s, h] - v_row)
            new_state[s, h] = new
            heads[pl.ds(i, 1), :] = jnp.sum(new * q_col, axis=0, keepdims=True)

    head_out = heads[...]
    normed = head_out * lax.rsqrt(jnp.mean(head_out * head_out, axis=1, keepdims=True) + EPS)
    mixed = normed * head_gain[...] * (gate_pre * jax.nn.sigmoid(gate_pre))
    mix_own[...] = mixed.astype(BF16)
    for d in far_first:
        remote(mix_own, mix.at[z], mix_send.at[0], mix_recv.at[0], peer(d), other).start()
    remote(mix_own, mix.at[z], mix_send.at[0], mix_recv.at[0], z, other).start()
    tok.wait_send()
    is_relay = (z == relays[0]) | (z == relays[last])

    @pl.when(jnp.logical_not(is_relay))
    def _():
        wait_all(sq_in, kv - 1, sq_send.at[0], False)
        wait_all(chunk_in, kv - 1, rs_send.at[0], False)

    @pl.when(is_relay)
    def _():
        wait_all(sq_in, kv - 2, sq_send.at[0], False)
        wait_all(chunk_in, kv - 2, rs_send.at[0], False)
        remote(relayed_out, relayed_in, relayed_send.at[0], relayed_recv.at[0], z, other).wait_send()

    weight_copies[0].wait()
    swaps[0].wait_recv()
    wait_all(mix, kv, mix_recv.at[0])
    by_head = dot(gather, mix[...].reshape(kv * group, dv)).astype(BF16)
    every = jnp.concatenate([by_head[h * rows : (h + 1) * rows] for h in range(heads_local)], axis=1)
    part_out[...] = packed(dot_t(every, out_w[1]))
    part = remote(part_out, part_in, pair_send.at[5], pair_recv.at[5], z, other)
    part.start()
    kept = packed(dot_t(every, out_w[0])) + packed(own)
    part.wait_recv()
    middle = (kept + part_in[...]).astype(BF16)
    mid_own[...] = middle
    half = z // half_kv
    half_z = lax.rem(z, half_kv)
    kept_here = half == c
    for d in far_first:
        remote(mid_own, mid.at[half_z * tp + c], mid_send.at[0], mid_recv.at[0], peer(d), half).start()

    @pl.when(kept_here)
    def _():
        mid[half_z * tp + c] = middle

    @pl.when(jnp.logical_not(kept_here))
    def _():
        remote(mid_own, mid.at[half_z * tp + c], mid_send.at[0], mid_recv.at[0], z, half).start()

    part.wait_send()
    wait_all(mix, kv, mix_send.at[0], False)
    for copy in swaps:
        copy.wait_send()
    gain = mlp_gain[pl.ds(pl.multiple_of(c * half_kv, half_kv), half_kv), :]
    for w in weight_copies[1:]:
        w.wait()
    for s in swaps[1:]:
        s.wait_recv()
    def wait_others(buffer, sem, received=True):
        @pl.when(kept_here)
        def _():
            wait_all(buffer, kv - 1, sem, received)

        @pl.when(jnp.logical_not(kept_here))
        def _():
            wait_all(buffer, kv, sem, received)

    wait_others(mid, mid_recv.at[0])
    tops, bottoms = [], []
    squares = jnp.zeros((half_rows, tp * feats), F32)
    for i in range(half_kv):
        a = mid[tp * i].astype(F32)
        b = mid[tp * i + 1].astype(F32)
        squares = squares + a * a + b * b
        g = gain[i : i + 1]
        tops.append((jnp.where(low, a, halves_swapped(b)) * g).astype(BF16))
        bottoms.append((jnp.where(low, halves_swapped(a), b) * g).astype(BF16))
    features = jnp.concatenate(
        [jnp.concatenate(tops, axis=1), jnp.concatenate(bottoms, axis=1)], axis=0
    )
    sq_top = jnp.sum(jnp.where(low, squares, 0.0), axis=1, keepdims=True)
    sq_bottom = jnp.sum(jnp.where(low, 0.0, squares), axis=1, keepdims=True)
    sq_mid = jnp.concatenate([sq_top, sq_bottom], axis=0)
    wide_out[4, :, :] = jnp.broadcast_to(sq_mid, wide_out.shape[1:])
    sums = [dot_t(features, mlp_w[i]) for i in range(4)]
    for i in range(4):
        wide_out[i, :, pl.ds(0, units)] = sums[i]
    remote(wide_out, wide_in, pair_send.at[6], pair_recv.at[6], z, other).start()
    remote(wide_out, wide_in, pair_send.at[6], pair_recv.at[6], z, other).wait_recv()
    mlp_scale = lax.rsqrt((sq_mid + wide_in[4, :, 0:1]) / width + EPS)
    terms = None
    for i in range(2):
        gate = (sums[2 * i] + wide_in[2 - 2 * i, :, pl.ds(0, units)]) * mlp_scale
        upward = (sums[2 * i + 1] + wide_in[3 - 2 * i, :, pl.ds(0, units)]) * mlp_scale
        hidden = (gate * jax.nn.sigmoid(gate) * upward).astype(BF16)
        term = dot(hidden, down_w[i])
        terms = term if terms is None else terms + term

    for i in range(half_kv):
        at = slice(i * tp * feats, (i + 1) * tp * feats)
        top, bottom = terms[:half_rows, at], terms[half_rows:, at]
        to = c * half_kv + i
        for to_c, message in (
            (0, jnp.where(low, top, halves_swapped(bottom))),
            (1, jnp.where(low, halves_swapped(top), bottom)),
        ):
            n = 2 * i + to_c
            terms_out[n] = message.astype(BF16)
            copy = remote(terms_out.at[n], terms_in.at[z], term_send.at[0], term_recv.at[0], to, to_c)
            to_self = jnp.logical_and(to == z, to_c == c)

            @pl.when(jnp.logical_not(to_self))
            def _(copy=copy):
                copy.start()

            @pl.when(to_self)
            def _(n=n):
                terms_in[z] = terms_out[n]

    remote(wide_out, wide_in, pair_send.at[6], pair_recv.at[6], z, other).wait_send()
    wait_others(mid, mid_send.at[0], False)
    wait_others(terms_in, term_recv.at[0])
    summed = middle.astype(F32) + jnp.sum(terms_in[...].astype(F32), axis=0)
    result[pl.ds(0, half_rows), :] = summed[:, :feats].astype(BF16)
    result[pl.ds(half_rows, half_rows), :] = summed[:, feats:].astype(BF16)

    wait_others(terms_in, term_send.at[0], False)


def write_out(result, new_state, result_out, new_state_out, sem):
    copies = [
        pltpu.make_async_copy(new_state, new_state_out, sem.at[0]),
        pltpu.make_async_copy(result, result_out, sem.at[1]),
    ]
    for copy in copies:
        copy.start()
    for copy in copies:
        copy.wait()


def body(
    kv,
    tp,
    tokens,
    past_state,
    mix_gain,
    w_query,
    w_forget,
    w_value,
    w_gate_out,
    floor_logits,
    head_gain,
    w_out,
    mlp_gain,
    w_gate,
    w_up,
    w_down,
):
    rows, feats = tokens.shape
    seqs, heads_local, dk, dv = past_state.shape
    units = w_gate.shape[1]
    group = heads_local * seqs
    channels = heads_local * dv
    half_cols = w_down.shape[1] // tp
    wide = -(-units // 128) * 128
    in_vmem = pl.BlockSpec(memory_space=pltpu.VMEM)
    dma = pltpu.SemaphoreType.DMA
    outputs = pl.pallas_call(
        functools.partial(kernel, kv, tp),
        name="decode_step",
        out_shape=(
            jax.ShapeDtypeStruct((rows, feats), BF16),
            jax.ShapeDtypeStruct(past_state.shape, F32),
        ),
        in_specs=[pl.BlockSpec(memory_space=pltpu.HBM)] * 14,
        out_specs=(in_vmem, in_vmem),
        scratch_shapes=[
            pltpu.VMEM((rows, feats), BF16),
            pltpu.VMEM((1, tp * feats), F32),
            pltpu.VMEM((heads_local, dk), F32),
            pltpu.VMEM((1, dv), F32),
            pltpu.VMEM((kv, tp * feats), F32),
            pltpu.VMEM((rows // 2, 2 * feats), BF16),
            pltpu.VMEM((rows // 2, 2 * feats), BF16),
            pltpu.VMEM((4, *w_query.shape), BF16),
            pltpu.VMEM(past_state.shape, F32),
            pltpu.VMEM((2, feats, channels), BF16),
            pltpu.VMEM((4, units, half_cols), BF16),
            pltpu.VMEM((2, units, half_cols), BF16),
            pltpu.VMEM((group, dk), F32),
            pltpu.VMEM((group, dv), F32),
            pltpu.VMEM((kv, 4 * group, dk), BF16),
            pltpu.VMEM((kv, 4 * group, dk), BF16),
            pltpu.VMEM((kv, seqs, dk), F32),
            pltpu.VMEM((kv, seqs, dk), F32),
            pltpu.VMEM((4 * group + 8, dk), F32),
            pltpu.VMEM((kv, 4 * group, dk), BF16),
            pltpu.VMEM((kv, seqs, dk), F32),
            pltpu.VMEM((4 * group + 8, dk), F32),
            pltpu.VMEM((4 * group + 8, dk), F32),
            pltpu.VMEM((group, dv), BF16),
            pltpu.VMEM((kv, group, dv), BF16),
            pltpu.VMEM((rows // 2, 2 * feats), F32),
            pltpu.VMEM((rows // 2, 2 * feats), F32),
            pltpu.VMEM((rows // 2, 2 * feats), BF16),
            pltpu.VMEM((kv, rows // 2, 2 * feats), BF16),
            pltpu.VMEM((5, rows, wide), F32),
            pltpu.VMEM((5, rows, wide), F32),
            pltpu.VMEM((kv, rows // 2, 2 * feats), BF16),
            pltpu.VMEM((kv, rows // 2, 2 * feats), BF16),
            dma((11,)),
            dma((7,)),
            dma((7,)),
            *[dma((1,))] * 14,
            pltpu.SemaphoreType.REGULAR,
            pltpu.SemaphoreType.REGULAR((kv,)),
        ],
        compiler_params=pltpu.CompilerParams(
            collective_id=0, has_side_effects=True, vmem_limit_bytes=VMEM_BYTES
        ),
    )(*hbm(
        tokens,
        past_state,
        mix_gain.reshape(1, -1),
        w_query,
        w_forget,
        w_value,
        w_gate_out,
        floor_logits.reshape(heads_local, dk),
        head_gain.reshape(1, -1),
        w_out.T,
        mlp_gain.reshape(kv, tp * feats),
        w_gate.T,
        w_up.T,
        w_down,
    ))
    return pl.pallas_call(
        write_out,
        name="write_out",
        out_shape=tuple(jax.ShapeDtypeStruct(a.shape, a.dtype) for a in outputs),
        in_specs=[in_vmem] * len(outputs),
        out_specs=(pl.BlockSpec(memory_space=pltpu.HBM),) * len(outputs),
        scratch_shapes=[dma((len(outputs),))],
        compiler_params=pltpu.CompilerParams(vmem_limit_bytes=16 * 1024 * 1024),
    )(*outputs)


def solution(mesh):
    placed = (
        P(("grp", "dp"), ("kv", "tp")),
        P(("grp", "dp", "kv"), "tp", None, None),
        P("kv"),
        P("kv", "tp"),
        P("kv", "tp"),
        P("kv", "tp"),
        P("kv", "tp"),
        P("tp"),
        P(),
        P(None, ("kv", "tp")),
        P(),
        P(None, ("kv", "tp")),
        P(None, ("kv", "tp")),
        P(("kv", "tp"), None),
    )
    return jax.shard_map(
        functools.partial(body, mesh.shape["kv"], mesh.shape["tp"]),
        mesh=mesh,
        in_specs=placed,
        out_specs=(P(("grp", "dp"), ("kv", "tp")), P(("grp", "dp", "kv"), "tp", None, None)),
        check_vma=False,
    )
```

```python
import functools

import jax
import jax.numpy as jnp
from jax import lax
from jax.experimental import pallas as pl
from jax.experimental.pallas import tpu as pltpu
from jax.sharding import PartitionSpec as P

MESH = pl.DeviceIdType.MESH
EPS = 1e-06
VMEM_BYTES = 48 * 1024 * 1024
F32 = jnp.float32
BF16 = jnp.bfloat16


def dot(a, b):
    return jnp.dot(a, b, preferred_element_type=F32)


def dot_t(a, b):
    return lax.dot_general(a, b, (((1,), (1,)), ((), ())), preferred_element_type=F32)


def hbm(*arrays):
    return [pltpu.with_memory_space_constraint(a, pltpu.HBM) for a in arrays]


def packed(x):
    half = x.shape[0] // 2
    return jnp.concatenate([x[:half], x[half:]], axis=1)


def halves_swapped(x):
    return pltpu.roll(x, x.shape[1] // 2, 1)


def kernel(
    kv,
    tp,
    tokens_hbm,
    past_state,
    mix_gain_hbm,
    w_query,
    w_forget,
    w_value,
    w_gate_out,
    floor_hbm,
    head_gain_hbm,
    w_out,
    mlp_gain_hbm,
    w_gate,
    w_up,
    w_down,
    result,
    new_state,
    tokens,
    mix_gain,
    floor_logits,
    head_gain,
    mlp_gain,
    tok_own,
    tok_other,
    proj_w,
    state,
    out_w,
    mlp_w,
    down_w,
    floors,
    heads,
    chunk_out,
    chunk_in,
    sq_out,
    sq_in,
    total,
    relay_in,
    relay_sq_in,
    relayed_out,
    relayed_in,
    mix_own,
    mix,
    part_out,
    part_in,
    mid_own,
    mid,
    wide_out,
    wide_in,
    terms_out,
    terms_in,
    local_sem,
    pair_send,
    pair_recv,
    rs_send,
    rs_recv,
    sq_send,
    sq_recv,
    mix_send,
    mix_recv,
    mid_send,
    mid_recv,
    term_send,
    term_recv,
    relay_recv,
    relay_sq_recv,
    relayed_send,
    relayed_recv,
    pair_in,
    ready,
):
    z = lax.axis_index("kv")
    c = lax.axis_index("tp")
    other = 1 - c
    rows, feats = tokens.shape
    seqs, heads_local, dk, dv = past_state.shape
    units = w_gate.shape[0]
    group = heads_local * seqs
    half_rows = rows // 2
    width = kv * tp * feats
    half_kv = kv // tp
    half_cols = half_kv * tp * feats

    def local(src, dst, i):
        copy = pltpu.make_async_copy(src, dst, local_sem.at[i])
        copy.start()
        return copy

    def remote(src, dst, send, recv, to_z, to_c):
        return pltpu.make_async_remote_copy(
            src_ref=src,
            dst_ref=dst,
            send_sem=send,
            recv_sem=recv,
            device_id={"kv": to_z, "tp": to_c},
            device_id_type=MESH,
        )

    def peer(d):
        return lax.rem(z + d, kv)

    def place(w):
        return jnp.where(w == 0, kv - 2, jnp.where(w == kv - 1, kv - 1, w - 1))

    order = [*range(1, kv - 1), 0, kv - 1]
    last = kv - 1
    near_last = [w for w in range(kv - tp - 2, kv - 1)]
    relays = {0: kv // 4, last: near_last[0] - 1}
    behind = near_last[0] - 1
    listeners = {0: [relays[0], *near_last], last: [relays[last], *near_last, 0]}
    far_first = sorted(range(1, kv), key=lambda d: -min(d, kv - d))

    def wait_all(buffer, count, sem, received=True):
        part_of = buffer.at[pl.ds(0, count)]
        copy = remote(part_of, part_of, sem, sem, z, other)
        copy.wait_recv() if received else copy.wait_send()

    barrier = pltpu.get_barrier_semaphore()

    def signal(sem, to_z, to_c):
        pl.semaphore_signal(sem, inc=1, device_id={"kv": to_z, "tp": to_c}, device_id_type=MESH)

    @pl.when(c == 1)
    def _():
        signal(barrier, z, 0)

    tokens_copy = local(tokens_hbm, tokens, 2)
    gain_copy = local(mix_gain_hbm, mix_gain, 3)
    for i, w in enumerate((w_query, w_forget, w_value, w_gate_out)):
        local(w, proj_w.at[i], 0)
    state_copy = local(past_state, state, 1)
    small_copies = [
        local(floor_hbm, floor_logits, 4),
        local(head_gain_hbm, head_gain, 5),
        local(mlp_gain_hbm, mlp_gain, 6),
    ]
    half_of = pl.ds(pl.multiple_of(c * half_cols, half_cols), half_cols)
    half_of_other = pl.ds(pl.multiple_of(other * half_cols, half_cols), half_cols)
    weight_copies = [
        local(w_out.at[:, half_of_other], out_w.at[0], 7),
        local(w_gate.at[:, half_of], mlp_w.at[0], 8),
        local(w_up.at[:, half_of], mlp_w.at[1], 9),
        local(w_down.at[:, half_of], down_w.at[0], 10),
    ]

    @pl.when(c == 0)
    def _():
        pl.semaphore_wait(barrier, 1)
        signal(pair_in, z, 1)

    @pl.when(c == 1)
    def _():
        pl.semaphore_wait(pair_in, 1)
        for w in order:

            @pl.when(place(z) < place(w))
            def _(w=w):
                signal(barrier, w, 1)

    def count():
        @pl.when(c == 1)
        def _():
            @pl.when(place(z) > 0)
            def _():
                pl.semaphore_wait(barrier, place(z))

            signal(pair_in, z, 0)

        @pl.when(c == 0)
        def _():
            pl.semaphore_wait(pair_in, 1)

    def count_and_tell_listeners(special):
        @pl.when(z == special)
        def _():
            count()
            for w in listeners[special]:
                if order.index(w) < order.index(special):
                    signal(ready.at[special], w, c)

    @pl.when((z != 0) & (z != last))
    def _():
        count()
        for d in far_first:
            to = peer(d)

            @pl.when(place(to) < place(z))
            def _(to=to):
                signal(ready.at[z], to, c)

    tokens_copy.wait()
    own = tokens[...].astype(F32)
    tok_own[...] = packed(own).astype(BF16)
    tok = remote(tok_own, tok_other, pair_send.at[0], pair_recv.at[0], z, other)
    tok.start()

    r = lax.broadcasted_iota(jnp.int32, (kv * group, kv * group), 0)
    col = lax.broadcasted_iota(jnp.int32, (kv * group, kv * group), 1)
    s_of = lax.rem(r, seqs)
    to_chunks = lax.rem(r // seqs, heads_local) * (kv * seqs) + (r // group) * seqs + s_of
    spread = jnp.where(col == to_chunks, 1.0, 0.0).astype(BF16)
    to_heads = lax.rem(r // seqs, kv) * group + (r // (kv * seqs)) * seqs + s_of
    gather = jnp.where(col == to_heads, 1.0, 0.0).astype(BF16)

    lane = lax.broadcasted_iota(jnp.int32, (1, tp * feats), 1)
    low = lane < feats
    own_twice = jnp.concatenate([own, own], axis=1)
    tok.wait_recv()

    count_and_tell_listeners(last)
    got = tok_other[...].astype(F32)
    got_swapped = halves_swapped(got)
    got_twice = jnp.concatenate(
        [jnp.where(low, got, got_swapped), jnp.where(low, got_swapped, got)], axis=0
    )
    mine = lax.broadcasted_iota(jnp.int32, (rows, tp * feats), 1) // feats == c
    block = jnp.where(mine, own_twice, got_twice)
    squares = jnp.sum(block * block, axis=1, keepdims=True)
    sq_out[...] = jnp.broadcast_to(squares, (rows, dk)).reshape(kv, seqs, dk)
    gain_copy.wait()
    gained = (block * mix_gain[...]).astype(BF16)
    def sq_copy(to):
        return remote(sq_out.at[to], sq_in.at[z], sq_send.at[0], sq_recv.at[0], to, c)

    def chunk_copy(to):
        return remote(chunk_out.at[to], chunk_in.at[z], rs_send.at[0], rs_recv.at[0], to, c)

    def sq_to_relay(special):
        return remote(
            sq_out.at[special], relay_sq_in.at[z - 1], sq_send.at[0], relay_sq_recv.at[0], relays[special], c
        )

    def chunk_to_relay(special):
        return remote(
            chunk_out.at[special], relay_in.at[z - 1], rs_send.at[0], relay_recv.at[0], relays[special], c
        )

    pltpu.make_async_copy(proj_w, proj_w, local_sem.at[0]).wait()
    products = [dot(gained, proj_w[i]).astype(BF16) for i in range(4)]
    for i in (0, 2):
        stack = jnp.concatenate(
            [
                jnp.concatenate([p[:, h * dk : (h + 1) * dk] for p in products[i : i + 2]], axis=1)
                for h in range(heads_local)
            ],
            axis=0,
        )
        ordered = dot(spread, stack).astype(BF16)
        for j in range(2):
            chunk_out[:, pl.ds((i + j) * group, group), :] = ordered[:, j * dk : (j + 1) * dk].reshape(
                kv, group, dk
            )

    count_and_tell_listeners(0)

    for d in far_first:
        to = peer(d)

        @pl.when(place(to) < place(z))
        def _(to=to):
            sq_copy(to).start()
            chunk_copy(to).start()

    for special, relay in relays.items():

        @pl.when((z > relay) & (z <= behind))
        def _(special=special):
            sq_to_relay(special).start()
            chunk_to_relay(special).start()

    swaps = [
        remote(w_out.at[:, half_of], out_w.at[1], pair_send.at[1], pair_recv.at[1], z, other),
        remote(w_gate.at[:, half_of_other], mlp_w.at[2], pair_send.at[2], pair_recv.at[2], z, other),
        remote(w_up.at[:, half_of_other], mlp_w.at[3], pair_send.at[3], pair_recv.at[3], z, other),
        remote(w_down.at[:, half_of_other], down_w.at[1], pair_send.at[4], pair_recv.at[4], z, other),
    ]
    is_special = (z == 0) | (z == last)

    @pl.when(jnp.logical_not(is_special))
    def _():
        for s in swaps:
            s.start()


    sq_in[z] = sq_out[z]
    chunk_in[z] = chunk_out[z]
    for copy in small_copies:
        copy.wait()
    lower_in = jax.nn.sigmoid(floor_logits[...])
    for h in range(heads_local):
        floors[pl.ds(h * seqs, seqs), :] = jnp.broadcast_to(lower_in[h : h + 1], (seqs, dk))

    for w in order[:-2]:

        @pl.when(place(z) < place(w))
        def _(w=w):
            pl.semaphore_wait(ready.at[w], 1)
            sq_copy(w).start()
            chunk_copy(w).start()
            for special, relay in relays.items():
                if relay == w:
                    sq_to_relay(special).start()
                    chunk_to_relay(special).start()

    for special, relay in relays.items():
        forward = remote(relayed_out, relayed_in, relayed_send.at[0], relayed_recv.at[0], special, c)

        @pl.when(z == relay)
        def _(special=special, forward=forward):
            wait_all(relay_sq_in, behind - 1, relay_sq_recv.at[0])
            wait_all(relay_in, behind - 1, relay_recv.at[0])
            relay_sq_in[z - 1] = sq_out[special]
            relay_in[z - 1] = chunk_out[special]
            sums = relay_in[0].astype(F32)
            squares = relay_sq_in[0]
            for i in range(1, behind):
                sums = sums + relay_in[i].astype(F32)
                squares = squares + relay_sq_in[i]
            relayed_out[pl.ds(0, 4 * group), :] = sums
            relayed_out[pl.ds(4 * group, seqs), :] = squares
            pl.semaphore_wait(ready.at[special], 1)
            forward.start()

        for w in listeners[special]:
            if w != relay and order.index(w) < order.index(special):

                @pl.when(z == w)
                def _(special=special):
                    pl.semaphore_wait(ready.at[special], 1)
                    sq_copy(special).start()
                    chunk_copy(special).start()

    def add_up(slots):
        sums = chunk_in[slots[0]].astype(F32)
        squares = sq_in[slots[0]]
        for w in slots[1:]:
            sums = sums + chunk_in[w].astype(F32)
            squares = squares + sq_in[w]
        return sums, squares

    is_special = (z == 0) | (z == last)

    @pl.when(jnp.logical_not(is_special))
    def _():
        wait_all(sq_in, kv - 1, sq_recv.at[0])
        wait_all(chunk_in, kv - 1, rs_recv.at[0])
        sums, squares = add_up(order)
        total[pl.ds(0, 4 * group), :] = sums
        total[pl.ds(4 * group, seqs), :] = squares

    @pl.when(is_special)
    def _():
        wait_all(sq_in, len(near_last) + 1, sq_recv.at[0])
        wait_all(chunk_in, len(near_last) + 1, rs_recv.at[0])
        sums, squares = add_up([*near_last, 0, last])
        remote(relayed_out, relayed_in, relayed_send.at[0], relayed_recv.at[0], z, other).wait_recv()
        total[pl.ds(0, 4 * group), :] = sums + relayed_in[pl.ds(0, 4 * group), :]
        total[pl.ds(4 * group, seqs), :] = squares + relayed_in[pl.ds(4 * group, seqs), :]
        for s in swaps:
            s.start()

    total_sq = total[pl.ds(4 * group, seqs), :]
    scale_s = lax.rsqrt(total_sq / width + EPS)
    row_of = lax.broadcasted_iota(jnp.int32, (group, dk), 0)
    scale = jnp.broadcast_to(scale_s[0:1], (group, dk))
    for s in range(1, seqs):
        scale = jnp.where(lax.rem(row_of, seqs) == s, jnp.broadcast_to(scale_s[s : s + 1], (group, dk)), scale)
    query = total[pl.ds(0, group), :] * scale
    forget_pre = total[pl.ds(group, group), :] * scale
    value = total[pl.ds(2 * group, group), :] * scale
    gate_pre = total[pl.ds(3 * group, group), :] * scale
    lower = floors[...]
    forget = lower + (1.0 - lower) * jax.nn.sigmoid(forget_pre)
    activ = query * jax.nn.sigmoid(query)
    columns = jnp.concatenate([forget, activ, jnp.zeros((dk - 2 * group, dk), F32)], axis=0).T

    state_copy.wait()
    for h in range(heads_local):
        for s in range(seqs):
            i = h * seqs + s
            v_row = value[i : i + 1]
            f_col = columns[:, i : i + 1]
            q_col = columns[:, group + i : group + i + 1]
            new = v_row + f_col * (state[s, h] - v_row)
            new_state[s, h] = new
            heads[pl.ds(i, 1), :] = jnp.sum(new * q_col, axis=0, keepdims=True)

    head_out = heads[...]
    normed = head_out * lax.rsqrt(jnp.mean(head_out * head_out, axis=1, keepdims=True) + EPS)
    mixed = normed * head_gain[...] * (gate_pre * jax.nn.sigmoid(gate_pre))
    mix_own[...] = mixed.astype(BF16)
    for d in far_first:
        remote(mix_own, mix.at[z], mix_send.at[0], mix_recv.at[0], peer(d), other).start()
    remote(mix_own, mix.at[z], mix_send.at[0], mix_recv.at[0], z, other).start()
    tok.wait_send()
    is_relay = (z == relays[0]) | (z == relays[last])

    @pl.when(jnp.logical_not(is_relay))
    def _():
        wait_all(sq_in, kv - 1, sq_send.at[0], False)
        wait_all(chunk_in, kv - 1, rs_send.at[0], False)

    @pl.when(is_relay)
    def _():
        wait_all(sq_in, kv - 2, sq_send.at[0], False)
        wait_all(chunk_in, kv - 2, rs_send.at[0], False)
        remote(relayed_out, relayed_in, relayed_send.at[0], relayed_recv.at[0], z, other).wait_send()

    weight_copies[0].wait()
    swaps[0].wait_recv()
    wait_all(mix, kv, mix_recv.at[0])
    by_head = dot(gather, mix[...].reshape(kv * group, dv)).astype(BF16)
    every = jnp.concatenate([by_head[h * rows : (h + 1) * rows] for h in range(heads_local)], axis=1)
    part_out[...] = packed(dot_t(every, out_w[1]))
    part = remote(part_out, part_in, pair_send.at[5], pair_recv.at[5], z, other)
    part.start()
    kept = packed(dot_t(every, out_w[0])) + packed(own)
    part.wait_recv()
    middle = (kept + part_in[...]).astype(BF16)
    mid_own[...] = middle
    half = z // half_kv
    half_z = lax.rem(z, half_kv)
    kept_here = half == c
    for d in far_first:
        remote(mid_own, mid.at[half_z * tp + c], mid_send.at[0], mid_recv.at[0], peer(d), half).start()

    @pl.when(kept_here)
    def _():
        mid[half_z * tp + c] = middle

    @pl.when(jnp.logical_not(kept_here))
    def _():
        remote(mid_own, mid.at[half_z * tp + c], mid_send.at[0], mid_recv.at[0], z, half).start()

    part.wait_send()
    wait_all(mix, kv, mix_send.at[0], False)
    for copy in swaps:
        copy.wait_send()
    gain = mlp_gain[pl.ds(pl.multiple_of(c * half_kv, half_kv), half_kv), :]
    for w in weight_copies[1:]:
        w.wait()
    for s in swaps[1:]:
        s.wait_recv()
    def wait_others(buffer, sem, received=True):
        @pl.when(kept_here)
        def _():
            wait_all(buffer, kv - 1, sem, received)

        @pl.when(jnp.logical_not(kept_here))
        def _():
            wait_all(buffer, kv, sem, received)

    wait_others(mid, mid_recv.at[0])
    tops, bottoms = [], []
    squares = jnp.zeros((half_rows, tp * feats), F32)
    for i in range(half_kv):
        a = mid[tp * i].astype(F32)
        b = mid[tp * i + 1].astype(F32)
        squares = squares + a * a + b * b
        g = gain[i : i + 1]
        tops.append((jnp.where(low, a, halves_swapped(b)) * g).astype(BF16))
        bottoms.append((jnp.where(low, halves_swapped(a), b) * g).astype(BF16))
    features = jnp.concatenate(
        [jnp.concatenate(tops, axis=1), jnp.concatenate(bottoms, axis=1)], axis=0
    )
    sq_top = jnp.sum(jnp.where(low, squares, 0.0), axis=1, keepdims=True)
    sq_bottom = jnp.sum(jnp.where(low, 0.0, squares), axis=1, keepdims=True)
    sq_mid = jnp.concatenate([sq_top, sq_bottom], axis=0)
    wide_out[4, :, :] = jnp.broadcast_to(sq_mid, wide_out.shape[1:])
    sums = [dot_t(features, mlp_w[i]) for i in range(4)]
    for i in range(4):
        wide_out[i, :, pl.ds(0, units)] = sums[i]
    remote(wide_out, wide_in, pair_send.at[6], pair_recv.at[6], z, other).start()
    remote(wide_out, wide_in, pair_send.at[6], pair_recv.at[6], z, other).wait_recv()
    mlp_scale = lax.rsqrt((sq_mid + wide_in[4, :, 0:1]) / width + EPS)
    terms = None
    for i in range(2):
        gate = (sums[2 * i] + wide_in[2 - 2 * i, :, pl.ds(0, units)]) * mlp_scale
        upward = (sums[2 * i + 1] + wide_in[3 - 2 * i, :, pl.ds(0, units)]) * mlp_scale
        hidden = (gate * jax.nn.sigmoid(gate) * upward).astype(BF16)
        term = dot(hidden, down_w[i])
        terms = term if terms is None else terms + term

    for i in range(half_kv):
        at = slice(i * tp * feats, (i + 1) * tp * feats)
        top, bottom = terms[:half_rows, at], terms[half_rows:, at]
        for to_c, message in (
            (0, jnp.where(low, top, halves_swapped(bottom))),
            (1, jnp.where(low, halves_swapped(top), bottom)),
        ):
            terms_out[tp * i + to_c] = message.astype(BF16)

    def term_copy(to, to_c):
        n = tp * (to - c * half_kv) + to_c
        return remote(terms_out.at[n], terms_in.at[z], term_send.at[0], term_recv.at[0], to, to_c)

    for d in far_first:
        to = peer(d)

        @pl.when(to // half_kv == c)
        def _(to=to):
            for to_c in range(tp):
                term_copy(to, to_c).start()

    @pl.when(kept_here)
    def _():
        term_copy(z, other).start()
        terms_in[z] = terms_out[tp * (z - c * half_kv) + c]

    remote(wide_out, wide_in, pair_send.at[6], pair_recv.at[6], z, other).wait_send()
    wait_others(mid, mid_send.at[0], False)
    wait_others(terms_in, term_recv.at[0])
    summed = middle.astype(F32) + jnp.sum(terms_in[...].astype(F32), axis=0)
    result[pl.ds(0, half_rows), :] = summed[:, :feats].astype(BF16)
    result[pl.ds(half_rows, half_rows), :] = summed[:, feats:].astype(BF16)

    wait_others(terms_in, term_send.at[0], False)


def write_out(result, new_state, result_out, new_state_out, sem):
    copies = [
        pltpu.make_async_copy(new_state, new_state_out, sem.at[0]),
        pltpu.make_async_copy(result, result_out, sem.at[1]),
    ]
    for copy in copies:
        copy.start()
    for copy in copies:
        copy.wait()


def body(
    kv,
    tp,
    tokens,
    past_state,
    mix_gain,
    w_query,
    w_forget,
    w_value,
    w_gate_out,
    floor_logits,
    head_gain,
    w_out,
    mlp_gain,
    w_gate,
    w_up,
    w_down,
):
    rows, feats = tokens.shape
    seqs, heads_local, dk, dv = past_state.shape
    units = w_gate.shape[1]
    group = heads_local * seqs
    channels = heads_local * dv
    half_cols = w_down.shape[1] // tp
    wide = -(-units // 128) * 128
    in_vmem = pl.BlockSpec(memory_space=pltpu.VMEM)
    dma = pltpu.SemaphoreType.DMA
    outputs = pl.pallas_call(
        functools.partial(kernel, kv, tp),
        name="decode_step",
        out_shape=(
            jax.ShapeDtypeStruct((rows, feats), BF16),
            jax.ShapeDtypeStruct(past_state.shape, F32),
        ),
        in_specs=[pl.BlockSpec(memory_space=pltpu.HBM)] * 14,
        out_specs=(in_vmem, in_vmem),
        scratch_shapes=[
            pltpu.VMEM((rows, feats), BF16),
            pltpu.VMEM((1, tp * feats), F32),
            pltpu.VMEM((heads_local, dk), F32),
            pltpu.VMEM((1, dv), F32),
            pltpu.VMEM((kv, tp * feats), F32),
            pltpu.VMEM((rows // 2, 2 * feats), BF16),
            pltpu.VMEM((rows // 2, 2 * feats), BF16),
            pltpu.VMEM((4, *w_query.shape), BF16),
            pltpu.VMEM(past_state.shape, F32),
            pltpu.VMEM((2, feats, channels), BF16),
            pltpu.VMEM((4, units, half_cols), BF16),
            pltpu.VMEM((2, units, half_cols), BF16),
            pltpu.VMEM((group, dk), F32),
            pltpu.VMEM((group, dv), F32),
            pltpu.VMEM((kv, 4 * group, dk), BF16),
            pltpu.VMEM((kv, 4 * group, dk), BF16),
            pltpu.VMEM((kv, seqs, dk), F32),
            pltpu.VMEM((kv, seqs, dk), F32),
            pltpu.VMEM((4 * group + 8, dk), F32),
            pltpu.VMEM((kv, 4 * group, dk), BF16),
            pltpu.VMEM((kv, seqs, dk), F32),
            pltpu.VMEM((4 * group + 8, dk), F32),
            pltpu.VMEM((4 * group + 8, dk), F32),
            pltpu.VMEM((group, dv), BF16),
            pltpu.VMEM((kv, group, dv), BF16),
            pltpu.VMEM((rows // 2, 2 * feats), F32),
            pltpu.VMEM((rows // 2, 2 * feats), F32),
            pltpu.VMEM((rows // 2, 2 * feats), BF16),
            pltpu.VMEM((kv, rows // 2, 2 * feats), BF16),
            pltpu.VMEM((5, rows, wide), F32),
            pltpu.VMEM((5, rows, wide), F32),
            pltpu.VMEM((kv, rows // 2, 2 * feats), BF16),
            pltpu.VMEM((kv, rows // 2, 2 * feats), BF16),
            dma((11,)),
            dma((7,)),
            dma((7,)),
            *[dma((1,))] * 14,
            pltpu.SemaphoreType.REGULAR,
            pltpu.SemaphoreType.REGULAR((kv,)),
        ],
        compiler_params=pltpu.CompilerParams(
            collective_id=0, has_side_effects=True, vmem_limit_bytes=VMEM_BYTES
        ),
    )(*hbm(
        tokens,
        past_state,
        mix_gain.reshape(1, -1),
        w_query,
        w_forget,
        w_value,
        w_gate_out,
        floor_logits.reshape(heads_local, dk),
        head_gain.reshape(1, -1),
        w_out.T,
        mlp_gain.reshape(kv, tp * feats),
        w_gate.T,
        w_up.T,
        w_down,
    ))
    return pl.pallas_call(
        write_out,
        name="write_out",
        out_shape=tuple(jax.ShapeDtypeStruct(a.shape, a.dtype) for a in outputs),
        in_specs=[in_vmem] * len(outputs),
        out_specs=(pl.BlockSpec(memory_space=pltpu.HBM),) * len(outputs),
        scratch_shapes=[dma((len(outputs),))],
        compiler_params=pltpu.CompilerParams(vmem_limit_bytes=16 * 1024 * 1024),
    )(*outputs)


def solution(mesh):
    placed = (
        P(("grp", "dp"), ("kv", "tp")),
        P(("grp", "dp", "kv"), "tp", None, None),
        P("kv"),
        P("kv", "tp"),
        P("kv", "tp"),
        P("kv", "tp"),
        P("kv", "tp"),
        P("tp"),
        P(),
        P(None, ("kv", "tp")),
        P(),
        P(None, ("kv", "tp")),
        P(None, ("kv", "tp")),
        P(("kv", "tp"), None),
    )
    return jax.shard_map(
        functools.partial(body, mesh.shape["kv"], mesh.shape["tp"]),
        mesh=mesh,
        in_specs=placed,
        out_specs=(P(("grp", "dp"), ("kv", "tp")), P(("grp", "dp", "kv"), "tp", None, None)),
        check_vma=False,
    )
```

```python
import functools

import jax
import jax.numpy as jnp
from jax import lax
from jax.experimental import pallas as pl
from jax.experimental.pallas import tpu as pltpu
from jax.sharding import PartitionSpec as P

MESH = pl.DeviceIdType.MESH
EPS = 1e-06
VMEM_BYTES = 48 * 1024 * 1024
F32 = jnp.float32
BF16 = jnp.bfloat16


def dot(a, b):
    return jnp.dot(a, b, preferred_element_type=F32)


def dot_t(a, b):
    return lax.dot_general(a, b, (((1,), (1,)), ((), ())), preferred_element_type=F32)


def hbm(*arrays):
    return [pltpu.with_memory_space_constraint(a, pltpu.HBM) for a in arrays]


def packed(x):
    half = x.shape[0] // 2
    return jnp.concatenate([x[:half], x[half:]], axis=1)


def halves_swapped(x):
    return pltpu.roll(x, x.shape[1] // 2, 1)


def kernel(
    kv,
    tp,
    tokens_hbm,
    past_state,
    mix_gain_hbm,
    w_query,
    w_forget,
    w_value,
    w_gate_out,
    floor_hbm,
    head_gain_hbm,
    w_out,
    mlp_gain_hbm,
    w_gate,
    w_up,
    w_down,
    result,
    new_state,
    tokens,
    mix_gain,
    floor_logits,
    head_gain,
    mlp_gain,
    tok_own,
    tok_other,
    proj_w,
    state,
    out_w,
    mlp_w,
    down_w,
    floors,
    heads,
    chunk_out,
    chunk_in,
    sq_out,
    sq_in,
    total,
    joint_in,
    relay_in,
    relay_sq_in,
    relayed_out,
    relayed_in,
    mix_own,
    mix,
    part_out,
    part_in,
    mid_own,
    mid,
    wide_out,
    wide_in,
    terms_out,
    terms_in,
    local_sem,
    pair_send,
    pair_recv,
    rs_send,
    rs_recv,
    sq_send,
    sq_recv,
    mix_send,
    mix_recv,
    mid_send,
    mid_recv,
    term_send,
    term_recv,
    joint_recv,
    relay_recv,
    relay_sq_recv,
    relayed_send,
    relayed_recv,
    pair_in,
    ready,
):
    z = lax.axis_index("kv")
    c = lax.axis_index("tp")
    other = 1 - c
    rows, feats = tokens.shape
    seqs, heads_local, dk, dv = past_state.shape
    units = w_gate.shape[0]
    group = heads_local * seqs
    half_rows = rows // 2
    width = kv * tp * feats
    half_kv = kv // tp
    half_cols = half_kv * tp * feats

    def local(src, dst, i):
        copy = pltpu.make_async_copy(src, dst, local_sem.at[i])
        copy.start()
        return copy

    def remote(src, dst, send, recv, to_z, to_c):
        return pltpu.make_async_remote_copy(
            src_ref=src,
            dst_ref=dst,
            send_sem=send,
            recv_sem=recv,
            device_id={"kv": to_z, "tp": to_c},
            device_id_type=MESH,
        )

    def peer(d):
        return lax.rem(z + d, kv)

    def place(w):
        return jnp.where(w == 0, kv - 2, jnp.where(w == kv - 1, kv - 1, w - 1))

    order = [*range(1, kv - 1), 0, kv - 1]
    last = kv - 1
    near_last = [w for w in range(kv - tp - 2, kv - 1)]
    relays = {0: kv // 4, last: near_last[0] - 1}
    behind = near_last[0] - 1
    listeners = {0: [relays[0], *near_last], last: [relays[last], *near_last, 0]}
    far_first = sorted(range(1, kv), key=lambda d: -min(d, kv - d))

    def wait_all(buffer, count, sem, received=True):
        part_of = buffer.at[pl.ds(0, count)]
        copy = remote(part_of, part_of, sem, sem, z, other)
        copy.wait_recv() if received else copy.wait_send()

    barrier = pltpu.get_barrier_semaphore()

    def signal(sem, to_z, to_c):
        pl.semaphore_signal(sem, inc=1, device_id={"kv": to_z, "tp": to_c}, device_id_type=MESH)

    @pl.when(c == 1)
    def _():
        signal(barrier, z, 0)

    tokens_copy = local(tokens_hbm, tokens, 2)
    gain_copy = local(mix_gain_hbm, mix_gain, 3)
    for i, w in enumerate((w_query, w_forget, w_value, w_gate_out)):
        local(w, proj_w.at[i], 0)
    state_copy = local(past_state, state, 1)
    small_copies = [
        local(floor_hbm, floor_logits, 4),
        local(head_gain_hbm, head_gain, 5),
        local(mlp_gain_hbm, mlp_gain, 6),
    ]
    is_special = (z == 0) | (z == last)
    half_of = pl.ds(pl.multiple_of(c * half_cols, half_cols), half_cols)
    half_of_other = pl.ds(pl.multiple_of(other * half_cols, half_cols), half_cols)
    weight_copies = [
        local(w_out.at[:, half_of_other], out_w.at[0], 7),
        local(w_gate.at[:, half_of], mlp_w.at[0], 8),
        local(w_up.at[:, half_of], mlp_w.at[1], 9),
        local(w_down.at[:, half_of], down_w.at[0], 10),
    ]

    @pl.when(c == 0)
    def _():
        pl.semaphore_wait(barrier, 1)
        signal(pair_in, z, 1)

    @pl.when(c == 1)
    def _():
        pl.semaphore_wait(pair_in, 1)
        for w in order:

            @pl.when(place(z) < place(w))
            def _(w=w):
                signal(barrier, w, 1)

    def count_and_tell():
        @pl.when(c == 1)
        def _():
            @pl.when(place(z) > 0)
            def _():
                pl.semaphore_wait(barrier, place(z))

            signal(pair_in, z, 0)

        @pl.when(c == 0)
        def _():
            pl.semaphore_wait(pair_in, 1)

        for special, told in listeners.items():

            @pl.when(z == special)
            def _(special=special, told=told):
                for w in told:
                    if order.index(w) < order.index(special):
                        signal(ready.at[special], w, c)

        for d in far_first:
            to = peer(d)

            @pl.when((place(to) < place(z)) & (place(z) < kv - 2))
            def _(to=to):
                signal(ready.at[z], to, c)

    @pl.when(z != last)
    def _():
        count_and_tell()

    tokens_copy.wait()
    own = tokens[...].astype(F32)
    tok_own[...] = packed(own).astype(BF16)
    tok = remote(tok_own, tok_other, pair_send.at[0], pair_recv.at[0], z, other)
    tok.start()

    r = lax.broadcasted_iota(jnp.int32, (kv * group, kv * group), 0)
    col = lax.broadcasted_iota(jnp.int32, (kv * group, kv * group), 1)
    s_of = lax.rem(r, seqs)
    to_chunks = lax.rem(r // seqs, heads_local) * (kv * seqs) + (r // group) * seqs + s_of
    spread = jnp.where(col == to_chunks, 1.0, 0.0).astype(BF16)
    to_heads = lax.rem(r // seqs, kv) * group + (r // (kv * seqs)) * seqs + s_of
    gather = jnp.where(col == to_heads, 1.0, 0.0).astype(BF16)

    lane = lax.broadcasted_iota(jnp.int32, (1, tp * feats), 1)
    low = lane < feats
    own_twice = jnp.concatenate([own, own], axis=1)
    tok.wait_recv()

    @pl.when(z == last)
    def _():
        count_and_tell()

    got = tok_other[...].astype(F32)
    got_swapped = halves_swapped(got)
    got_twice = jnp.concatenate(
        [jnp.where(low, got, got_swapped), jnp.where(low, got_swapped, got)], axis=0
    )
    mine = lax.broadcasted_iota(jnp.int32, (rows, tp * feats), 1) // feats == c
    block = jnp.where(mine, own_twice, got_twice)
    squares = jnp.sum(block * block, axis=1, keepdims=True)
    sq_out[...] = jnp.broadcast_to(squares, (rows, dk)).reshape(kv, seqs, dk)
    gain_copy.wait()
    gained = (block * mix_gain[...]).astype(BF16)
    def sq_copy(to):
        return remote(sq_out.at[to], sq_in.at[z], sq_send.at[0], sq_recv.at[0], to, c)

    def chunk_copy(to):
        return remote(chunk_out.at[to], chunk_in.at[z], rs_send.at[0], rs_recv.at[0], to, c)

    def sq_to_relay(special):
        return remote(
            sq_out.at[special], relay_sq_in.at[z - 1], sq_send.at[0], relay_sq_recv.at[0], relays[special], c
        )

    def chunk_to_relay(special):
        return remote(
            chunk_out.at[special], relay_in.at[z - 1], rs_send.at[0], relay_recv.at[0], relays[special], c
        )

    for d in far_first:
        to = peer(d)

        @pl.when(place(to) < place(z))
        def _(to=to):
            sq_copy(to).start()

    for special, relay in relays.items():

        @pl.when((z > relay) & (z <= behind))
        def _(special=special):
            sq_to_relay(special).start()

    pltpu.make_async_copy(proj_w, proj_w, local_sem.at[0]).wait()
    products = [dot(gained, proj_w[i]).astype(BF16) for i in range(4)]
    for i in (0, 2):
        stack = jnp.concatenate(
            [
                jnp.concatenate([p[:, h * dk : (h + 1) * dk] for p in products[i : i + 2]], axis=1)
                for h in range(heads_local)
            ],
            axis=0,
        )
        ordered = dot(spread, stack).astype(BF16)
        for j in range(2):
            chunk_out[:, pl.ds((i + j) * group, group), :] = ordered[:, j * dk : (j + 1) * dk].reshape(
                kv, group, dk
            )

    for d in far_first:
        to = peer(d)

        @pl.when((place(to) < place(z)) & jnp.logical_not(is_special))
        def _(to=to):
            chunk_copy(to).start()

    for special, relay in relays.items():

        @pl.when((z > relay) & (z <= behind))
        def _(special=special):
            chunk_to_relay(special).start()

    swaps = [
        remote(w_out.at[:, half_of], out_w.at[1], pair_send.at[1], pair_recv.at[1], z, other),
        remote(w_gate.at[:, half_of_other], mlp_w.at[2], pair_send.at[2], pair_recv.at[2], z, other),
        remote(w_up.at[:, half_of_other], mlp_w.at[3], pair_send.at[3], pair_recv.at[3], z, other),
        remote(w_down.at[:, half_of_other], down_w.at[1], pair_send.at[4], pair_recv.at[4], z, other),
    ]
    @pl.when(jnp.logical_not(is_special))
    def _():
        for s in swaps:
            s.start()


    sq_in[z] = sq_out[z]
    chunk_in[z] = chunk_out[z]
    for copy in small_copies:
        copy.wait()
    lower_in = jax.nn.sigmoid(floor_logits[...])
    for h in range(heads_local):
        floors[pl.ds(h * seqs, seqs), :] = jnp.broadcast_to(lower_in[h : h + 1], (seqs, dk))

    for w in order[:-2]:

        @pl.when(place(z) < place(w))
        def _(w=w):
            pl.semaphore_wait(ready.at[w], 1)
            sq_copy(w).start()
            chunk_copy(w).start()
            for special, relay in relays.items():
                if relay == w:
                    sq_to_relay(special).start()
                    chunk_to_relay(special).start()

    for special, relay in relays.items():
        forward = remote(relayed_out, relayed_in, relayed_send.at[0], relayed_recv.at[0], special, c)

        @pl.when(z == relay)
        def _(special=special, forward=forward):
            wait_all(relay_sq_in, behind - 1, relay_sq_recv.at[0])
            wait_all(relay_in, behind - 1, relay_recv.at[0])
            relay_sq_in[z - 1] = sq_out[special]
            relay_in[z - 1] = chunk_out[special]
            sums = relay_in[0].astype(F32)
            squares = relay_sq_in[0]
            for i in range(1, behind):
                sums = sums + relay_in[i].astype(F32)
                squares = squares + relay_sq_in[i]
            relayed_out[pl.ds(0, 4 * group), :] = sums
            relayed_out[pl.ds(4 * group, seqs), :] = squares
            pl.semaphore_wait(ready.at[special], 1)
            forward.start()

        for w in listeners[special]:
            if w != relay and order.index(w) < order.index(special):

                @pl.when(z == w)
                def _(special=special):
                    pl.semaphore_wait(ready.at[special], 1)
                    sq_copy(special).start()
                    chunk_copy(special).start()

    middle_z = kv // 2
    sides = {0: list(range(middle_z, 0, -1)), last: list(range(middle_z + 1, last))}
    for special, partner in ((last, 0), (0, last)):

        @pl.when(z == special)
        def _(special=special, partner=partner):
            for w in sides[partner]:
                remote(
                    chunk_out.at[w], joint_in.at[w], rs_send.at[0], joint_recv.at[w], partner, c
                ).start()
            if special == last:
                chunk_copy(partner).start()
            for w in sides[special]:
                remote(joint_in.at[w], joint_in.at[w], joint_recv.at[w], joint_recv.at[w], z, other).wait_recv()
                chunk_out[w] = (chunk_out[w].astype(F32) + joint_in[w].astype(F32)).astype(BF16)
                remote(chunk_out.at[w], chunk_in.at[0], rs_send.at[0], rs_recv.at[0], w, c).start()

    def add_up(slots, joint):
        sums = chunk_in[slots[0]].astype(F32)
        squares = sq_in[slots[0]]
        for w in slots[1:]:
            if not (joint and w == last):
                sums = sums + chunk_in[w].astype(F32)
            squares = squares + sq_in[w]
        return sums, squares

    is_special = (z == 0) | (z == last)

    @pl.when(jnp.logical_not(is_special))
    def _():
        wait_all(sq_in, kv - 1, sq_recv.at[0])
        wait_all(chunk_in, kv - 2, rs_recv.at[0])
        sums, squares = add_up(order, True)
        total[pl.ds(0, 4 * group), :] = sums
        total[pl.ds(4 * group, seqs), :] = squares

    @pl.when(is_special)
    def _():
        wait_all(sq_in, len(near_last) + 1, sq_recv.at[0])
        wait_all(chunk_in, len(near_last) + 1, rs_recv.at[0])
        sums, squares = add_up([*near_last, 0, last], False)
        remote(relayed_out, relayed_in, relayed_send.at[0], relayed_recv.at[0], z, other).wait_recv()
        total[pl.ds(0, 4 * group), :] = sums + relayed_in[pl.ds(0, 4 * group), :]
        total[pl.ds(4 * group, seqs), :] = squares + relayed_in[pl.ds(4 * group, seqs), :]
        for s in swaps:
            s.start()

    total_sq = total[pl.ds(4 * group, seqs), :]
    scale_s = lax.rsqrt(total_sq / width + EPS)
    row_of = lax.broadcasted_iota(jnp.int32, (group, dk), 0)
    scale = jnp.broadcast_to(scale_s[0:1], (group, dk))
    for s in range(1, seqs):
        scale = jnp.where(lax.rem(row_of, seqs) == s, jnp.broadcast_to(scale_s[s : s + 1], (group, dk)), scale)
    query = total[pl.ds(0, group), :] * scale
    forget_pre = total[pl.ds(group, group), :] * scale
    value = total[pl.ds(2 * group, group), :] * scale
    gate_pre = total[pl.ds(3 * group, group), :] * scale
    lower = floors[...]
    forget = lower + (1.0 - lower) * jax.nn.sigmoid(forget_pre)
    activ = query * jax.nn.sigmoid(query)
    columns = jnp.concatenate([forget, activ, jnp.zeros((dk - 2 * group, dk), F32)], axis=0).T

    state_copy.wait()
    for h in range(heads_local):
        for s in range(seqs):
            i = h * seqs + s
            v_row = value[i : i + 1]
            f_col = columns[:, i : i + 1]
            q_col = columns[:, group + i : group + i + 1]
            new = v_row + f_col * (state[s, h] - v_row)
            new_state[s, h] = new
            heads[pl.ds(i, 1), :] = jnp.sum(new * q_col, axis=0, keepdims=True)

    head_out = heads[...]
    normed = head_out * lax.rsqrt(jnp.mean(head_out * head_out, axis=1, keepdims=True) + EPS)
    mixed = normed * head_gain[...] * (gate_pre * jax.nn.sigmoid(gate_pre))
    mix_own[...] = mixed.astype(BF16)
    for d in far_first:
        remote(mix_own, mix.at[z], mix_send.at[0], mix_recv.at[0], peer(d), other).start()
    remote(mix_own, mix.at[z], mix_send.at[0], mix_recv.at[0], z, other).start()
    tok.wait_send()
    is_relay = (z == relays[0]) | (z == relays[last])

    @pl.when(jnp.logical_not(is_relay))
    def _():
        wait_all(sq_in, kv - 1, sq_send.at[0], False)
        wait_all(chunk_in, kv - 1, rs_send.at[0], False)

    @pl.when(is_relay)
    def _():
        wait_all(sq_in, kv - 2, sq_send.at[0], False)
        wait_all(chunk_in, kv - 2, rs_send.at[0], False)
        remote(relayed_out, relayed_in, relayed_send.at[0], relayed_recv.at[0], z, other).wait_send()

    weight_copies[0].wait()
    swaps[0].wait_recv()
    wait_all(mix, kv, mix_recv.at[0])
    by_head = dot(gather, mix[...].reshape(kv * group, dv)).astype(BF16)
    every = jnp.concatenate([by_head[h * rows : (h + 1) * rows] for h in range(heads_local)], axis=1)
    part_out[...] = packed(dot_t(every, out_w[1]))
    part = remote(part_out, part_in, pair_send.at[5], pair_recv.at[5], z, other)
    part.start()
    kept = packed(dot_t(every, out_w[0])) + packed(own)
    part.wait_recv()
    middle = (kept + part_in[...]).astype(BF16)
    mid_own[...] = middle
    half = z // half_kv
    half_z = lax.rem(z, half_kv)
    kept_here = half == c
    for d in far_first:
        remote(mid_own, mid.at[half_z * tp + c], mid_send.at[0], mid_recv.at[0], peer(d), half).start()

    @pl.when(kept_here)
    def _():
        mid[half_z * tp + c] = middle

    @pl.when(jnp.logical_not(kept_here))
    def _():
        remote(mid_own, mid.at[half_z * tp + c], mid_send.at[0], mid_recv.at[0], z, half).start()

    part.wait_send()
    wait_all(mix, kv, mix_send.at[0], False)
    for copy in swaps:
        copy.wait_send()
    gain = mlp_gain[pl.ds(pl.multiple_of(c * half_kv, half_kv), half_kv), :]
    for w in weight_copies[1:]:
        w.wait()
    for s in swaps[1:]:
        s.wait_recv()
    def wait_others(buffer, sem, received=True):
        @pl.when(kept_here)
        def _():
            wait_all(buffer, kv - 1, sem, received)

        @pl.when(jnp.logical_not(kept_here))
        def _():
            wait_all(buffer, kv, sem, received)

    wait_others(mid, mid_recv.at[0])
    tops, bottoms = [], []
    squares = jnp.zeros((half_rows, tp * feats), F32)
    for i in range(half_kv):
        a = mid[tp * i].astype(F32)
        b = mid[tp * i + 1].astype(F32)
        squares = squares + a * a + b * b
        g = gain[i : i + 1]
        tops.append((jnp.where(low, a, halves_swapped(b)) * g).astype(BF16))
        bottoms.append((jnp.where(low, halves_swapped(a), b) * g).astype(BF16))
    features = jnp.concatenate(
        [jnp.concatenate(tops, axis=1), jnp.concatenate(bottoms, axis=1)], axis=0
    )
    sq_top = jnp.sum(jnp.where(low, squares, 0.0), axis=1, keepdims=True)
    sq_bottom = jnp.sum(jnp.where(low, 0.0, squares), axis=1, keepdims=True)
    sq_mid = jnp.concatenate([sq_top, sq_bottom], axis=0)
    wide_out[4, :, :] = jnp.broadcast_to(sq_mid, wide_out.shape[1:])
    sums = [dot_t(features, mlp_w[i]) for i in range(4)]
    for i in range(4):
        wide_out[i, :, pl.ds(0, units)] = sums[i]
    remote(wide_out, wide_in, pair_send.at[6], pair_recv.at[6], z, other).start()
    remote(wide_out, wide_in, pair_send.at[6], pair_recv.at[6], z, other).wait_recv()
    mlp_scale = lax.rsqrt((sq_mid + wide_in[4, :, 0:1]) / width + EPS)
    terms = None
    for i in range(2):
        gate = (sums[2 * i] + wide_in[2 - 2 * i, :, pl.ds(0, units)]) * mlp_scale
        upward = (sums[2 * i + 1] + wide_in[3 - 2 * i, :, pl.ds(0, units)]) * mlp_scale
        hidden = (gate * jax.nn.sigmoid(gate) * upward).astype(BF16)
        term = dot(hidden, down_w[i])
        terms = term if terms is None else terms + term

    for i in range(half_kv):
        at = slice(i * tp * feats, (i + 1) * tp * feats)
        top, bottom = terms[:half_rows, at], terms[half_rows:, at]
        to = c * half_kv + i
        for to_c, message in (
            (0, jnp.where(low, top, halves_swapped(bottom))),
            (1, jnp.where(low, halves_swapped(top), bottom)),
        ):
            n = 2 * i + to_c
            terms_out[n] = message.astype(BF16)
            copy = remote(terms_out.at[n], terms_in.at[z], term_send.at[0], term_recv.at[0], to, to_c)
            to_self = jnp.logical_and(to == z, to_c == c)

            @pl.when(jnp.logical_not(to_self))
            def _(copy=copy):
                copy.start()

            @pl.when(to_self)
            def _(n=n):
                terms_in[z] = terms_out[n]

    remote(wide_out, wide_in, pair_send.at[6], pair_recv.at[6], z, other).wait_send()
    wait_others(mid, mid_send.at[0], False)
    wait_others(terms_in, term_recv.at[0])
    summed = middle.astype(F32) + jnp.sum(terms_in[...].astype(F32), axis=0)
    result[pl.ds(0, half_rows), :] = summed[:, :feats].astype(BF16)
    result[pl.ds(half_rows, half_rows), :] = summed[:, feats:].astype(BF16)

    wait_others(terms_in, term_send.at[0], False)


def write_out(result, new_state, result_out, new_state_out, sem):
    copies = [
        pltpu.make_async_copy(new_state, new_state_out, sem.at[0]),
        pltpu.make_async_copy(result, result_out, sem.at[1]),
    ]
    for copy in copies:
        copy.start()
    for copy in copies:
        copy.wait()


def body(
    kv,
    tp,
    tokens,
    past_state,
    mix_gain,
    w_query,
    w_forget,
    w_value,
    w_gate_out,
    floor_logits,
    head_gain,
    w_out,
    mlp_gain,
    w_gate,
    w_up,
    w_down,
):
    rows, feats = tokens.shape
    seqs, heads_local, dk, dv = past_state.shape
    units = w_gate.shape[1]
    group = heads_local * seqs
    channels = heads_local * dv
    half_cols = w_down.shape[1] // tp
    wide = -(-units // 128) * 128
    in_vmem = pl.BlockSpec(memory_space=pltpu.VMEM)
    dma = pltpu.SemaphoreType.DMA
    outputs = pl.pallas_call(
        functools.partial(kernel, kv, tp),
        name="decode_step",
        out_shape=(
            jax.ShapeDtypeStruct((rows, feats), BF16),
            jax.ShapeDtypeStruct(past_state.shape, F32),
        ),
        in_specs=[pl.BlockSpec(memory_space=pltpu.HBM)] * 14,
        out_specs=(in_vmem, in_vmem),
        scratch_shapes=[
            pltpu.VMEM((rows, feats), BF16),
            pltpu.VMEM((1, tp * feats), F32),
            pltpu.VMEM((heads_local, dk), F32),
            pltpu.VMEM((1, dv), F32),
            pltpu.VMEM((kv, tp * feats), F32),
            pltpu.VMEM((rows // 2, 2 * feats), BF16),
            pltpu.VMEM((rows // 2, 2 * feats), BF16),
            pltpu.VMEM((4, *w_query.shape), BF16),
            pltpu.VMEM(past_state.shape, F32),
            pltpu.VMEM((2, feats, channels), BF16),
            pltpu.VMEM((4, units, half_cols), BF16),
            pltpu.VMEM((2, units, half_cols), BF16),
            pltpu.VMEM((group, dk), F32),
            pltpu.VMEM((group, dv), F32),
            pltpu.VMEM((kv, 4 * group, dk), BF16),
            pltpu.VMEM((kv, 4 * group, dk), BF16),
            pltpu.VMEM((kv, seqs, dk), F32),
            pltpu.VMEM((kv, seqs, dk), F32),
            pltpu.VMEM((4 * group + 8, dk), F32),
            pltpu.VMEM((kv, 4 * group, dk), BF16),
            pltpu.VMEM((kv, 4 * group, dk), BF16),
            pltpu.VMEM((kv, seqs, dk), F32),
            pltpu.VMEM((4 * group + 8, dk), F32),
            pltpu.VMEM((4 * group + 8, dk), F32),
            pltpu.VMEM((group, dv), BF16),
            pltpu.VMEM((kv, group, dv), BF16),
            pltpu.VMEM((rows // 2, 2 * feats), F32),
            pltpu.VMEM((rows // 2, 2 * feats), F32),
            pltpu.VMEM((rows // 2, 2 * feats), BF16),
            pltpu.VMEM((kv, rows // 2, 2 * feats), BF16),
            pltpu.VMEM((5, rows, wide), F32),
            pltpu.VMEM((5, rows, wide), F32),
            pltpu.VMEM((kv, rows // 2, 2 * feats), BF16),
            pltpu.VMEM((kv, rows // 2, 2 * feats), BF16),
            dma((11,)),
            dma((7,)),
            dma((7,)),
            *[dma((1,))] * 10,
            dma((kv,)),
            *[dma((1,))] * 4,
            pltpu.SemaphoreType.REGULAR,
            pltpu.SemaphoreType.REGULAR((kv,)),
        ],
        compiler_params=pltpu.CompilerParams(
            collective_id=0, has_side_effects=True, vmem_limit_bytes=VMEM_BYTES
        ),
    )(*hbm(
        tokens,
        past_state,
        mix_gain.reshape(1, -1),
        w_query,
        w_forget,
        w_value,
        w_gate_out,
        floor_logits.reshape(heads_local, dk),
        head_gain.reshape(1, -1),
        w_out.T,
        mlp_gain.reshape(kv, tp * feats),
        w_gate.T,
        w_up.T,
        w_down,
    ))
    return pl.pallas_call(
        write_out,
        name="write_out",
        out_shape=tuple(jax.ShapeDtypeStruct(a.shape, a.dtype) for a in outputs),
        in_specs=[in_vmem] * len(outputs),
        out_specs=(pl.BlockSpec(memory_space=pltpu.HBM),) * len(outputs),
        scratch_shapes=[dma((len(outputs),))],
        compiler_params=pltpu.CompilerParams(vmem_limit_bytes=16 * 1024 * 1024),
    )(*outputs)


def solution(mesh):
    placed = (
        P(("grp", "dp"), ("kv", "tp")),
        P(("grp", "dp", "kv"), "tp", None, None),
        P("kv"),
        P("kv", "tp"),
        P("kv", "tp"),
        P("kv", "tp"),
        P("kv", "tp"),
        P("tp"),
        P(),
        P(None, ("kv", "tp")),
        P(),
        P(None, ("kv", "tp")),
        P(None, ("kv", "tp")),
        P(("kv", "tp"), None),
    )
    return jax.shard_map(
        functools.partial(body, mesh.shape["kv"], mesh.shape["tp"]),
        mesh=mesh,
        in_specs=placed,
        out_specs=(P(("grp", "dp"), ("kv", "tp")), P(("grp", "dp", "kv"), "tp", None, None)),
        check_vma=False,
    )
```

```python
import functools

import jax
import jax.numpy as jnp
from jax import lax
from jax.experimental import pallas as pl
from jax.experimental.pallas import tpu as pltpu
from jax.sharding import PartitionSpec as P

MESH = pl.DeviceIdType.MESH
EPS = 1e-06
VMEM_BYTES = 48 * 1024 * 1024
F32 = jnp.float32
BF16 = jnp.bfloat16


def dot(a, b):
    return jnp.dot(a, b, preferred_element_type=F32)


def dot_t(a, b):
    return lax.dot_general(a, b, (((1,), (1,)), ((), ())), preferred_element_type=F32)


def hbm(*arrays):
    return [pltpu.with_memory_space_constraint(a, pltpu.HBM) for a in arrays]


def packed(x):
    half = x.shape[0] // 2
    return jnp.concatenate([x[:half], x[half:]], axis=1)


def halves_swapped(x):
    return pltpu.roll(x, x.shape[1] // 2, 1)


def kernel(
    kv,
    tp,
    tokens_hbm,
    past_state,
    mix_gain_hbm,
    w_query,
    w_forget,
    w_value,
    w_gate_out,
    floor_hbm,
    head_gain_hbm,
    w_out,
    mlp_gain_hbm,
    w_gate,
    w_up,
    w_down,
    result,
    new_state,
    tokens,
    mix_gain,
    floor_logits,
    head_gain,
    mlp_gain,
    tok_own,
    tok_other,
    proj_w,
    state,
    out_w,
    mlp_w,
    down_w,
    floors,
    heads,
    chunk_out,
    chunk_in,
    sq_out,
    sq_in,
    total,
    joint_in,
    relay_in,
    relay_sq_in,
    relayed_out,
    relayed_in,
    mix_own,
    mix,
    part_out,
    part_in,
    mid_own,
    mid,
    wide_out,
    wide_in,
    terms_out,
    terms_in,
    local_sem,
    pair_send,
    pair_recv,
    rs_send,
    rs_recv,
    sq_send,
    sq_recv,
    mix_send,
    mix_recv,
    mid_send,
    mid_recv,
    term_send,
    term_recv,
    joint_recv,
    relay_recv,
    relay_sq_recv,
    relayed_send,
    relayed_recv,
    pair_in,
    ready,
):
    z = lax.axis_index("kv")
    c = lax.axis_index("tp")
    other = 1 - c
    rows, feats = tokens.shape
    seqs, heads_local, dk, dv = past_state.shape
    units = w_gate.shape[0]
    group = heads_local * seqs
    half_rows = rows // 2
    width = kv * tp * feats
    half_kv = kv // tp
    half_cols = half_kv * tp * feats

    def local(src, dst, i):
        copy = pltpu.make_async_copy(src, dst, local_sem.at[i])
        copy.start()
        return copy

    def remote(src, dst, send, recv, to_z, to_c):
        return pltpu.make_async_remote_copy(
            src_ref=src,
            dst_ref=dst,
            send_sem=send,
            recv_sem=recv,
            device_id={"kv": to_z, "tp": to_c},
            device_id_type=MESH,
        )

    def peer(d):
        return lax.rem(z + d, kv)

    def place(w):
        return jnp.where(w == 0, kv - 2, jnp.where(w == kv - 1, kv - 1, w - 1))

    order = [*range(1, kv - 1), 0, kv - 1]
    last = kv - 1
    near_last = [w for w in range(kv - tp - 2, kv - 1)]
    middle_z = kv // 2
    far_side = list(range(middle_z - 2, middle_z + 2))
    relays = {0: kv // 4, last: near_last[0] - 1}
    behind = near_last[0] - 1
    listeners = {0: [relays[0], *near_last], last: [relays[last], *near_last, 0]}
    far_first = sorted(range(1, kv), key=lambda d: -min(d, kv - d))

    def wait_all(buffer, count, sem, received=True):
        part_of = buffer.at[pl.ds(0, count)]
        copy = remote(part_of, part_of, sem, sem, z, other)
        copy.wait_recv() if received else copy.wait_send()

    barrier = pltpu.get_barrier_semaphore()

    def signal(sem, to_z, to_c):
        pl.semaphore_signal(sem, inc=1, device_id={"kv": to_z, "tp": to_c}, device_id_type=MESH)

    @pl.when(c == 1)
    def _():
        signal(barrier, z, 0)

    tokens_copy = local(tokens_hbm, tokens, 2)
    gain_copy = local(mix_gain_hbm, mix_gain, 3)
    for i, w in enumerate((w_query, w_forget, w_value, w_gate_out)):
        local(w, proj_w.at[i], 0)
    state_copy = local(past_state, state, 1)
    small_copies = [
        local(floor_hbm, floor_logits, 4),
        local(head_gain_hbm, head_gain, 5),
        local(mlp_gain_hbm, mlp_gain, 6),
    ]
    is_special = (z == 0) | (z == last)
    half_of = pl.ds(pl.multiple_of(c * half_cols, half_cols), half_cols)
    half_of_other = pl.ds(pl.multiple_of(other * half_cols, half_cols), half_cols)
    weight_copies = [
        local(w_out.at[:, half_of_other], out_w.at[0], 7),
        local(w_gate.at[:, half_of], mlp_w.at[0], 8),
        local(w_up.at[:, half_of], mlp_w.at[1], 9),
        local(w_down.at[:, half_of], down_w.at[0], 10),
    ]

    @pl.when(c == 0)
    def _():
        pl.semaphore_wait(barrier, 1)
        signal(pair_in, z, 1)

    @pl.when(c == 1)
    def _():
        pl.semaphore_wait(pair_in, 1)
        for w in order:

            @pl.when(place(z) < place(w))
            def _(w=w):
                signal(barrier, w, 1)

    def count_and_tell():
        @pl.when(c == 1)
        def _():
            @pl.when(place(z) > 0)
            def _():
                pl.semaphore_wait(barrier, place(z))

            signal(pair_in, z, 0)

        @pl.when(c == 0)
        def _():
            pl.semaphore_wait(pair_in, 1)

        for special, told in listeners.items():

            @pl.when(z == special)
            def _(special=special, told=told):
                for w in told:
                    if order.index(w) < order.index(special):
                        signal(ready.at[special], w, c)

        for d in far_first:
            to = peer(d)

            @pl.when((place(to) < place(z)) & (place(z) < kv - 2))
            def _(to=to):
                signal(ready.at[z], to, c)

    @pl.when(z != last)
    def _():
        count_and_tell()

    tokens_copy.wait()
    own = tokens[...].astype(F32)
    tok_own[...] = packed(own).astype(BF16)
    tok = remote(tok_own, tok_other, pair_send.at[0], pair_recv.at[0], z, other)
    tok.start()

    r = lax.broadcasted_iota(jnp.int32, (kv * group, kv * group), 0)
    col = lax.broadcasted_iota(jnp.int32, (kv * group, kv * group), 1)
    s_of = lax.rem(r, seqs)
    to_chunks = lax.rem(r // seqs, heads_local) * (kv * seqs) + (r // group) * seqs + s_of
    spread = jnp.where(col == to_chunks, 1.0, 0.0).astype(BF16)
    to_heads = lax.rem(r // seqs, kv) * group + (r // (kv * seqs)) * seqs + s_of
    gather = jnp.where(col == to_heads, 1.0, 0.0).astype(BF16)

    lane = lax.broadcasted_iota(jnp.int32, (1, tp * feats), 1)
    low = lane < feats
    own_twice = jnp.concatenate([own, own], axis=1)
    tok.wait_recv()

    @pl.when(z == last)
    def _():
        count_and_tell()

    got = tok_other[...].astype(F32)
    got_swapped = halves_swapped(got)
    got_twice = jnp.concatenate(
        [jnp.where(low, got, got_swapped), jnp.where(low, got_swapped, got)], axis=0
    )
    mine = lax.broadcasted_iota(jnp.int32, (rows, tp * feats), 1) // feats == c
    block = jnp.where(mine, own_twice, got_twice)
    squares = jnp.sum(block * block, axis=1, keepdims=True)
    sq_out[...] = jnp.broadcast_to(squares, (rows, dk)).reshape(kv, seqs, dk)
    gain_copy.wait()
    gained = (block * mix_gain[...]).astype(BF16)
    def sq_copy(to):
        return remote(sq_out.at[to], sq_in.at[z], sq_send.at[0], sq_recv.at[0], to, c)

    def chunk_copy(to):
        return remote(chunk_out.at[to], chunk_in.at[z], rs_send.at[0], rs_recv.at[0], to, c)

    def sq_to_relay(special):
        return remote(
            sq_out.at[special], relay_sq_in.at[z - 1], sq_send.at[0], relay_sq_recv.at[0], relays[special], c
        )

    def chunk_to_relay(special):
        return remote(
            chunk_out.at[special], relay_in.at[z - 1], rs_send.at[0], relay_recv.at[0], relays[special], c
        )

    for d in far_first:
        to = peer(d)

        @pl.when(place(to) < place(z))
        def _(to=to):
            sq_copy(to).start()

    for special, relay in relays.items():

        @pl.when((z > relay) & (z <= behind))
        def _(special=special):
            sq_to_relay(special).start()

    pltpu.make_async_copy(proj_w, proj_w, local_sem.at[0]).wait()
    products = [dot(gained, proj_w[i]).astype(BF16) for i in range(4)]
    for i in (0, 2):
        stack = jnp.concatenate(
            [
                jnp.concatenate([p[:, h * dk : (h + 1) * dk] for p in products[i : i + 2]], axis=1)
                for h in range(heads_local)
            ],
            axis=0,
        )
        ordered = dot(spread, stack).astype(BF16)
        for j in range(2):
            chunk_out[:, pl.ds((i + j) * group, group), :] = ordered[:, j * dk : (j + 1) * dk].reshape(
                kv, group, dk
            )

    for d in far_first:
        to = peer(d)

        @pl.when((place(to) < place(z)) & jnp.logical_not(is_special))
        def _(to=to):
            chunk_copy(to).start()

    for special in (0, last):

        @pl.when(z == special)
        def _(special=special):
            for w in sorted(far_side, key=lambda w: -min(abs(w - special), kv - abs(w - special))):
                chunk_copy(w).start()

    for special, relay in relays.items():

        @pl.when((z > relay) & (z <= behind))
        def _(special=special):
            chunk_to_relay(special).start()

    swaps = [
        remote(w_out.at[:, half_of], out_w.at[1], pair_send.at[1], pair_recv.at[1], z, other),
        remote(w_gate.at[:, half_of_other], mlp_w.at[2], pair_send.at[2], pair_recv.at[2], z, other),
        remote(w_up.at[:, half_of_other], mlp_w.at[3], pair_send.at[3], pair_recv.at[3], z, other),
        remote(w_down.at[:, half_of_other], down_w.at[1], pair_send.at[4], pair_recv.at[4], z, other),
    ]
    @pl.when(jnp.logical_not(is_special))
    def _():
        for s in swaps:
            s.start()


    sq_in[z] = sq_out[z]
    chunk_in[z] = chunk_out[z]
    for copy in small_copies:
        copy.wait()
    lower_in = jax.nn.sigmoid(floor_logits[...])
    for h in range(heads_local):
        floors[pl.ds(h * seqs, seqs), :] = jnp.broadcast_to(lower_in[h : h + 1], (seqs, dk))

    for w in order[:-2]:

        @pl.when(place(z) < place(w))
        def _(w=w):
            pl.semaphore_wait(ready.at[w], 1)
            sq_copy(w).start()
            chunk_copy(w).start()
            for special, relay in relays.items():
                if relay == w:
                    sq_to_relay(special).start()
                    chunk_to_relay(special).start()

    for special, relay in relays.items():
        forward = remote(relayed_out, relayed_in, relayed_send.at[0], relayed_recv.at[0], special, c)

        @pl.when(z == relay)
        def _(special=special, forward=forward):
            wait_all(relay_sq_in, behind - 1, relay_sq_recv.at[0])
            wait_all(relay_in, behind - 1, relay_recv.at[0])
            relay_sq_in[z - 1] = sq_out[special]
            relay_in[z - 1] = chunk_out[special]
            sums = relay_in[0].astype(F32)
            squares = relay_sq_in[0]
            for i in range(1, behind):
                sums = sums + relay_in[i].astype(F32)
                squares = squares + relay_sq_in[i]
            relayed_out[pl.ds(0, 4 * group), :] = sums
            relayed_out[pl.ds(4 * group, seqs), :] = squares
            pl.semaphore_wait(ready.at[special], 1)
            forward.start()

        for w in listeners[special]:
            if w != relay and order.index(w) < order.index(special):

                @pl.when(z == w)
                def _(special=special):
                    pl.semaphore_wait(ready.at[special], 1)
                    sq_copy(special).start()
                    chunk_copy(special).start()

    sides = {0: list(range(far_side[0] - 1, 0, -1)), last: list(range(far_side[-1] + 1, last))}
    is_far = (z >= far_side[0]) & (z <= far_side[-1])

    @pl.when(jnp.logical_not(is_far | is_special))
    def _():
        chunk_in[last] = jnp.zeros(chunk_in.shape[1:], BF16)

    for special, partner in ((last, 0), (0, last)):

        @pl.when(z == special)
        def _(special=special, partner=partner):
            for w in sides[partner]:
                remote(
                    chunk_out.at[w], joint_in.at[w], rs_send.at[0], joint_recv.at[w], partner, c
                ).start()
            if special == last:
                chunk_copy(partner).start()
            for w in sides[special]:
                remote(joint_in.at[w], joint_in.at[w], joint_recv.at[w], joint_recv.at[w], z, other).wait_recv()
                chunk_out[w] = (chunk_out[w].astype(F32) + joint_in[w].astype(F32)).astype(BF16)
                remote(chunk_out.at[w], chunk_in.at[0], rs_send.at[0], rs_recv.at[0], w, c).start()

    def add_up(slots):
        sums = chunk_in[slots[0]].astype(F32)
        squares = sq_in[slots[0]]
        for w in slots[1:]:
            sums = sums + chunk_in[w].astype(F32)
            squares = squares + sq_in[w]
        return sums, squares

    is_special = (z == 0) | (z == last)

    @pl.when(jnp.logical_not(is_special))
    def _():
        wait_all(sq_in, kv - 1, sq_recv.at[0])
        @pl.when(is_far)
        def _():
            wait_all(chunk_in, kv - 1, rs_recv.at[0])

        @pl.when(jnp.logical_not(is_far))
        def _():
            wait_all(chunk_in, kv - 2, rs_recv.at[0])

        sums, squares = add_up(order)
        total[pl.ds(0, 4 * group), :] = sums
        total[pl.ds(4 * group, seqs), :] = squares

    @pl.when(is_special)
    def _():
        wait_all(sq_in, len(near_last) + 1, sq_recv.at[0])
        wait_all(chunk_in, len(near_last) + 1, rs_recv.at[0])
        sums, squares = add_up([*near_last, 0, last])
        remote(relayed_out, relayed_in, relayed_send.at[0], relayed_recv.at[0], z, other).wait_recv()
        total[pl.ds(0, 4 * group), :] = sums + relayed_in[pl.ds(0, 4 * group), :]
        total[pl.ds(4 * group, seqs), :] = squares + relayed_in[pl.ds(4 * group, seqs), :]
        for s in swaps:
            s.start()

    total_sq = total[pl.ds(4 * group, seqs), :]
    scale_s = lax.rsqrt(total_sq / width + EPS)
    row_of = lax.broadcasted_iota(jnp.int32, (group, dk), 0)
    scale = jnp.broadcast_to(scale_s[0:1], (group, dk))
    for s in range(1, seqs):
        scale = jnp.where(lax.rem(row_of, seqs) == s, jnp.broadcast_to(scale_s[s : s + 1], (group, dk)), scale)
    query = total[pl.ds(0, group), :] * scale
    forget_pre = total[pl.ds(group, group), :] * scale
    value = total[pl.ds(2 * group, group), :] * scale
    gate_pre = total[pl.ds(3 * group, group), :] * scale
    lower = floors[...]
    forget = lower + (1.0 - lower) * jax.nn.sigmoid(forget_pre)
    activ = query * jax.nn.sigmoid(query)
    columns = jnp.concatenate([forget, activ, jnp.zeros((dk - 2 * group, dk), F32)], axis=0).T

    state_copy.wait()
    for h in range(heads_local):
        for s in range(seqs):
            i = h * seqs + s
            v_row = value[i : i + 1]
            f_col = columns[:, i : i + 1]
            q_col = columns[:, group + i : group + i + 1]
            new = v_row + f_col * (state[s, h] - v_row)
            new_state[s, h] = new
            heads[pl.ds(i, 1), :] = jnp.sum(new * q_col, axis=0, keepdims=True)

    head_out = heads[...]
    normed = head_out * lax.rsqrt(jnp.mean(head_out * head_out, axis=1, keepdims=True) + EPS)
    mixed = normed * head_gain[...] * (gate_pre * jax.nn.sigmoid(gate_pre))
    mix_own[...] = mixed.astype(BF16)
    for d in far_first:
        remote(mix_own, mix.at[z], mix_send.at[0], mix_recv.at[0], peer(d), other).start()
    remote(mix_own, mix.at[z], mix_send.at[0], mix_recv.at[0], z, other).start()
    tok.wait_send()
    is_relay = (z == relays[0]) | (z == relays[last])

    @pl.when(jnp.logical_not(is_relay))
    def _():
        wait_all(sq_in, kv - 1, sq_send.at[0], False)
        wait_all(chunk_in, kv - 1, rs_send.at[0], False)

    @pl.when(is_relay)
    def _():
        wait_all(sq_in, kv - 2, sq_send.at[0], False)
        wait_all(chunk_in, kv - 2, rs_send.at[0], False)
        remote(relayed_out, relayed_in, relayed_send.at[0], relayed_recv.at[0], z, other).wait_send()

    weight_copies[0].wait()
    swaps[0].wait_recv()
    wait_all(mix, kv, mix_recv.at[0])
    by_head = dot(gather, mix[...].reshape(kv * group, dv)).astype(BF16)
    every = jnp.concatenate([by_head[h * rows : (h + 1) * rows] for h in range(heads_local)], axis=1)
    part_out[...] = packed(dot_t(every, out_w[1]))
    part = remote(part_out, part_in, pair_send.at[5], pair_recv.at[5], z, other)
    part.start()
    kept = packed(dot_t(every, out_w[0])) + packed(own)
    part.wait_recv()
    middle = (kept + part_in[...]).astype(BF16)
    mid_own[...] = middle
    half = z // half_kv
    half_z = lax.rem(z, half_kv)
    kept_here = half == c
    for d in far_first:
        remote(mid_own, mid.at[half_z * tp + c], mid_send.at[0], mid_recv.at[0], peer(d), half).start()

    @pl.when(kept_here)
    def _():
        mid[half_z * tp + c] = middle

    @pl.when(jnp.logical_not(kept_here))
    def _():
        remote(mid_own, mid.at[half_z * tp + c], mid_send.at[0], mid_recv.at[0], z, half).start()

    part.wait_send()
    wait_all(mix, kv, mix_send.at[0], False)
    for copy in swaps:
        copy.wait_send()
    gain = mlp_gain[pl.ds(pl.multiple_of(c * half_kv, half_kv), half_kv), :]
    for w in weight_copies[1:]:
        w.wait()
    for s in swaps[1:]:
        s.wait_recv()
    def wait_others(buffer, sem, received=True):
        @pl.when(kept_here)
        def _():
            wait_all(buffer, kv - 1, sem, received)

        @pl.when(jnp.logical_not(kept_here))
        def _():
            wait_all(buffer, kv, sem, received)

    wait_others(mid, mid_recv.at[0])
    tops, bottoms = [], []
    squares = jnp.zeros((half_rows, tp * feats), F32)
    for i in range(half_kv):
        a = mid[tp * i].astype(F32)
        b = mid[tp * i + 1].astype(F32)
        squares = squares + a * a + b * b
        g = gain[i : i + 1]
        tops.append((jnp.where(low, a, halves_swapped(b)) * g).astype(BF16))
        bottoms.append((jnp.where(low, halves_swapped(a), b) * g).astype(BF16))
    features = jnp.concatenate(
        [jnp.concatenate(tops, axis=1), jnp.concatenate(bottoms, axis=1)], axis=0
    )
    sq_top = jnp.sum(jnp.where(low, squares, 0.0), axis=1, keepdims=True)
    sq_bottom = jnp.sum(jnp.where(low, 0.0, squares), axis=1, keepdims=True)
    sq_mid = jnp.concatenate([sq_top, sq_bottom], axis=0)
    wide_out[4, :, :] = jnp.broadcast_to(sq_mid, wide_out.shape[1:])
    sums = [dot_t(features, mlp_w[i]) for i in range(4)]
    for i in range(4):
        wide_out[i, :, pl.ds(0, units)] = sums[i]
    remote(wide_out, wide_in, pair_send.at[6], pair_recv.at[6], z, other).start()
    remote(wide_out, wide_in, pair_send.at[6], pair_recv.at[6], z, other).wait_recv()
    mlp_scale = lax.rsqrt((sq_mid + wide_in[4, :, 0:1]) / width + EPS)
    terms = None
    for i in range(2):
        gate = (sums[2 * i] + wide_in[2 - 2 * i, :, pl.ds(0, units)]) * mlp_scale
        upward = (sums[2 * i + 1] + wide_in[3 - 2 * i, :, pl.ds(0, units)]) * mlp_scale
        hidden = (gate * jax.nn.sigmoid(gate) * upward).astype(BF16)
        term = dot(hidden, down_w[i])
        terms = term if terms is None else terms + term

    for i in range(half_kv):
        at = slice(i * tp * feats, (i + 1) * tp * feats)
        top, bottom = terms[:half_rows, at], terms[half_rows:, at]
        to = c * half_kv + i
        for to_c, message in (
            (0, jnp.where(low, top, halves_swapped(bottom))),
            (1, jnp.where(low, halves_swapped(top), bottom)),
        ):
            n = 2 * i + to_c
            terms_out[n] = message.astype(BF16)
            copy = remote(terms_out.at[n], terms_in.at[z], term_send.at[0], term_recv.at[0], to, to_c)
            to_self = jnp.logical_and(to == z, to_c == c)

            @pl.when(jnp.logical_not(to_self))
            def _(copy=copy):
                copy.start()

            @pl.when(to_self)
            def _(n=n):
                terms_in[z] = terms_out[n]

    remote(wide_out, wide_in, pair_send.at[6], pair_recv.at[6], z, other).wait_send()
    wait_others(mid, mid_send.at[0], False)
    wait_others(terms_in, term_recv.at[0])
    summed = middle.astype(F32) + jnp.sum(terms_in[...].astype(F32), axis=0)
    result[pl.ds(0, half_rows), :] = summed[:, :feats].astype(BF16)
    result[pl.ds(half_rows, half_rows), :] = summed[:, feats:].astype(BF16)

    wait_others(terms_in, term_send.at[0], False)


def write_out(result, new_state, result_out, new_state_out, sem):
    copies = [
        pltpu.make_async_copy(new_state, new_state_out, sem.at[0]),
        pltpu.make_async_copy(result, result_out, sem.at[1]),
    ]
    for copy in copies:
        copy.start()
    for copy in copies:
        copy.wait()


def body(
    kv,
    tp,
    tokens,
    past_state,
    mix_gain,
    w_query,
    w_forget,
    w_value,
    w_gate_out,
    floor_logits,
    head_gain,
    w_out,
    mlp_gain,
    w_gate,
    w_up,
    w_down,
):
    rows, feats = tokens.shape
    seqs, heads_local, dk, dv = past_state.shape
    units = w_gate.shape[1]
    group = heads_local * seqs
    channels = heads_local * dv
    half_cols = w_down.shape[1] // tp
    wide = -(-units // 128) * 128
    in_vmem = pl.BlockSpec(memory_space=pltpu.VMEM)
    dma = pltpu.SemaphoreType.DMA
    outputs = pl.pallas_call(
        functools.partial(kernel, kv, tp),
        name="decode_step",
        out_shape=(
            jax.ShapeDtypeStruct((rows, feats), BF16),
            jax.ShapeDtypeStruct(past_state.shape, F32),
        ),
        in_specs=[pl.BlockSpec(memory_space=pltpu.HBM)] * 14,
        out_specs=(in_vmem, in_vmem),
        scratch_shapes=[
            pltpu.VMEM((rows, feats), BF16),
            pltpu.VMEM((1, tp * feats), F32),
            pltpu.VMEM((heads_local, dk), F32),
            pltpu.VMEM((1, dv), F32),
            pltpu.VMEM((kv, tp * feats), F32),
            pltpu.VMEM((rows // 2, 2 * feats), BF16),
            pltpu.VMEM((rows // 2, 2 * feats), BF16),
            pltpu.VMEM((4, *w_query.shape), BF16),
            pltpu.VMEM(past_state.shape, F32),
            pltpu.VMEM((2, feats, channels), BF16),
            pltpu.VMEM((4, units, half_cols), BF16),
            pltpu.VMEM((2, units, half_cols), BF16),
            pltpu.VMEM((group, dk), F32),
            pltpu.VMEM((group, dv), F32),
            pltpu.VMEM((kv, 4 * group, dk), BF16),
            pltpu.VMEM((kv, 4 * group, dk), BF16),
            pltpu.VMEM((kv, seqs, dk), F32),
            pltpu.VMEM((kv, seqs, dk), F32),
            pltpu.VMEM((4 * group + 8, dk), F32),
            pltpu.VMEM((kv, 4 * group, dk), BF16),
            pltpu.VMEM((kv, 4 * group, dk), BF16),
            pltpu.VMEM((kv, seqs, dk), F32),
            pltpu.VMEM((4 * group + 8, dk), F32),
            pltpu.VMEM((4 * group + 8, dk), F32),
            pltpu.VMEM((group, dv), BF16),
            pltpu.VMEM((kv, group, dv), BF16),
            pltpu.VMEM((rows // 2, 2 * feats), F32),
            pltpu.VMEM((rows // 2, 2 * feats), F32),
            pltpu.VMEM((rows // 2, 2 * feats), BF16),
            pltpu.VMEM((kv, rows // 2, 2 * feats), BF16),
            pltpu.VMEM((5, rows, wide), F32),
            pltpu.VMEM((5, rows, wide), F32),
            pltpu.VMEM((kv, rows // 2, 2 * feats), BF16),
            pltpu.VMEM((kv, rows // 2, 2 * feats), BF16),
            dma((11,)),
            dma((7,)),
            dma((7,)),
            *[dma((1,))] * 10,
            dma((kv,)),
            *[dma((1,))] * 4,
            pltpu.SemaphoreType.REGULAR,
            pltpu.SemaphoreType.REGULAR((kv,)),
        ],
        compiler_params=pltpu.CompilerParams(
            collective_id=0, has_side_effects=True, vmem_limit_bytes=VMEM_BYTES
        ),
    )(*hbm(
        tokens,
        past_state,
        mix_gain.reshape(1, -1),
        w_query,
        w_forget,
        w_value,
        w_gate_out,
        floor_logits.reshape(heads_local, dk),
        head_gain.reshape(1, -1),
        w_out.T,
        mlp_gain.reshape(kv, tp * feats),
        w_gate.T,
        w_up.T,
        w_down,
    ))
    return pl.pallas_call(
        write_out,
        name="write_out",
        out_shape=tuple(jax.ShapeDtypeStruct(a.shape, a.dtype) for a in outputs),
        in_specs=[in_vmem] * len(outputs),
        out_specs=(pl.BlockSpec(memory_space=pltpu.HBM),) * len(outputs),
        scratch_shapes=[dma((len(outputs),))],
        compiler_params=pltpu.CompilerParams(vmem_limit_bytes=16 * 1024 * 1024),
    )(*outputs)


def solution(mesh):
    placed = (
        P(("grp", "dp"), ("kv", "tp")),
        P(("grp", "dp", "kv"), "tp", None, None),
        P("kv"),
        P("kv", "tp"),
        P("kv", "tp"),
        P("kv", "tp"),
        P("kv", "tp"),
        P("tp"),
        P(),
        P(None, ("kv", "tp")),
        P(),
        P(None, ("kv", "tp")),
        P(None, ("kv", "tp")),
        P(("kv", "tp"), None),
    )
    return jax.shard_map(
        functools.partial(body, mesh.shape["kv"], mesh.shape["tp"]),
        mesh=mesh,
        in_specs=placed,
        out_specs=(P(("grp", "dp"), ("kv", "tp")), P(("grp", "dp", "kv"), "tp", None, None)),
        check_vma=False,
    )
```

```python
import functools

import jax
import jax.numpy as jnp
from jax import lax
from jax.experimental import pallas as pl
from jax.experimental.pallas import tpu as pltpu
from jax.sharding import PartitionSpec as P

MESH = pl.DeviceIdType.MESH
EPS = 1e-06
VMEM_BYTES = 48 * 1024 * 1024
F32 = jnp.float32
BF16 = jnp.bfloat16


def dot(a, b):
    return jnp.dot(a, b, preferred_element_type=F32)


def dot_t(a, b):
    return lax.dot_general(a, b, (((1,), (1,)), ((), ())), preferred_element_type=F32)


def hbm(*arrays):
    return [pltpu.with_memory_space_constraint(a, pltpu.HBM) for a in arrays]


def packed(x):
    half = x.shape[0] // 2
    return jnp.concatenate([x[:half], x[half:]], axis=1)


def halves_swapped(x):
    return pltpu.roll(x, x.shape[1] // 2, 1)


def kernel(
    kv,
    tp,
    tokens_hbm,
    past_state,
    mix_gain_hbm,
    w_query,
    w_forget,
    w_value,
    w_gate_out,
    floor_hbm,
    head_gain_hbm,
    w_out,
    mlp_gain_hbm,
    w_gate,
    w_up,
    w_down,
    result,
    new_state,
    tokens,
    mix_gain,
    floor_logits,
    head_gain,
    mlp_gain,
    tok_own,
    tok_other,
    proj_w,
    state,
    out_w,
    mlp_w,
    down_w,
    floors,
    heads,
    chunk_out,
    chunk_in,
    sq_out,
    sq_in,
    total,
    joint_in,
    relay_in,
    relay_sq_in,
    relayed_out,
    relayed_in,
    mix_own,
    mix,
    part_out,
    part_in,
    mid_own,
    mid,
    wide_out,
    wide_in,
    terms_out,
    terms_in,
    local_sem,
    pair_send,
    pair_recv,
    rs_send,
    rs_recv,
    sq_send,
    sq_recv,
    mix_send,
    mix_recv,
    mid_send,
    mid_recv,
    term_send,
    term_recv,
    joint_recv,
    relay_recv,
    relay_sq_recv,
    relayed_send,
    relayed_recv,
    pair_in,
    ready,
):
    z = lax.axis_index("kv")
    c = lax.axis_index("tp")
    other = 1 - c
    rows, feats = tokens.shape
    seqs, heads_local, dk, dv = past_state.shape
    units = w_gate.shape[0]
    group = heads_local * seqs
    half_rows = rows // 2
    width = kv * tp * feats
    half_kv = kv // tp
    half_cols = half_kv * tp * feats

    def local(src, dst, i):
        copy = pltpu.make_async_copy(src, dst, local_sem.at[i])
        copy.start()
        return copy

    def remote(src, dst, send, recv, to_z, to_c):
        return pltpu.make_async_remote_copy(
            src_ref=src,
            dst_ref=dst,
            send_sem=send,
            recv_sem=recv,
            device_id={"kv": to_z, "tp": to_c},
            device_id_type=MESH,
        )

    def peer(d):
        return lax.rem(z + d, kv)

    def place(w):
        return jnp.where(w == 0, kv - 2, jnp.where(w == kv - 1, kv - 1, w - 1))

    order = [*range(1, kv - 1), 0, kv - 1]
    last = kv - 1
    near_last = [w for w in range(kv - tp - 2, kv - 1)]
    middle_z = kv // 2
    far_side = list(range(middle_z - 3, middle_z + 3))
    relays = {0: kv // 4, last: near_last[0] - 1}
    behind = near_last[0] - 1
    listeners = {0: [relays[0], *near_last], last: [relays[last], *near_last, 0]}
    far_first = sorted(range(1, kv), key=lambda d: -min(d, kv - d))

    def wait_all(buffer, count, sem, received=True):
        part_of = buffer.at[pl.ds(0, count)]
        copy = remote(part_of, part_of, sem, sem, z, other)
        copy.wait_recv() if received else copy.wait_send()

    barrier = pltpu.get_barrier_semaphore()

    def signal(sem, to_z, to_c):
        pl.semaphore_signal(sem, inc=1, device_id={"kv": to_z, "tp": to_c}, device_id_type=MESH)

    @pl.when(c == 1)
    def _():
        signal(barrier, z, 0)

    tokens_copy = local(tokens_hbm, tokens, 2)
    gain_copy = local(mix_gain_hbm, mix_gain, 3)
    for i, w in enumerate((w_query, w_forget, w_value, w_gate_out)):
        local(w, proj_w.at[i], 0)
    state_copy = local(past_state, state, 1)
    small_copies = [
        local(floor_hbm, floor_logits, 4),
        local(head_gain_hbm, head_gain, 5),
        local(mlp_gain_hbm, mlp_gain, 6),
    ]
    is_special = (z == 0) | (z == last)
    half_of = pl.ds(pl.multiple_of(c * half_cols, half_cols), half_cols)
    half_of_other = pl.ds(pl.multiple_of(other * half_cols, half_cols), half_cols)
    weight_copies = [
        local(w_out.at[:, half_of_other], out_w.at[0], 7),
        local(w_gate.at[:, half_of], mlp_w.at[0], 8),
        local(w_up.at[:, half_of], mlp_w.at[1], 9),
        local(w_down.at[:, half_of], down_w.at[0], 10),
    ]

    @pl.when(c == 0)
    def _():
        pl.semaphore_wait(barrier, 1)
        signal(pair_in, z, 1)

    @pl.when(c == 1)
    def _():
        pl.semaphore_wait(pair_in, 1)
        for w in order:

            @pl.when(place(z) < place(w))
            def _(w=w):
                signal(barrier, w, 1)

    def count_and_tell():
        @pl.when(c == 1)
        def _():
            @pl.when(place(z) > 0)
            def _():
                pl.semaphore_wait(barrier, place(z))

            signal(pair_in, z, 0)

        @pl.when(c == 0)
        def _():
            pl.semaphore_wait(pair_in, 1)

        for special, told in listeners.items():

            @pl.when(z == special)
            def _(special=special, told=told):
                for w in told:
                    if order.index(w) < order.index(special):
                        signal(ready.at[special], w, c)

        for d in far_first:
            to = peer(d)

            @pl.when((place(to) < place(z)) & (place(z) < kv - 2))
            def _(to=to):
                signal(ready.at[z], to, c)

    @pl.when(z != last)
    def _():
        count_and_tell()

    tokens_copy.wait()
    own = tokens[...].astype(F32)
    tok_own[...] = packed(own).astype(BF16)
    tok = remote(tok_own, tok_other, pair_send.at[0], pair_recv.at[0], z, other)
    tok.start()

    r = lax.broadcasted_iota(jnp.int32, (kv * group, kv * group), 0)
    col = lax.broadcasted_iota(jnp.int32, (kv * group, kv * group), 1)
    s_of = lax.rem(r, seqs)
    to_chunks = lax.rem(r // seqs, heads_local) * (kv * seqs) + (r // group) * seqs + s_of
    spread = jnp.where(col == to_chunks, 1.0, 0.0).astype(BF16)
    to_heads = lax.rem(r // seqs, kv) * group + (r // (kv * seqs)) * seqs + s_of
    gather = jnp.where(col == to_heads, 1.0, 0.0).astype(BF16)

    lane = lax.broadcasted_iota(jnp.int32, (1, tp * feats), 1)
    low = lane < feats
    own_twice = jnp.concatenate([own, own], axis=1)
    tok.wait_recv()

    @pl.when(z == last)
    def _():
        count_and_tell()

    got = tok_other[...].astype(F32)
    got_swapped = halves_swapped(got)
    got_twice = jnp.concatenate(
        [jnp.where(low, got, got_swapped), jnp.where(low, got_swapped, got)], axis=0
    )
    mine = lax.broadcasted_iota(jnp.int32, (rows, tp * feats), 1) // feats == c
    block = jnp.where(mine, own_twice, got_twice)
    squares = jnp.sum(block * block, axis=1, keepdims=True)
    sq_out[...] = jnp.broadcast_to(squares, (rows, dk)).reshape(kv, seqs, dk)
    gain_copy.wait()
    gained = (block * mix_gain[...]).astype(BF16)
    def sq_copy(to):
        return remote(sq_out.at[to], sq_in.at[z], sq_send.at[0], sq_recv.at[0], to, c)

    def chunk_copy(to):
        return remote(chunk_out.at[to], chunk_in.at[z], rs_send.at[0], rs_recv.at[0], to, c)

    def sq_to_relay(special):
        return remote(
            sq_out.at[special], relay_sq_in.at[z - 1], sq_send.at[0], relay_sq_recv.at[0], relays[special], c
        )

    def chunk_to_relay(special):
        return remote(
            chunk_out.at[special], relay_in.at[z - 1], rs_send.at[0], relay_recv.at[0], relays[special], c
        )

    for d in far_first:
        to = peer(d)

        @pl.when(place(to) < place(z))
        def _(to=to):
            sq_copy(to).start()

    for special, relay in relays.items():

        @pl.when((z > relay) & (z <= behind))
        def _(special=special):
            sq_to_relay(special).start()

    pltpu.make_async_copy(proj_w, proj_w, local_sem.at[0]).wait()
    products = [dot(gained, proj_w[i]).astype(BF16) for i in range(4)]
    for i in (0, 2):
        stack = jnp.concatenate(
            [
                jnp.concatenate([p[:, h * dk : (h + 1) * dk] for p in products[i : i + 2]], axis=1)
                for h in range(heads_local)
            ],
            axis=0,
        )
        ordered = dot(spread, stack).astype(BF16)
        for j in range(2):
            chunk_out[:, pl.ds((i + j) * group, group), :] = ordered[:, j * dk : (j + 1) * dk].reshape(
                kv, group, dk
            )

    for d in far_first:
        to = peer(d)

        @pl.when((place(to) < place(z)) & jnp.logical_not(is_special))
        def _(to=to):
            chunk_copy(to).start()

    for special in (0, last):

        @pl.when(z == special)
        def _(special=special):
            for w in sorted(far_side, key=lambda w: -min(abs(w - special), kv - abs(w - special))):
                chunk_copy(w).start()

    for special, relay in relays.items():

        @pl.when((z > relay) & (z <= behind))
        def _(special=special):
            chunk_to_relay(special).start()

    swaps = [
        remote(w_out.at[:, half_of], out_w.at[1], pair_send.at[1], pair_recv.at[1], z, other),
        remote(w_gate.at[:, half_of_other], mlp_w.at[2], pair_send.at[2], pair_recv.at[2], z, other),
        remote(w_up.at[:, half_of_other], mlp_w.at[3], pair_send.at[3], pair_recv.at[3], z, other),
        remote(w_down.at[:, half_of_other], down_w.at[1], pair_send.at[4], pair_recv.at[4], z, other),
    ]
    @pl.when(jnp.logical_not(is_special))
    def _():
        for s in swaps:
            s.start()


    sq_in[z] = sq_out[z]
    chunk_in[z] = chunk_out[z]
    for copy in small_copies:
        copy.wait()
    lower_in = jax.nn.sigmoid(floor_logits[...])
    for h in range(heads_local):
        floors[pl.ds(h * seqs, seqs), :] = jnp.broadcast_to(lower_in[h : h + 1], (seqs, dk))

    for w in order[:-2]:

        @pl.when(place(z) < place(w))
        def _(w=w):
            pl.semaphore_wait(ready.at[w], 1)
            sq_copy(w).start()
            chunk_copy(w).start()
            for special, relay in relays.items():
                if relay == w:
                    sq_to_relay(special).start()
                    chunk_to_relay(special).start()

    for special, relay in relays.items():
        forward = remote(relayed_out, relayed_in, relayed_send.at[0], relayed_recv.at[0], special, c)

        @pl.when(z == relay)
        def _(special=special, forward=forward):
            wait_all(relay_sq_in, behind - 1, relay_sq_recv.at[0])
            wait_all(relay_in, behind - 1, relay_recv.at[0])
            relay_sq_in[z - 1] = sq_out[special]
            relay_in[z - 1] = chunk_out[special]
            sums = relay_in[0].astype(F32)
            squares = relay_sq_in[0]
            for i in range(1, behind):
                sums = sums + relay_in[i].astype(F32)
                squares = squares + relay_sq_in[i]
            relayed_out[pl.ds(0, 4 * group), :] = sums
            relayed_out[pl.ds(4 * group, seqs), :] = squares
            pl.semaphore_wait(ready.at[special], 1)
            forward.start()

        for w in listeners[special]:
            if w != relay and order.index(w) < order.index(special):

                @pl.when(z == w)
                def _(special=special):
                    pl.semaphore_wait(ready.at[special], 1)
                    sq_copy(special).start()
                    chunk_copy(special).start()

    sides = {0: list(range(far_side[0] - 1, 0, -1)), last: list(range(far_side[-1] + 1, last))}
    is_far = (z >= far_side[0]) & (z <= far_side[-1])

    @pl.when(jnp.logical_not(is_far | is_special))
    def _():
        chunk_in[last] = jnp.zeros(chunk_in.shape[1:], BF16)

    for special, partner in ((last, 0), (0, last)):

        @pl.when(z == special)
        def _(special=special, partner=partner):
            for w in sides[partner]:
                remote(
                    chunk_out.at[w], joint_in.at[w], rs_send.at[0], joint_recv.at[w], partner, c
                ).start()
            if special == last:
                chunk_copy(partner).start()
            for w in sides[special]:
                remote(joint_in.at[w], joint_in.at[w], joint_recv.at[w], joint_recv.at[w], z, other).wait_recv()
                chunk_out[w] = (chunk_out[w].astype(F32) + joint_in[w].astype(F32)).astype(BF16)
                remote(chunk_out.at[w], chunk_in.at[0], rs_send.at[0], rs_recv.at[0], w, c).start()

    def add_up(slots):
        sums = chunk_in[slots[0]].astype(F32)
        squares = sq_in[slots[0]]
        for w in slots[1:]:
            sums = sums + chunk_in[w].astype(F32)
            squares = squares + sq_in[w]
        return sums, squares

    is_special = (z == 0) | (z == last)

    @pl.when(jnp.logical_not(is_special))
    def _():
        wait_all(sq_in, kv - 1, sq_recv.at[0])
        @pl.when(is_far)
        def _():
            wait_all(chunk_in, kv - 1, rs_recv.at[0])

        @pl.when(jnp.logical_not(is_far))
        def _():
            wait_all(chunk_in, kv - 2, rs_recv.at[0])

        sums, squares = add_up(order)
        total[pl.ds(0, 4 * group), :] = sums
        total[pl.ds(4 * group, seqs), :] = squares

    @pl.when(is_special)
    def _():
        wait_all(sq_in, len(near_last) + 1, sq_recv.at[0])
        wait_all(chunk_in, len(near_last) + 1, rs_recv.at[0])
        sums, squares = add_up([*near_last, 0, last])
        remote(relayed_out, relayed_in, relayed_send.at[0], relayed_recv.at[0], z, other).wait_recv()
        total[pl.ds(0, 4 * group), :] = sums + relayed_in[pl.ds(0, 4 * group), :]
        total[pl.ds(4 * group, seqs), :] = squares + relayed_in[pl.ds(4 * group, seqs), :]
        for s in swaps:
            s.start()

    total_sq = total[pl.ds(4 * group, seqs), :]
    scale_s = lax.rsqrt(total_sq / width + EPS)
    row_of = lax.broadcasted_iota(jnp.int32, (group, dk), 0)
    scale = jnp.broadcast_to(scale_s[0:1], (group, dk))
    for s in range(1, seqs):
        scale = jnp.where(lax.rem(row_of, seqs) == s, jnp.broadcast_to(scale_s[s : s + 1], (group, dk)), scale)
    query = total[pl.ds(0, group), :] * scale
    forget_pre = total[pl.ds(group, group), :] * scale
    value = total[pl.ds(2 * group, group), :] * scale
    gate_pre = total[pl.ds(3 * group, group), :] * scale
    lower = floors[...]
    forget = lower + (1.0 - lower) * jax.nn.sigmoid(forget_pre)
    activ = query * jax.nn.sigmoid(query)
    columns = jnp.concatenate([forget, activ, jnp.zeros((dk - 2 * group, dk), F32)], axis=0).T

    state_copy.wait()
    for h in range(heads_local):
        for s in range(seqs):
            i = h * seqs + s
            v_row = value[i : i + 1]
            f_col = columns[:, i : i + 1]
            q_col = columns[:, group + i : group + i + 1]
            new = v_row + f_col * (state[s, h] - v_row)
            new_state[s, h] = new
            heads[pl.ds(i, 1), :] = jnp.sum(new * q_col, axis=0, keepdims=True)

    head_out = heads[...]
    normed = head_out * lax.rsqrt(jnp.mean(head_out * head_out, axis=1, keepdims=True) + EPS)
    mixed = normed * head_gain[...] * (gate_pre * jax.nn.sigmoid(gate_pre))
    mix_own[...] = mixed.astype(BF16)
    for d in far_first:
        remote(mix_own, mix.at[z], mix_send.at[0], mix_recv.at[0], peer(d), other).start()
    remote(mix_own, mix.at[z], mix_send.at[0], mix_recv.at[0], z, other).start()
    tok.wait_send()
    is_relay = (z == relays[0]) | (z == relays[last])

    @pl.when(jnp.logical_not(is_relay))
    def _():
        wait_all(sq_in, kv - 1, sq_send.at[0], False)
        wait_all(chunk_in, kv - 1, rs_send.at[0], False)

    @pl.when(is_relay)
    def _():
        wait_all(sq_in, kv - 2, sq_send.at[0], False)
        wait_all(chunk_in, kv - 2, rs_send.at[0], False)
        remote(relayed_out, relayed_in, relayed_send.at[0], relayed_recv.at[0], z, other).wait_send()

    weight_copies[0].wait()
    swaps[0].wait_recv()
    wait_all(mix, kv, mix_recv.at[0])
    by_head = dot(gather, mix[...].reshape(kv * group, dv)).astype(BF16)
    every = jnp.concatenate([by_head[h * rows : (h + 1) * rows] for h in range(heads_local)], axis=1)
    part_out[...] = packed(dot_t(every, out_w[1]))
    part = remote(part_out, part_in, pair_send.at[5], pair_recv.at[5], z, other)
    part.start()
    kept = packed(dot_t(every, out_w[0])) + packed(own)
    part.wait_recv()
    middle = (kept + part_in[...]).astype(BF16)
    mid_own[...] = middle
    half = z // half_kv
    half_z = lax.rem(z, half_kv)
    kept_here = half == c
    for d in far_first:
        remote(mid_own, mid.at[half_z * tp + c], mid_send.at[0], mid_recv.at[0], peer(d), half).start()

    @pl.when(kept_here)
    def _():
        mid[half_z * tp + c] = middle

    @pl.when(jnp.logical_not(kept_here))
    def _():
        remote(mid_own, mid.at[half_z * tp + c], mid_send.at[0], mid_recv.at[0], z, half).start()

    part.wait_send()
    wait_all(mix, kv, mix_send.at[0], False)
    for copy in swaps:
        copy.wait_send()
    gain = mlp_gain[pl.ds(pl.multiple_of(c * half_kv, half_kv), half_kv), :]
    for w in weight_copies[1:]:
        w.wait()
    for s in swaps[1:]:
        s.wait_recv()
    def wait_others(buffer, sem, received=True):
        @pl.when(kept_here)
        def _():
            wait_all(buffer, kv - 1, sem, received)

        @pl.when(jnp.logical_not(kept_here))
        def _():
            wait_all(buffer, kv, sem, received)

    wait_others(mid, mid_recv.at[0])
    tops, bottoms = [], []
    squares = jnp.zeros((half_rows, tp * feats), F32)
    for i in range(half_kv):
        a = mid[tp * i].astype(F32)
        b = mid[tp * i + 1].astype(F32)
        squares = squares + a * a + b * b
        g = gain[i : i + 1]
        tops.append((jnp.where(low, a, halves_swapped(b)) * g).astype(BF16))
        bottoms.append((jnp.where(low, halves_swapped(a), b) * g).astype(BF16))
    features = jnp.concatenate(
        [jnp.concatenate(tops, axis=1), jnp.concatenate(bottoms, axis=1)], axis=0
    )
    sq_top = jnp.sum(jnp.where(low, squares, 0.0), axis=1, keepdims=True)
    sq_bottom = jnp.sum(jnp.where(low, 0.0, squares), axis=1, keepdims=True)
    sq_mid = jnp.concatenate([sq_top, sq_bottom], axis=0)
    wide_out[4, :, :] = jnp.broadcast_to(sq_mid, wide_out.shape[1:])
    sums = [dot_t(features, mlp_w[i]) for i in range(4)]
    for i in range(4):
        wide_out[i, :, pl.ds(0, units)] = sums[i]
    remote(wide_out, wide_in, pair_send.at[6], pair_recv.at[6], z, other).start()
    remote(wide_out, wide_in, pair_send.at[6], pair_recv.at[6], z, other).wait_recv()
    mlp_scale = lax.rsqrt((sq_mid + wide_in[4, :, 0:1]) / width + EPS)
    terms = None
    for i in range(2):
        gate = (sums[2 * i] + wide_in[2 - 2 * i, :, pl.ds(0, units)]) * mlp_scale
        upward = (sums[2 * i + 1] + wide_in[3 - 2 * i, :, pl.ds(0, units)]) * mlp_scale
        hidden = (gate * jax.nn.sigmoid(gate) * upward).astype(BF16)
        term = dot(hidden, down_w[i])
        terms = term if terms is None else terms + term

    for i in range(half_kv):
        at = slice(i * tp * feats, (i + 1) * tp * feats)
        top, bottom = terms[:half_rows, at], terms[half_rows:, at]
        to = c * half_kv + i
        for to_c, message in (
            (0, jnp.where(low, top, halves_swapped(bottom))),
            (1, jnp.where(low, halves_swapped(top), bottom)),
        ):
            n = 2 * i + to_c
            terms_out[n] = message.astype(BF16)
            copy = remote(terms_out.at[n], terms_in.at[z], term_send.at[0], term_recv.at[0], to, to_c)
            to_self = jnp.logical_and(to == z, to_c == c)

            @pl.when(jnp.logical_not(to_self))
            def _(copy=copy):
                copy.start()

            @pl.when(to_self)
            def _(n=n):
                terms_in[z] = terms_out[n]

    remote(wide_out, wide_in, pair_send.at[6], pair_recv.at[6], z, other).wait_send()
    wait_others(mid, mid_send.at[0], False)
    wait_others(terms_in, term_recv.at[0])
    summed = middle.astype(F32) + jnp.sum(terms_in[...].astype(F32), axis=0)
    result[pl.ds(0, half_rows), :] = summed[:, :feats].astype(BF16)
    result[pl.ds(half_rows, half_rows), :] = summed[:, feats:].astype(BF16)

    wait_others(terms_in, term_send.at[0], False)


def write_out(result, new_state, result_out, new_state_out, sem):
    copies = [
        pltpu.make_async_copy(new_state, new_state_out, sem.at[0]),
        pltpu.make_async_copy(result, result_out, sem.at[1]),
    ]
    for copy in copies:
        copy.start()
    for copy in copies:
        copy.wait()


def body(
    kv,
    tp,
    tokens,
    past_state,
    mix_gain,
    w_query,
    w_forget,
    w_value,
    w_gate_out,
    floor_logits,
    head_gain,
    w_out,
    mlp_gain,
    w_gate,
    w_up,
    w_down,
):
    rows, feats = tokens.shape
    seqs, heads_local, dk, dv = past_state.shape
    units = w_gate.shape[1]
    group = heads_local * seqs
    channels = heads_local * dv
    half_cols = w_down.shape[1] // tp
    wide = -(-units // 128) * 128
    in_vmem = pl.BlockSpec(memory_space=pltpu.VMEM)
    dma = pltpu.SemaphoreType.DMA
    outputs = pl.pallas_call(
        functools.partial(kernel, kv, tp),
        name="decode_step",
        out_shape=(
            jax.ShapeDtypeStruct((rows, feats), BF16),
            jax.ShapeDtypeStruct(past_state.shape, F32),
        ),
        in_specs=[pl.BlockSpec(memory_space=pltpu.HBM)] * 14,
        out_specs=(in_vmem, in_vmem),
        scratch_shapes=[
            pltpu.VMEM((rows, feats), BF16),
            pltpu.VMEM((1, tp * feats), F32),
            pltpu.VMEM((heads_local, dk), F32),
            pltpu.VMEM((1, dv), F32),
            pltpu.VMEM((kv, tp * feats), F32),
            pltpu.VMEM((rows // 2, 2 * feats), BF16),
            pltpu.VMEM((rows // 2, 2 * feats), BF16),
            pltpu.VMEM((4, *w_query.shape), BF16),
            pltpu.VMEM(past_state.shape, F32),
            pltpu.VMEM((2, feats, channels), BF16),
            pltpu.VMEM((4, units, half_cols), BF16),
            pltpu.VMEM((2, units, half_cols), BF16),
            pltpu.VMEM((group, dk), F32),
            pltpu.VMEM((group, dv), F32),
            pltpu.VMEM((kv, 4 * group, dk), BF16),
            pltpu.VMEM((kv, 4 * group, dk), BF16),
            pltpu.VMEM((kv, seqs, dk), F32),
            pltpu.VMEM((kv, seqs, dk), F32),
            pltpu.VMEM((4 * group + 8, dk), F32),
            pltpu.VMEM((kv, 4 * group, dk), BF16),
            pltpu.VMEM((kv, 4 * group, dk), BF16),
            pltpu.VMEM((kv, seqs, dk), F32),
            pltpu.VMEM((4 * group + 8, dk), F32),
            pltpu.VMEM((4 * group + 8, dk), F32),
            pltpu.VMEM((group, dv), BF16),
            pltpu.VMEM((kv, group, dv), BF16),
            pltpu.VMEM((rows // 2, 2 * feats), F32),
            pltpu.VMEM((rows // 2, 2 * feats), F32),
            pltpu.VMEM((rows // 2, 2 * feats), BF16),
            pltpu.VMEM((kv, rows // 2, 2 * feats), BF16),
            pltpu.VMEM((5, rows, wide), F32),
            pltpu.VMEM((5, rows, wide), F32),
            pltpu.VMEM((kv, rows // 2, 2 * feats), BF16),
            pltpu.VMEM((kv, rows // 2, 2 * feats), BF16),
            dma((11,)),
            dma((7,)),
            dma((7,)),
            *[dma((1,))] * 10,
            dma((kv,)),
            *[dma((1,))] * 4,
            pltpu.SemaphoreType.REGULAR,
            pltpu.SemaphoreType.REGULAR((kv,)),
        ],
        compiler_params=pltpu.CompilerParams(
            collective_id=0, has_side_effects=True, vmem_limit_bytes=VMEM_BYTES
        ),
    )(*hbm(
        tokens,
        past_state,
        mix_gain.reshape(1, -1),
        w_query,
        w_forget,
        w_value,
        w_gate_out,
        floor_logits.reshape(heads_local, dk),
        head_gain.reshape(1, -1),
        w_out.T,
        mlp_gain.reshape(kv, tp * feats),
        w_gate.T,
        w_up.T,
        w_down,
    ))
    return pl.pallas_call(
        write_out,
        name="write_out",
        out_shape=tuple(jax.ShapeDtypeStruct(a.shape, a.dtype) for a in outputs),
        in_specs=[in_vmem] * len(outputs),
        out_specs=(pl.BlockSpec(memory_space=pltpu.HBM),) * len(outputs),
        scratch_shapes=[dma((len(outputs),))],
        compiler_params=pltpu.CompilerParams(vmem_limit_bytes=16 * 1024 * 1024),
    )(*outputs)


def solution(mesh):
    placed = (
        P(("grp", "dp"), ("kv", "tp")),
        P(("grp", "dp", "kv"), "tp", None, None),
        P("kv"),
        P("kv", "tp"),
        P("kv", "tp"),
        P("kv", "tp"),
        P("kv", "tp"),
        P("tp"),
        P(),
        P(None, ("kv", "tp")),
        P(),
        P(None, ("kv", "tp")),
        P(None, ("kv", "tp")),
        P(("kv", "tp"), None),
    )
    return jax.shard_map(
        functools.partial(body, mesh.shape["kv"], mesh.shape["tp"]),
        mesh=mesh,
        in_specs=placed,
        out_specs=(P(("grp", "dp"), ("kv", "tp")), P(("grp", "dp", "kv"), "tp", None, None)),
        check_vma=False,
    )
```

```python
import functools

import jax
import jax.numpy as jnp
from jax import lax
from jax.experimental import pallas as pl
from jax.experimental.pallas import tpu as pltpu
from jax.sharding import PartitionSpec as P

MESH = pl.DeviceIdType.MESH
EPS = 1e-06
VMEM_BYTES = 48 * 1024 * 1024
F32 = jnp.float32
BF16 = jnp.bfloat16


def dot(a, b):
    return jnp.dot(a, b, preferred_element_type=F32)


def dot_t(a, b):
    return lax.dot_general(a, b, (((1,), (1,)), ((), ())), preferred_element_type=F32)


def hbm(*arrays):
    return [pltpu.with_memory_space_constraint(a, pltpu.HBM) for a in arrays]


def packed(x):
    half = x.shape[0] // 2
    return jnp.concatenate([x[:half], x[half:]], axis=1)


def halves_swapped(x):
    return pltpu.roll(x, x.shape[1] // 2, 1)


def kernel(
    kv,
    tp,
    tokens_hbm,
    past_state,
    mix_gain_hbm,
    w_query,
    w_forget,
    w_value,
    w_gate_out,
    floor_hbm,
    head_gain_hbm,
    w_out,
    mlp_gain_hbm,
    w_gate,
    w_up,
    w_down,
    result,
    new_state,
    tokens,
    mix_gain,
    floor_logits,
    head_gain,
    mlp_gain,
    tok_own,
    tok_other,
    proj_w,
    state,
    out_w,
    mlp_w,
    down_w,
    floors,
    heads,
    chunk_out,
    chunk_in,
    sq_out,
    sq_in,
    total,
    joint_in,
    relay_in,
    relay_sq_in,
    relayed_out,
    relayed_in,
    mix_own,
    mix,
    part_out,
    part_in,
    mid_own,
    mid,
    wide_out,
    wide_in,
    terms_out,
    terms_in,
    local_sem,
    pair_send,
    pair_recv,
    rs_send,
    rs_recv,
    sq_send,
    sq_recv,
    mix_send,
    mix_recv,
    mid_send,
    mid_recv,
    term_send,
    term_recv,
    joint_recv,
    relay_recv,
    relay_sq_recv,
    relayed_send,
    relayed_recv,
    pair_in,
    ready,
):
    z = lax.axis_index("kv")
    c = lax.axis_index("tp")
    other = 1 - c
    rows, feats = tokens.shape
    seqs, heads_local, dk, dv = past_state.shape
    units = w_gate.shape[0]
    group = heads_local * seqs
    half_rows = rows // 2
    width = kv * tp * feats
    half_kv = kv // tp
    half_cols = half_kv * tp * feats

    def local(src, dst, i):
        copy = pltpu.make_async_copy(src, dst, local_sem.at[i])
        copy.start()
        return copy

    def remote(src, dst, send, recv, to_z, to_c):
        return pltpu.make_async_remote_copy(
            src_ref=src,
            dst_ref=dst,
            send_sem=send,
            recv_sem=recv,
            device_id={"kv": to_z, "tp": to_c},
            device_id_type=MESH,
        )

    def peer(d):
        return lax.rem(z + d, kv)

    def place(w):
        return jnp.where(w == 0, kv - 2, jnp.where(w == kv - 1, kv - 1, w - 1))

    order = [*range(1, kv - 1), 0, kv - 1]
    last = kv - 1
    near_last = [w for w in range(kv - tp - 2, kv - 1)]
    middle_z = kv // 2
    far_side = list(range(middle_z - 3, middle_z + 3))
    relays = {0: kv // 4, last: near_last[0] - 1}
    behind = near_last[0] - 1
    listeners = {0: [relays[0], *near_last], last: [relays[last], *near_last, 0]}
    far_first = sorted(range(1, kv), key=lambda d: -min(d, kv - d))

    def wait_all(buffer, count, sem, received=True):
        part_of = buffer.at[pl.ds(0, count)]
        copy = remote(part_of, part_of, sem, sem, z, other)
        copy.wait_recv() if received else copy.wait_send()

    barrier = pltpu.get_barrier_semaphore()

    def signal(sem, to_z, to_c):
        pl.semaphore_signal(sem, inc=1, device_id={"kv": to_z, "tp": to_c}, device_id_type=MESH)

    @pl.when(c == 1)
    def _():
        signal(barrier, z, 0)

    tokens_copy = local(tokens_hbm, tokens, 2)
    gain_copy = local(mix_gain_hbm, mix_gain, 3)
    for i, w in enumerate((w_query, w_forget, w_value, w_gate_out)):
        local(w, proj_w.at[i], 0)
    state_copy = local(past_state, state, 1)
    small_copies = [
        local(floor_hbm, floor_logits, 4),
        local(head_gain_hbm, head_gain, 5),
        local(mlp_gain_hbm, mlp_gain, 6),
    ]
    is_special = (z == 0) | (z == last)
    half_of = pl.ds(pl.multiple_of(c * half_cols, half_cols), half_cols)
    half_of_other = pl.ds(pl.multiple_of(other * half_cols, half_cols), half_cols)
    weight_copies = [
        local(w_out.at[:, half_of_other], out_w.at[0], 7),
        local(w_gate.at[:, half_of], mlp_w.at[0], 8),
        local(w_up.at[:, half_of], mlp_w.at[1], 9),
        local(w_down.at[:, half_of], down_w.at[0], 10),
    ]

    @pl.when(c == 0)
    def _():
        pl.semaphore_wait(barrier, 1)
        signal(pair_in, z, 1)

    @pl.when(c == 1)
    def _():
        pl.semaphore_wait(pair_in, 1)
        for w in order:

            @pl.when(place(z) < place(w))
            def _(w=w):
                signal(barrier, w, 1)

    def count_and_tell():
        @pl.when(c == 1)
        def _():
            @pl.when(place(z) > 0)
            def _():
                pl.semaphore_wait(barrier, place(z))

            signal(pair_in, z, 0)

        @pl.when(c == 0)
        def _():
            pl.semaphore_wait(pair_in, 1)

        for special, told in listeners.items():

            @pl.when(z == special)
            def _(special=special, told=told):
                for w in told:
                    if order.index(w) < order.index(special):
                        signal(ready.at[special], w, c)

        for d in far_first:
            to = peer(d)

            @pl.when((place(to) < place(z)) & (place(z) < kv - 2))
            def _(to=to):
                signal(ready.at[z], to, c)

    @pl.when(z != last)
    def _():
        count_and_tell()

    tokens_copy.wait()
    own = tokens[...].astype(F32)
    tok_own[...] = packed(own).astype(BF16)
    tok = remote(tok_own, tok_other, pair_send.at[0], pair_recv.at[0], z, other)
    tok.start()

    r = lax.broadcasted_iota(jnp.int32, (kv * group, kv * group), 0)
    col = lax.broadcasted_iota(jnp.int32, (kv * group, kv * group), 1)
    s_of = lax.rem(r, seqs)
    to_chunks = lax.rem(r // seqs, heads_local) * (kv * seqs) + (r // group) * seqs + s_of
    spread = jnp.where(col == to_chunks, 1.0, 0.0).astype(BF16)
    to_heads = lax.rem(r // seqs, kv) * group + (r // (kv * seqs)) * seqs + s_of
    gather = jnp.where(col == to_heads, 1.0, 0.0).astype(BF16)

    lane = lax.broadcasted_iota(jnp.int32, (1, tp * feats), 1)
    low = lane < feats
    own_twice = jnp.concatenate([own, own], axis=1)
    tok.wait_recv()

    @pl.when(z == last)
    def _():
        count_and_tell()

    got = tok_other[...].astype(F32)
    got_swapped = halves_swapped(got)
    got_twice = jnp.concatenate(
        [jnp.where(low, got, got_swapped), jnp.where(low, got_swapped, got)], axis=0
    )
    mine = lax.broadcasted_iota(jnp.int32, (rows, tp * feats), 1) // feats == c
    block = jnp.where(mine, own_twice, got_twice)
    squares = jnp.sum(block * block, axis=1, keepdims=True)
    sq_out[...] = jnp.broadcast_to(squares, (rows, dk)).reshape(kv, seqs, dk)
    gain_copy.wait()
    gained = (block * mix_gain[...]).astype(BF16)
    def sq_copy(to):
        return remote(sq_out.at[to], sq_in.at[z], sq_send.at[0], sq_recv.at[0], to, c)

    def chunk_copy(to):
        return remote(chunk_out.at[to], chunk_in.at[z], rs_send.at[0], rs_recv.at[0], to, c)

    def sq_to_relay(special):
        return remote(
            sq_out.at[special], relay_sq_in.at[z - 1], sq_send.at[0], relay_sq_recv.at[0], relays[special], c
        )

    def chunk_to_relay(special):
        return remote(
            chunk_out.at[special], relay_in.at[z - 1], rs_send.at[0], relay_recv.at[0], relays[special], c
        )

    for d in far_first:
        to = peer(d)

        @pl.when(place(to) < place(z))
        def _(to=to):
            sq_copy(to).start()

    for special, relay in relays.items():

        @pl.when((z > relay) & (z <= behind))
        def _(special=special):
            sq_to_relay(special).start()

    pltpu.make_async_copy(proj_w, proj_w, local_sem.at[0]).wait()
    products = [dot(gained, proj_w[i]).astype(BF16) for i in range(4)]
    for i in (0, 2):
        stack = jnp.concatenate(
            [
                jnp.concatenate([p[:, h * dk : (h + 1) * dk] for p in products[i : i + 2]], axis=1)
                for h in range(heads_local)
            ],
            axis=0,
        )
        ordered = dot(spread, stack).astype(BF16)
        for j in range(2):
            chunk_out[:, pl.ds((i + j) * group, group), :] = ordered[:, j * dk : (j + 1) * dk].reshape(
                kv, group, dk
            )

    for d in far_first:
        to = peer(d)

        @pl.when((place(to) < place(z)) & jnp.logical_not(is_special))
        def _(to=to):
            chunk_copy(to).start()

    for special in (0, last):

        @pl.when(z == special)
        def _(special=special):
            for w in sorted(far_side, key=lambda w: -min(abs(w - special), kv - abs(w - special))):
                chunk_copy(w).start()

    for special, relay in relays.items():

        @pl.when((z > relay) & (z <= behind))
        def _(special=special):
            chunk_to_relay(special).start()

    swaps = [
        remote(w_out.at[:, half_of], out_w.at[1], pair_send.at[1], pair_recv.at[1], z, other),
        remote(w_gate.at[:, half_of_other], mlp_w.at[2], pair_send.at[2], pair_recv.at[2], z, other),
        remote(w_up.at[:, half_of_other], mlp_w.at[3], pair_send.at[3], pair_recv.at[3], z, other),
        remote(w_down.at[:, half_of_other], down_w.at[1], pair_send.at[4], pair_recv.at[4], z, other),
    ]
    @pl.when(jnp.logical_not(is_special))
    def _():
        for s in swaps:
            s.start()


    sq_in[z] = sq_out[z]
    chunk_in[z] = chunk_out[z]
    for copy in small_copies:
        copy.wait()
    lower_in = jax.nn.sigmoid(floor_logits[...])
    for h in range(heads_local):
        floors[pl.ds(h * seqs, seqs), :] = jnp.broadcast_to(lower_in[h : h + 1], (seqs, dk))

    for w in order[:-2]:

        @pl.when(place(z) < place(w))
        def _(w=w):
            pl.semaphore_wait(ready.at[w], 1)
            sq_copy(w).start()
            chunk_copy(w).start()
            for special, relay in relays.items():
                if relay == w:
                    sq_to_relay(special).start()
                    chunk_to_relay(special).start()

    for special, relay in relays.items():
        forward = remote(relayed_out, relayed_in, relayed_send.at[0], relayed_recv.at[0], special, c)

        @pl.when(z == relay)
        def _(special=special, forward=forward):
            wait_all(relay_sq_in, behind - 1, relay_sq_recv.at[0])
            wait_all(relay_in, behind - 1, relay_recv.at[0])
            relay_sq_in[z - 1] = sq_out[special]
            relay_in[z - 1] = chunk_out[special]
            sums = relay_in[0].astype(F32)
            squares = relay_sq_in[0]
            for i in range(1, behind):
                sums = sums + relay_in[i].astype(F32)
                squares = squares + relay_sq_in[i]
            relayed_out[pl.ds(0, 4 * group), :] = sums
            relayed_out[pl.ds(4 * group, seqs), :] = squares
            pl.semaphore_wait(ready.at[special], 1)
            forward.start()

        for w in listeners[special]:
            if w != relay and order.index(w) < order.index(special):

                @pl.when(z == w)
                def _(special=special):
                    pl.semaphore_wait(ready.at[special], 1)
                    sq_copy(special).start()
                    chunk_copy(special).start()

    sides = {0: list(range(far_side[0] - 1, 0, -1)), last: list(range(far_side[-1] + 1, last))}
    is_far = (z >= far_side[0]) & (z <= far_side[-1])

    @pl.when(jnp.logical_not(is_far | is_special))
    def _():
        chunk_in[last] = jnp.zeros(chunk_in.shape[1:], BF16)

    for special, partner in ((last, 0), (0, last)):

        @pl.when(z == special)
        def _(special=special, partner=partner):
            for w in sides[partner]:
                remote(
                    chunk_out.at[w], joint_in.at[w], rs_send.at[0], joint_recv.at[w], partner, c
                ).start()
            if special == last:
                chunk_copy(partner).start()
            for w in sides[special]:
                remote(joint_in.at[w], joint_in.at[w], joint_recv.at[w], joint_recv.at[w], z, other).wait_recv()
                chunk_out[w] = (chunk_out[w].astype(F32) + joint_in[w].astype(F32)).astype(BF16)
                remote(chunk_out.at[w], chunk_in.at[0], rs_send.at[0], rs_recv.at[0], w, c).start()

    def add_up(slots):
        sums = chunk_in[slots[0]].astype(F32)
        squares = sq_in[slots[0]]
        for w in slots[1:]:
            sums = sums + chunk_in[w].astype(F32)
            squares = squares + sq_in[w]
        return sums, squares

    is_special = (z == 0) | (z == last)

    @pl.when(jnp.logical_not(is_special))
    def _():
        wait_all(sq_in, kv - 1, sq_recv.at[0])
        @pl.when(is_far)
        def _():
            wait_all(chunk_in, kv - 1, rs_recv.at[0])

        @pl.when(jnp.logical_not(is_far))
        def _():
            wait_all(chunk_in, kv - 2, rs_recv.at[0])

        sums, squares = add_up(order)
        total[pl.ds(0, 4 * group), :] = sums
        total[pl.ds(4 * group, seqs), :] = squares

    @pl.when(is_special)
    def _():
        wait_all(sq_in, len(near_last) + 1, sq_recv.at[0])
        wait_all(chunk_in, len(near_last) + 1, rs_recv.at[0])
        sums, squares = add_up([*near_last, 0, last])
        remote(relayed_out, relayed_in, relayed_send.at[0], relayed_recv.at[0], z, other).wait_recv()
        total[pl.ds(0, 4 * group), :] = sums + relayed_in[pl.ds(0, 4 * group), :]
        total[pl.ds(4 * group, seqs), :] = squares + relayed_in[pl.ds(4 * group, seqs), :]
        for s in swaps:
            s.start()

    total_sq = total[pl.ds(4 * group, seqs), :]
    scale_s = lax.rsqrt(total_sq / width + EPS)
    row_of = lax.broadcasted_iota(jnp.int32, (group, dk), 0)
    scale = jnp.broadcast_to(scale_s[0:1], (group, dk))
    for s in range(1, seqs):
        scale = jnp.where(lax.rem(row_of, seqs) == s, jnp.broadcast_to(scale_s[s : s + 1], (group, dk)), scale)
    query = total[pl.ds(0, group), :] * scale
    forget_pre = total[pl.ds(group, group), :] * scale
    value = total[pl.ds(2 * group, group), :] * scale
    gate_pre = total[pl.ds(3 * group, group), :] * scale
    lower = floors[...]
    forget = lower + (1.0 - lower) * jax.nn.sigmoid(forget_pre)
    activ = query * jax.nn.sigmoid(query)
    columns = jnp.concatenate([forget, activ, jnp.zeros((dk - 2 * group, dk), F32)], axis=0).T

    state_copy.wait()
    for h in range(heads_local):
        for s in range(seqs):
            i = h * seqs + s
            v_row = value[i : i + 1]
            f_col = columns[:, i : i + 1]
            q_col = columns[:, group + i : group + i + 1]
            new = v_row + f_col * (state[s, h] - v_row)
            new_state[s, h] = new
            heads[pl.ds(i, 1), :] = jnp.sum(new * q_col, axis=0, keepdims=True)

    head_out = heads[...]
    normed = head_out * lax.rsqrt(jnp.mean(head_out * head_out, axis=1, keepdims=True) + EPS)
    mixed = normed * head_gain[...] * (gate_pre * jax.nn.sigmoid(gate_pre))
    mix_own[...] = mixed.astype(BF16)
    for d in far_first:
        remote(mix_own, mix.at[z], mix_send.at[0], mix_recv.at[0], peer(d), other).start()
    remote(mix_own, mix.at[z], mix_send.at[0], mix_recv.at[0], z, other).start()
    tok.wait_send()
    is_relay = (z == relays[0]) | (z == relays[last])

    @pl.when(jnp.logical_not(is_relay))
    def _():
        wait_all(sq_in, kv - 1, sq_send.at[0], False)
        wait_all(chunk_in, kv - 1, rs_send.at[0], False)

    @pl.when(is_relay)
    def _():
        wait_all(sq_in, kv - 2, sq_send.at[0], False)
        wait_all(chunk_in, kv - 2, rs_send.at[0], False)
        remote(relayed_out, relayed_in, relayed_send.at[0], relayed_recv.at[0], z, other).wait_send()

    weight_copies[0].wait()
    swaps[0].wait_recv()
    wait_all(mix, kv, mix_recv.at[0])
    by_head = dot(gather, mix[...].reshape(kv * group, dv)).astype(BF16)
    every = jnp.concatenate([by_head[h * rows : (h + 1) * rows] for h in range(heads_local)], axis=1)
    part_out[...] = packed(dot_t(every, out_w[1]))
    part = remote(part_out, part_in, pair_send.at[5], pair_recv.at[5], z, other)
    part.start()
    kept = packed(dot_t(every, out_w[0])) + packed(own)
    part.wait_recv()
    middle = (kept + part_in[...]).astype(BF16)
    mid_own[...] = middle
    half = z // half_kv
    half_z = lax.rem(z, half_kv)
    kept_here = half == c
    for d in far_first:
        remote(mid_own, mid.at[half_z * tp + c], mid_send.at[0], mid_recv.at[0], peer(d), half).start()

    @pl.when(kept_here)
    def _():
        mid[half_z * tp + c] = middle

    @pl.when(jnp.logical_not(kept_here))
    def _():
        remote(mid_own, mid.at[half_z * tp + c], mid_send.at[0], mid_recv.at[0], z, half).start()

    part.wait_send()
    wait_all(mix, kv, mix_send.at[0], False)
    for copy in swaps:
        copy.wait_send()
    gain = mlp_gain[pl.ds(pl.multiple_of(c * half_kv, half_kv), half_kv), :]
    for w in weight_copies[1:]:
        w.wait()
    for s in swaps[1:]:
        s.wait_recv()
    def wait_others(buffer, sem, received=True):
        @pl.when(kept_here)
        def _():
            wait_all(buffer, kv - 1, sem, received)

        @pl.when(jnp.logical_not(kept_here))
        def _():
            wait_all(buffer, kv, sem, received)

    wait_others(mid, mid_recv.at[0])
    tops, bottoms = [], []
    squares = jnp.zeros((half_rows, tp * feats), F32)
    for i in range(half_kv):
        a = mid[tp * i].astype(F32)
        b = mid[tp * i + 1].astype(F32)
        squares = squares + a * a + b * b
        g = gain[i : i + 1]
        tops.append((jnp.where(low, a, halves_swapped(b)) * g).astype(BF16))
        bottoms.append((jnp.where(low, halves_swapped(a), b) * g).astype(BF16))
    features = jnp.concatenate(
        [jnp.concatenate(tops, axis=1), jnp.concatenate(bottoms, axis=1)], axis=0
    )
    sq_top = jnp.sum(jnp.where(low, squares, 0.0), axis=1, keepdims=True)
    sq_bottom = jnp.sum(jnp.where(low, 0.0, squares), axis=1, keepdims=True)
    sq_mid = jnp.concatenate([sq_top, sq_bottom], axis=0)
    wide_out[4, :, :] = jnp.broadcast_to(sq_mid, wide_out.shape[1:])
    sums = [dot_t(features, mlp_w[i]) for i in range(4)]
    for i in range(4):
        wide_out[i, :, pl.ds(0, units)] = sums[i]
    remote(wide_out, wide_in, pair_send.at[6], pair_recv.at[6], z, other).start()
    remote(wide_out, wide_in, pair_send.at[6], pair_recv.at[6], z, other).wait_recv()
    mlp_scale = lax.rsqrt((sq_mid + wide_in[4, :, 0:1]) / width + EPS)
    terms = None
    for i in range(2):
        gate = (sums[2 * i] + wide_in[2 - 2 * i, :, pl.ds(0, units)]) * mlp_scale
        upward = (sums[2 * i + 1] + wide_in[3 - 2 * i, :, pl.ds(0, units)]) * mlp_scale
        hidden = (gate * jax.nn.sigmoid(gate) * upward).astype(BF16)
        term = dot(hidden, down_w[i])
        terms = term if terms is None else terms + term

    for i in range(half_kv):
        at = slice(i * tp * feats, (i + 1) * tp * feats)
        top, bottom = terms[:half_rows, at], terms[half_rows:, at]
        for to_c, message in (
            (0, jnp.where(low, top, halves_swapped(bottom))),
            (1, jnp.where(low, halves_swapped(top), bottom)),
        ):
            terms_out[tp * i + to_c] = message.astype(BF16)

    def term_copy(to, to_c):
        n = tp * (to - c * half_kv) + to_c
        return remote(terms_out.at[n], terms_in.at[z], term_send.at[0], term_recv.at[0], to, to_c)

    for d in far_first:
        to = peer(d)

        @pl.when(to // half_kv == c)
        def _(to=to):
            for to_c in range(tp):
                term_copy(to, to_c).start()

    @pl.when(kept_here)
    def _():
        term_copy(z, other).start()
        terms_in[z] = terms_out[tp * (z - c * half_kv) + c]

    remote(wide_out, wide_in, pair_send.at[6], pair_recv.at[6], z, other).wait_send()
    wait_others(mid, mid_send.at[0], False)
    wait_others(terms_in, term_recv.at[0])
    summed = middle.astype(F32) + jnp.sum(terms_in[...].astype(F32), axis=0)
    result[pl.ds(0, half_rows), :] = summed[:, :feats].astype(BF16)
    result[pl.ds(half_rows, half_rows), :] = summed[:, feats:].astype(BF16)

    wait_others(terms_in, term_send.at[0], False)


def write_out(result, new_state, result_out, new_state_out, sem):
    copies = [
        pltpu.make_async_copy(new_state, new_state_out, sem.at[0]),
        pltpu.make_async_copy(result, result_out, sem.at[1]),
    ]
    for copy in copies:
        copy.start()
    for copy in copies:
        copy.wait()


def body(
    kv,
    tp,
    tokens,
    past_state,
    mix_gain,
    w_query,
    w_forget,
    w_value,
    w_gate_out,
    floor_logits,
    head_gain,
    w_out,
    mlp_gain,
    w_gate,
    w_up,
    w_down,
):
    rows, feats = tokens.shape
    seqs, heads_local, dk, dv = past_state.shape
    units = w_gate.shape[1]
    group = heads_local * seqs
    channels = heads_local * dv
    half_cols = w_down.shape[1] // tp
    wide = -(-units // 128) * 128
    in_vmem = pl.BlockSpec(memory_space=pltpu.VMEM)
    dma = pltpu.SemaphoreType.DMA
    outputs = pl.pallas_call(
        functools.partial(kernel, kv, tp),
        name="decode_step",
        out_shape=(
            jax.ShapeDtypeStruct((rows, feats), BF16),
            jax.ShapeDtypeStruct(past_state.shape, F32),
        ),
        in_specs=[pl.BlockSpec(memory_space=pltpu.HBM)] * 14,
        out_specs=(in_vmem, in_vmem),
        scratch_shapes=[
            pltpu.VMEM((rows, feats), BF16),
            pltpu.VMEM((1, tp * feats), F32),
            pltpu.VMEM((heads_local, dk), F32),
            pltpu.VMEM((1, dv), F32),
            pltpu.VMEM((kv, tp * feats), F32),
            pltpu.VMEM((rows // 2, 2 * feats), BF16),
            pltpu.VMEM((rows // 2, 2 * feats), BF16),
            pltpu.VMEM((4, *w_query.shape), BF16),
            pltpu.VMEM(past_state.shape, F32),
            pltpu.VMEM((2, feats, channels), BF16),
            pltpu.VMEM((4, units, half_cols), BF16),
            pltpu.VMEM((2, units, half_cols), BF16),
            pltpu.VMEM((group, dk), F32),
            pltpu.VMEM((group, dv), F32),
            pltpu.VMEM((kv, 4 * group, dk), BF16),
            pltpu.VMEM((kv, 4 * group, dk), BF16),
            pltpu.VMEM((kv, seqs, dk), F32),
            pltpu.VMEM((kv, seqs, dk), F32),
            pltpu.VMEM((4 * group + 8, dk), F32),
            pltpu.VMEM((kv, 4 * group, dk), BF16),
            pltpu.VMEM((kv, 4 * group, dk), BF16),
            pltpu.VMEM((kv, seqs, dk), F32),
            pltpu.VMEM((4 * group + 8, dk), F32),
            pltpu.VMEM((4 * group + 8, dk), F32),
            pltpu.VMEM((group, dv), BF16),
            pltpu.VMEM((kv, group, dv), BF16),
            pltpu.VMEM((rows // 2, 2 * feats), F32),
            pltpu.VMEM((rows // 2, 2 * feats), F32),
            pltpu.VMEM((rows // 2, 2 * feats), BF16),
            pltpu.VMEM((kv, rows // 2, 2 * feats), BF16),
            pltpu.VMEM((5, rows, wide), F32),
            pltpu.VMEM((5, rows, wide), F32),
            pltpu.VMEM((kv, rows // 2, 2 * feats), BF16),
            pltpu.VMEM((kv, rows // 2, 2 * feats), BF16),
            dma((11,)),
            dma((7,)),
            dma((7,)),
            *[dma((1,))] * 10,
            dma((kv,)),
            *[dma((1,))] * 4,
            pltpu.SemaphoreType.REGULAR,
            pltpu.SemaphoreType.REGULAR((kv,)),
        ],
        compiler_params=pltpu.CompilerParams(
            collective_id=0, has_side_effects=True, vmem_limit_bytes=VMEM_BYTES
        ),
    )(*hbm(
        tokens,
        past_state,
        mix_gain.reshape(1, -1),
        w_query,
        w_forget,
        w_value,
        w_gate_out,
        floor_logits.reshape(heads_local, dk),
        head_gain.reshape(1, -1),
        w_out.T,
        mlp_gain.reshape(kv, tp * feats),
        w_gate.T,
        w_up.T,
        w_down,
    ))
    return pl.pallas_call(
        write_out,
        name="write_out",
        out_shape=tuple(jax.ShapeDtypeStruct(a.shape, a.dtype) for a in outputs),
        in_specs=[in_vmem] * len(outputs),
        out_specs=(pl.BlockSpec(memory_space=pltpu.HBM),) * len(outputs),
        scratch_shapes=[dma((len(outputs),))],
        compiler_params=pltpu.CompilerParams(vmem_limit_bytes=16 * 1024 * 1024),
    )(*outputs)


def solution(mesh):
    placed = (
        P(("grp", "dp"), ("kv", "tp")),
        P(("grp", "dp", "kv"), "tp", None, None),
        P("kv"),
        P("kv", "tp"),
        P("kv", "tp"),
        P("kv", "tp"),
        P("kv", "tp"),
        P("tp"),
        P(),
        P(None, ("kv", "tp")),
        P(),
        P(None, ("kv", "tp")),
        P(None, ("kv", "tp")),
        P(("kv", "tp"), None),
    )
    return jax.shard_map(
        functools.partial(body, mesh.shape["kv"], mesh.shape["tp"]),
        mesh=mesh,
        in_specs=placed,
        out_specs=(P(("grp", "dp"), ("kv", "tp")), P(("grp", "dp", "kv"), "tp", None, None)),
        check_vma=False,
    )
```

```python
import functools

import jax
import jax.numpy as jnp
from jax import lax
from jax.experimental import pallas as pl
from jax.experimental.pallas import tpu as pltpu
from jax.sharding import PartitionSpec as P

MESH = pl.DeviceIdType.MESH
EPS = 1e-06
VMEM_BYTES = 48 * 1024 * 1024
F32 = jnp.float32
BF16 = jnp.bfloat16


def dot(a, b):
    return jnp.dot(a, b, preferred_element_type=F32)


def dot_t(a, b):
    return lax.dot_general(a, b, (((1,), (1,)), ((), ())), preferred_element_type=F32)


def hbm(*arrays):
    return [pltpu.with_memory_space_constraint(a, pltpu.HBM) for a in arrays]


def packed(x):
    half = x.shape[0] // 2
    return jnp.concatenate([x[:half], x[half:]], axis=1)


def halves_swapped(x):
    return pltpu.roll(x, x.shape[1] // 2, 1)


def kernel(
    kv,
    tp,
    tokens_hbm,
    past_state,
    mix_gain_hbm,
    w_query,
    w_forget,
    w_value,
    w_gate_out,
    floor_hbm,
    head_gain_hbm,
    w_out,
    mlp_gain_hbm,
    w_gate,
    w_up,
    w_down,
    result,
    new_state,
    tokens,
    mix_gain,
    floor_logits,
    head_gain,
    mlp_gain,
    tok_own,
    tok_other,
    proj_w,
    state,
    out_w,
    mlp_w,
    down_w,
    floors,
    heads,
    chunk_out,
    chunk_in,
    sq_out,
    sq_in,
    total,
    joint_in,
    relay_in,
    relay_sq_in,
    relayed_out,
    relayed_in,
    mix_own,
    mix,
    part_out,
    part_in,
    mid_own,
    mid,
    wide_out,
    wide_in,
    terms_out,
    terms_in,
    local_sem,
    pair_send,
    pair_recv,
    rs_send,
    rs_recv,
    sq_send,
    sq_recv,
    mix_send,
    mix_recv,
    mid_send,
    mid_recv,
    term_send,
    term_recv,
    joint_recv,
    relay_recv,
    relay_sq_recv,
    relayed_send,
    relayed_recv,
    pair_in,
    ready,
):
    z = lax.axis_index("kv")
    c = lax.axis_index("tp")
    other = 1 - c
    rows, feats = tokens.shape
    seqs, heads_local, dk, dv = past_state.shape
    units = w_gate.shape[0]
    group = heads_local * seqs
    half_rows = rows // 2
    width = kv * tp * feats
    half_kv = kv // tp
    half_cols = half_kv * tp * feats

    def local(src, dst, i):
        copy = pltpu.make_async_copy(src, dst, local_sem.at[i])
        copy.start()
        return copy

    def remote(src, dst, send, recv, to_z, to_c):
        return pltpu.make_async_remote_copy(
            src_ref=src,
            dst_ref=dst,
            send_sem=send,
            recv_sem=recv,
            device_id={"kv": to_z, "tp": to_c},
            device_id_type=MESH,
        )

    def peer(d):
        return lax.rem(z + d, kv)

    def place(w):
        return jnp.where(w == 0, kv - 2, jnp.where(w == kv - 1, kv - 1, w - 1))

    order = [*range(1, kv - 1), 0, kv - 1]
    last = kv - 1
    near_last = [w for w in range(kv - tp - 2, kv - 1)]
    middle_z = kv // 2
    far_side = list(range(middle_z - 3, middle_z + 3))
    relays = {0: kv // 4 - 1, last: near_last[0] - 1}
    behind = near_last[0] - 1
    listeners = {0: [relays[0], *near_last], last: [relays[last], *near_last, 0]}
    far_first = sorted(range(1, kv), key=lambda d: -min(d, kv - d))

    def wait_all(buffer, count, sem, received=True):
        part_of = buffer.at[pl.ds(0, count)]
        copy = remote(part_of, part_of, sem, sem, z, other)
        copy.wait_recv() if received else copy.wait_send()

    barrier = pltpu.get_barrier_semaphore()

    def signal(sem, to_z, to_c):
        pl.semaphore_signal(sem, inc=1, device_id={"kv": to_z, "tp": to_c}, device_id_type=MESH)

    @pl.when(c == 1)
    def _():
        signal(barrier, z, 0)

    tokens_copy = local(tokens_hbm, tokens, 2)
    gain_copy = local(mix_gain_hbm, mix_gain, 3)
    for i, w in enumerate((w_query, w_forget, w_value, w_gate_out)):
        local(w, proj_w.at[i], 0)
    state_copy = local(past_state, state, 1)
    small_copies = [
        local(floor_hbm, floor_logits, 4),
        local(head_gain_hbm, head_gain, 5),
        local(mlp_gain_hbm, mlp_gain, 6),
    ]
    is_special = (z == 0) | (z == last)
    half_of = pl.ds(pl.multiple_of(c * half_cols, half_cols), half_cols)
    half_of_other = pl.ds(pl.multiple_of(other * half_cols, half_cols), half_cols)
    weight_copies = [
        local(w_out.at[:, half_of_other], out_w.at[0], 7),
        local(w_gate.at[:, half_of], mlp_w.at[0], 8),
        local(w_up.at[:, half_of], mlp_w.at[1], 9),
        local(w_down.at[:, half_of], down_w.at[0], 10),
    ]

    @pl.when(c == 0)
    def _():
        pl.semaphore_wait(barrier, 1)
        signal(pair_in, z, 1)

    @pl.when(c == 1)
    def _():
        pl.semaphore_wait(pair_in, 1)
        for w in order:

            @pl.when(place(z) < place(w))
            def _(w=w):
                signal(barrier, w, 1)

    def count_and_tell():
        @pl.when(c == 1)
        def _():
            @pl.when(place(z) > 0)
            def _():
                pl.semaphore_wait(barrier, place(z))

            signal(pair_in, z, 0)

        @pl.when(c == 0)
        def _():
            pl.semaphore_wait(pair_in, 1)

        for special, told in listeners.items():

            @pl.when(z == special)
            def _(special=special, told=told):
                for w in told:
                    if order.index(w) < order.index(special):
                        signal(ready.at[special], w, c)

        for d in far_first:
            to = peer(d)

            @pl.when((place(to) < place(z)) & (place(z) < kv - 2))
            def _(to=to):
                signal(ready.at[z], to, c)

    @pl.when(z != last)
    def _():
        count_and_tell()

    tokens_copy.wait()
    own = tokens[...].astype(F32)
    tok_own[...] = packed(own).astype(BF16)
    tok = remote(tok_own, tok_other, pair_send.at[0], pair_recv.at[0], z, other)
    tok.start()

    r = lax.broadcasted_iota(jnp.int32, (kv * group, kv * group), 0)
    col = lax.broadcasted_iota(jnp.int32, (kv * group, kv * group), 1)
    s_of = lax.rem(r, seqs)
    to_chunks = lax.rem(r // seqs, heads_local) * (kv * seqs) + (r // group) * seqs + s_of
    spread = jnp.where(col == to_chunks, 1.0, 0.0).astype(BF16)
    to_heads = lax.rem(r // seqs, kv) * group + (r // (kv * seqs)) * seqs + s_of
    gather = jnp.where(col == to_heads, 1.0, 0.0).astype(BF16)

    lane = lax.broadcasted_iota(jnp.int32, (1, tp * feats), 1)
    low = lane < feats
    own_twice = jnp.concatenate([own, own], axis=1)
    tok.wait_recv()

    @pl.when(z == last)
    def _():
        count_and_tell()

    got = tok_other[...].astype(F32)
    got_swapped = halves_swapped(got)
    got_twice = jnp.concatenate(
        [jnp.where(low, got, got_swapped), jnp.where(low, got_swapped, got)], axis=0
    )
    mine = lax.broadcasted_iota(jnp.int32, (rows, tp * feats), 1) // feats == c
    block = jnp.where(mine, own_twice, got_twice)
    squares = jnp.sum(block * block, axis=1, keepdims=True)
    sq_out[...] = jnp.broadcast_to(squares, (rows, dk)).reshape(kv, seqs, dk)
    gain_copy.wait()
    gained = (block * mix_gain[...]).astype(BF16)
    def sq_copy(to):
        return remote(sq_out.at[to], sq_in.at[z], sq_send.at[0], sq_recv.at[0], to, c)

    def chunk_copy(to):
        return remote(chunk_out.at[to], chunk_in.at[z], rs_send.at[0], rs_recv.at[0], to, c)

    def sq_to_relay(special):
        return remote(
            sq_out.at[special], relay_sq_in.at[z - 1], sq_send.at[0], relay_sq_recv.at[0], relays[special], c
        )

    def chunk_to_relay(special):
        return remote(
            chunk_out.at[special], relay_in.at[z - 1], rs_send.at[0], relay_recv.at[0], relays[special], c
        )

    for d in far_first:
        to = peer(d)

        @pl.when(place(to) < place(z))
        def _(to=to):
            sq_copy(to).start()

    for special, relay in relays.items():

        @pl.when((z > relay) & (z <= behind))
        def _(special=special):
            sq_to_relay(special).start()

    pltpu.make_async_copy(proj_w, proj_w, local_sem.at[0]).wait()
    products = [dot(gained, proj_w[i]).astype(BF16) for i in range(4)]
    for i in (0, 2):
        stack = jnp.concatenate(
            [
                jnp.concatenate([p[:, h * dk : (h + 1) * dk] for p in products[i : i + 2]], axis=1)
                for h in range(heads_local)
            ],
            axis=0,
        )
        ordered = dot(spread, stack).astype(BF16)
        for j in range(2):
            chunk_out[:, pl.ds((i + j) * group, group), :] = ordered[:, j * dk : (j + 1) * dk].reshape(
                kv, group, dk
            )

    for d in far_first:
        to = peer(d)

        @pl.when((place(to) < place(z)) & jnp.logical_not(is_special))
        def _(to=to):
            chunk_copy(to).start()

    for special in (0, last):

        @pl.when(z == special)
        def _(special=special):
            for w in sorted(far_side, key=lambda w: -min(abs(w - special), kv - abs(w - special))):
                chunk_copy(w).start()

    for special, relay in relays.items():

        @pl.when((z > relay) & (z <= behind))
        def _(special=special):
            chunk_to_relay(special).start()

    swaps = [
        remote(w_out.at[:, half_of], out_w.at[1], pair_send.at[1], pair_recv.at[1], z, other),
        remote(w_gate.at[:, half_of_other], mlp_w.at[2], pair_send.at[2], pair_recv.at[2], z, other),
        remote(w_up.at[:, half_of_other], mlp_w.at[3], pair_send.at[3], pair_recv.at[3], z, other),
        remote(w_down.at[:, half_of_other], down_w.at[1], pair_send.at[4], pair_recv.at[4], z, other),
    ]
    @pl.when(jnp.logical_not(is_special))
    def _():
        for s in swaps:
            s.start()


    sq_in[z] = sq_out[z]
    chunk_in[z] = chunk_out[z]
    for copy in small_copies:
        copy.wait()
    lower_in = jax.nn.sigmoid(floor_logits[...])
    for h in range(heads_local):
        floors[pl.ds(h * seqs, seqs), :] = jnp.broadcast_to(lower_in[h : h + 1], (seqs, dk))

    for w in order[:-2]:

        @pl.when(place(z) < place(w))
        def _(w=w):
            pl.semaphore_wait(ready.at[w], 1)
            sq_copy(w).start()
            chunk_copy(w).start()
            for special, relay in relays.items():
                if relay == w:
                    sq_to_relay(special).start()
                    chunk_to_relay(special).start()

    for special, relay in relays.items():
        forward = remote(relayed_out, relayed_in, relayed_send.at[0], relayed_recv.at[0], special, c)

        @pl.when(z == relay)
        def _(special=special, forward=forward):
            wait_all(relay_sq_in, behind - 1, relay_sq_recv.at[0])
            wait_all(relay_in, behind - 1, relay_recv.at[0])
            relay_sq_in[z - 1] = sq_out[special]
            relay_in[z - 1] = chunk_out[special]
            sums = relay_in[0].astype(F32)
            squares = relay_sq_in[0]
            for i in range(1, behind):
                sums = sums + relay_in[i].astype(F32)
                squares = squares + relay_sq_in[i]
            relayed_out[pl.ds(0, 4 * group), :] = sums
            relayed_out[pl.ds(4 * group, seqs), :] = squares
            pl.semaphore_wait(ready.at[special], 1)
            forward.start()

        for w in listeners[special]:
            if w != relay and order.index(w) < order.index(special):

                @pl.when(z == w)
                def _(special=special):
                    pl.semaphore_wait(ready.at[special], 1)
                    sq_copy(special).start()
                    chunk_copy(special).start()

    sides = {0: list(range(far_side[0] - 1, 0, -1)), last: list(range(far_side[-1] + 1, last))}
    is_far = (z >= far_side[0]) & (z <= far_side[-1])

    @pl.when(jnp.logical_not(is_far | is_special))
    def _():
        chunk_in[last] = jnp.zeros(chunk_in.shape[1:], BF16)

    for special, partner in ((last, 0), (0, last)):

        @pl.when(z == special)
        def _(special=special, partner=partner):
            for w in sides[partner]:
                remote(
                    chunk_out.at[w], joint_in.at[w], rs_send.at[0], joint_recv.at[w], partner, c
                ).start()
            if special == last:
                chunk_copy(partner).start()
            for w in sides[special]:
                remote(joint_in.at[w], joint_in.at[w], joint_recv.at[w], joint_recv.at[w], z, other).wait_recv()
                chunk_out[w] = (chunk_out[w].astype(F32) + joint_in[w].astype(F32)).astype(BF16)
                remote(chunk_out.at[w], chunk_in.at[0], rs_send.at[0], rs_recv.at[0], w, c).start()

    def add_up(slots):
        sums = chunk_in[slots[0]].astype(F32)
        squares = sq_in[slots[0]]
        for w in slots[1:]:
            sums = sums + chunk_in[w].astype(F32)
            squares = squares + sq_in[w]
        return sums, squares

    is_special = (z == 0) | (z == last)

    @pl.when(jnp.logical_not(is_special))
    def _():
        wait_all(sq_in, kv - 1, sq_recv.at[0])
        @pl.when(is_far)
        def _():
            wait_all(chunk_in, kv - 1, rs_recv.at[0])

        @pl.when(jnp.logical_not(is_far))
        def _():
            wait_all(chunk_in, kv - 2, rs_recv.at[0])

        sums, squares = add_up(order)
        total[pl.ds(0, 4 * group), :] = sums
        total[pl.ds(4 * group, seqs), :] = squares

    @pl.when(is_special)
    def _():
        wait_all(sq_in, len(near_last) + 1, sq_recv.at[0])
        wait_all(chunk_in, len(near_last) + 1, rs_recv.at[0])
        sums, squares = add_up([*near_last, 0, last])
        remote(relayed_out, relayed_in, relayed_send.at[0], relayed_recv.at[0], z, other).wait_recv()
        total[pl.ds(0, 4 * group), :] = sums + relayed_in[pl.ds(0, 4 * group), :]
        total[pl.ds(4 * group, seqs), :] = squares + relayed_in[pl.ds(4 * group, seqs), :]
        for s in swaps:
            s.start()

    total_sq = total[pl.ds(4 * group, seqs), :]
    scale_s = lax.rsqrt(total_sq / width + EPS)
    row_of = lax.broadcasted_iota(jnp.int32, (group, dk), 0)
    scale = jnp.broadcast_to(scale_s[0:1], (group, dk))
    for s in range(1, seqs):
        scale = jnp.where(lax.rem(row_of, seqs) == s, jnp.broadcast_to(scale_s[s : s + 1], (group, dk)), scale)
    query = total[pl.ds(0, group), :] * scale
    forget_pre = total[pl.ds(group, group), :] * scale
    value = total[pl.ds(2 * group, group), :] * scale
    gate_pre = total[pl.ds(3 * group, group), :] * scale
    lower = floors[...]
    forget = lower + (1.0 - lower) * jax.nn.sigmoid(forget_pre)
    activ = query * jax.nn.sigmoid(query)
    columns = jnp.concatenate([forget, activ, jnp.zeros((dk - 2 * group, dk), F32)], axis=0).T

    state_copy.wait()
    for h in range(heads_local):
        for s in range(seqs):
            i = h * seqs + s
            v_row = value[i : i + 1]
            f_col = columns[:, i : i + 1]
            q_col = columns[:, group + i : group + i + 1]
            new = v_row + f_col * (state[s, h] - v_row)
            new_state[s, h] = new
            heads[pl.ds(i, 1), :] = jnp.sum(new * q_col, axis=0, keepdims=True)

    head_out = heads[...]
    normed = head_out * lax.rsqrt(jnp.mean(head_out * head_out, axis=1, keepdims=True) + EPS)
    mixed = normed * head_gain[...] * (gate_pre * jax.nn.sigmoid(gate_pre))
    mix_own[...] = mixed.astype(BF16)
    for d in far_first:
        remote(mix_own, mix.at[z], mix_send.at[0], mix_recv.at[0], peer(d), other).start()
    remote(mix_own, mix.at[z], mix_send.at[0], mix_recv.at[0], z, other).start()
    tok.wait_send()
    is_relay = (z == relays[0]) | (z == relays[last])

    @pl.when(jnp.logical_not(is_relay))
    def _():
        wait_all(sq_in, kv - 1, sq_send.at[0], False)
        wait_all(chunk_in, kv - 1, rs_send.at[0], False)

    @pl.when(is_relay)
    def _():
        wait_all(sq_in, kv - 2, sq_send.at[0], False)
        wait_all(chunk_in, kv - 2, rs_send.at[0], False)
        remote(relayed_out, relayed_in, relayed_send.at[0], relayed_recv.at[0], z, other).wait_send()

    weight_copies[0].wait()
    swaps[0].wait_recv()
    wait_all(mix, kv, mix_recv.at[0])
    by_head = dot(gather, mix[...].reshape(kv * group, dv)).astype(BF16)
    every = jnp.concatenate([by_head[h * rows : (h + 1) * rows] for h in range(heads_local)], axis=1)
    part_out[...] = packed(dot_t(every, out_w[1]))
    part = remote(part_out, part_in, pair_send.at[5], pair_recv.at[5], z, other)
    part.start()
    kept = packed(dot_t(every, out_w[0])) + packed(own)
    part.wait_recv()
    middle = (kept + part_in[...]).astype(BF16)
    mid_own[...] = middle
    half = z // half_kv
    half_z = lax.rem(z, half_kv)
    kept_here = half == c
    for d in far_first:
        remote(mid_own, mid.at[half_z * tp + c], mid_send.at[0], mid_recv.at[0], peer(d), half).start()

    @pl.when(kept_here)
    def _():
        mid[half_z * tp + c] = middle

    @pl.when(jnp.logical_not(kept_here))
    def _():
        remote(mid_own, mid.at[half_z * tp + c], mid_send.at[0], mid_recv.at[0], z, half).start()

    part.wait_send()
    wait_all(mix, kv, mix_send.at[0], False)
    for copy in swaps:
        copy.wait_send()
    gain = mlp_gain[pl.ds(pl.multiple_of(c * half_kv, half_kv), half_kv), :]
    for w in weight_copies[1:]:
        w.wait()
    for s in swaps[1:]:
        s.wait_recv()
    def wait_others(buffer, sem, received=True):
        @pl.when(kept_here)
        def _():
            wait_all(buffer, kv - 1, sem, received)

        @pl.when(jnp.logical_not(kept_here))
        def _():
            wait_all(buffer, kv, sem, received)

    wait_others(mid, mid_recv.at[0])
    tops, bottoms = [], []
    squares = jnp.zeros((half_rows, tp * feats), F32)
    for i in range(half_kv):
        a = mid[tp * i].astype(F32)
        b = mid[tp * i + 1].astype(F32)
        squares = squares + a * a + b * b
        g = gain[i : i + 1]
        tops.append((jnp.where(low, a, halves_swapped(b)) * g).astype(BF16))
        bottoms.append((jnp.where(low, halves_swapped(a), b) * g).astype(BF16))
    features = jnp.concatenate(
        [jnp.concatenate(tops, axis=1), jnp.concatenate(bottoms, axis=1)], axis=0
    )
    sq_top = jnp.sum(jnp.where(low, squares, 0.0), axis=1, keepdims=True)
    sq_bottom = jnp.sum(jnp.where(low, 0.0, squares), axis=1, keepdims=True)
    sq_mid = jnp.concatenate([sq_top, sq_bottom], axis=0)
    wide_out[4, :, :] = jnp.broadcast_to(sq_mid, wide_out.shape[1:])
    sums = [dot_t(features, mlp_w[i]) for i in range(4)]
    for i in range(4):
        wide_out[i, :, pl.ds(0, units)] = sums[i]
    remote(wide_out, wide_in, pair_send.at[6], pair_recv.at[6], z, other).start()
    remote(wide_out, wide_in, pair_send.at[6], pair_recv.at[6], z, other).wait_recv()
    mlp_scale = lax.rsqrt((sq_mid + wide_in[4, :, 0:1]) / width + EPS)
    terms = None
    for i in range(2):
        gate = (sums[2 * i] + wide_in[2 - 2 * i, :, pl.ds(0, units)]) * mlp_scale
        upward = (sums[2 * i + 1] + wide_in[3 - 2 * i, :, pl.ds(0, units)]) * mlp_scale
        hidden = (gate * jax.nn.sigmoid(gate) * upward).astype(BF16)
        term = dot(hidden, down_w[i])
        terms = term if terms is None else terms + term

    for i in range(half_kv):
        at = slice(i * tp * feats, (i + 1) * tp * feats)
        top, bottom = terms[:half_rows, at], terms[half_rows:, at]
        to = c * half_kv + i
        for to_c, message in (
            (0, jnp.where(low, top, halves_swapped(bottom))),
            (1, jnp.where(low, halves_swapped(top), bottom)),
        ):
            n = 2 * i + to_c
            terms_out[n] = message.astype(BF16)
            copy = remote(terms_out.at[n], terms_in.at[z], term_send.at[0], term_recv.at[0], to, to_c)
            to_self = jnp.logical_and(to == z, to_c == c)

            @pl.when(jnp.logical_not(to_self))
            def _(copy=copy):
                copy.start()

            @pl.when(to_self)
            def _(n=n):
                terms_in[z] = terms_out[n]

    remote(wide_out, wide_in, pair_send.at[6], pair_recv.at[6], z, other).wait_send()
    wait_others(mid, mid_send.at[0], False)
    wait_others(terms_in, term_recv.at[0])
    summed = middle.astype(F32) + jnp.sum(terms_in[...].astype(F32), axis=0)
    result[pl.ds(0, half_rows), :] = summed[:, :feats].astype(BF16)
    result[pl.ds(half_rows, half_rows), :] = summed[:, feats:].astype(BF16)

    wait_others(terms_in, term_send.at[0], False)


def write_out(result, new_state, result_out, new_state_out, sem):
    copies = [
        pltpu.make_async_copy(new_state, new_state_out, sem.at[0]),
        pltpu.make_async_copy(result, result_out, sem.at[1]),
    ]
    for copy in copies:
        copy.start()
    for copy in copies:
        copy.wait()


def body(
    kv,
    tp,
    tokens,
    past_state,
    mix_gain,
    w_query,
    w_forget,
    w_value,
    w_gate_out,
    floor_logits,
    head_gain,
    w_out,
    mlp_gain,
    w_gate,
    w_up,
    w_down,
):
    rows, feats = tokens.shape
    seqs, heads_local, dk, dv = past_state.shape
    units = w_gate.shape[1]
    group = heads_local * seqs
    channels = heads_local * dv
    half_cols = w_down.shape[1] // tp
    wide = -(-units // 128) * 128
    in_vmem = pl.BlockSpec(memory_space=pltpu.VMEM)
    dma = pltpu.SemaphoreType.DMA
    outputs = pl.pallas_call(
        functools.partial(kernel, kv, tp),
        name="decode_step",
        out_shape=(
            jax.ShapeDtypeStruct((rows, feats), BF16),
            jax.ShapeDtypeStruct(past_state.shape, F32),
        ),
        in_specs=[pl.BlockSpec(memory_space=pltpu.HBM)] * 14,
        out_specs=(in_vmem, in_vmem),
        scratch_shapes=[
            pltpu.VMEM((rows, feats), BF16),
            pltpu.VMEM((1, tp * feats), F32),
            pltpu.VMEM((heads_local, dk), F32),
            pltpu.VMEM((1, dv), F32),
            pltpu.VMEM((kv, tp * feats), F32),
            pltpu.VMEM((rows // 2, 2 * feats), BF16),
            pltpu.VMEM((rows // 2, 2 * feats), BF16),
            pltpu.VMEM((4, *w_query.shape), BF16),
            pltpu.VMEM(past_state.shape, F32),
            pltpu.VMEM((2, feats, channels), BF16),
            pltpu.VMEM((4, units, half_cols), BF16),
            pltpu.VMEM((2, units, half_cols), BF16),
            pltpu.VMEM((group, dk), F32),
            pltpu.VMEM((group, dv), F32),
            pltpu.VMEM((kv, 4 * group, dk), BF16),
            pltpu.VMEM((kv, 4 * group, dk), BF16),
            pltpu.VMEM((kv, seqs, dk), F32),
            pltpu.VMEM((kv, seqs, dk), F32),
            pltpu.VMEM((4 * group + 8, dk), F32),
            pltpu.VMEM((kv, 4 * group, dk), BF16),
            pltpu.VMEM((kv, 4 * group, dk), BF16),
            pltpu.VMEM((kv, seqs, dk), F32),
            pltpu.VMEM((4 * group + 8, dk), F32),
            pltpu.VMEM((4 * group + 8, dk), F32),
            pltpu.VMEM((group, dv), BF16),
            pltpu.VMEM((kv, group, dv), BF16),
            pltpu.VMEM((rows // 2, 2 * feats), F32),
            pltpu.VMEM((rows // 2, 2 * feats), F32),
            pltpu.VMEM((rows // 2, 2 * feats), BF16),
            pltpu.VMEM((kv, rows // 2, 2 * feats), BF16),
            pltpu.VMEM((5, rows, wide), F32),
            pltpu.VMEM((5, rows, wide), F32),
            pltpu.VMEM((kv, rows // 2, 2 * feats), BF16),
            pltpu.VMEM((kv, rows // 2, 2 * feats), BF16),
            dma((11,)),
            dma((7,)),
            dma((7,)),
            *[dma((1,))] * 10,
            dma((kv,)),
            *[dma((1,))] * 4,
            pltpu.SemaphoreType.REGULAR,
            pltpu.SemaphoreType.REGULAR((kv,)),
        ],
        compiler_params=pltpu.CompilerParams(
            collective_id=0, has_side_effects=True, vmem_limit_bytes=VMEM_BYTES
        ),
    )(*hbm(
        tokens,
        past_state,
        mix_gain.reshape(1, -1),
        w_query,
        w_forget,
        w_value,
        w_gate_out,
        floor_logits.reshape(heads_local, dk),
        head_gain.reshape(1, -1),
        w_out.T,
        mlp_gain.reshape(kv, tp * feats),
        w_gate.T,
        w_up.T,
        w_down,
    ))
    return pl.pallas_call(
        write_out,
        name="write_out",
        out_shape=tuple(jax.ShapeDtypeStruct(a.shape, a.dtype) for a in outputs),
        in_specs=[in_vmem] * len(outputs),
        out_specs=(pl.BlockSpec(memory_space=pltpu.HBM),) * len(outputs),
        scratch_shapes=[dma((len(outputs),))],
        compiler_params=pltpu.CompilerParams(vmem_limit_bytes=16 * 1024 * 1024),
    )(*outputs)


def solution(mesh):
    placed = (
        P(("grp", "dp"), ("kv", "tp")),
        P(("grp", "dp", "kv"), "tp", None, None),
        P("kv"),
        P("kv", "tp"),
        P("kv", "tp"),
        P("kv", "tp"),
        P("kv", "tp"),
        P("tp"),
        P(),
        P(None, ("kv", "tp")),
        P(),
        P(None, ("kv", "tp")),
        P(None, ("kv", "tp")),
        P(("kv", "tp"), None),
    )
    return jax.shard_map(
        functools.partial(body, mesh.shape["kv"], mesh.shape["tp"]),
        mesh=mesh,
        in_specs=placed,
        out_specs=(P(("grp", "dp"), ("kv", "tp")), P(("grp", "dp", "kv"), "tp", None, None)),
        check_vma=False,
    )
```
